32 devices in a mesh: ep: 8 (over z, x), tp: 4 (over y, core).
Axes of the slice: x: 2, y: 2, z: 4, core: 2. Of those that a mesh axis runs over, the one named last changes fastest.
Arguments:
- mixer_input: bfloat16 [2048, 2048], P('ep', 'tp'), may hold values from -80 to 80
- mixer_gain: float32 [2048], P('tp'), may hold values from 0.1 to 1.9
- time_step: float32 [2048, 128], P('ep', 'tp'), may hold values from 0.25 to 4
- pole_real: float32 [128, 32], P('tp'), may hold values from -0.1 to 0, as said below
- pole_imag: float32 [128, 32], P('tp'), may hold values from 0.25 to 3
- input_real: float32 [128, 32, 16], P('tp'), may hold values from -1 to 1
- input_imag: float32 [128, 32, 16], P('tp'), may hold values from -1 to 1
- read_real: float32 [128, 16, 32], P('tp'), may hold values from -1 to 1
- read_imag: float32 [128, 16, 32], P('tp'), may hold values from -1 to 1
- out_value: bfloat16 [2048, 2048], P(None, 'tp'), may hold values from -0.125 to 0.125
- out_gate: bfloat16 [2048, 2048], P(None, 'tp'), may hold values from -0.125 to 0.125
- expert_input: bfloat16 [1024, 2048], P('ep', 'tp'), may hold values from -80 to 80
- expert_gain: float32 [2048], P('tp'), may hold values from 0.1 to 1.9
- routes: int32 [1024, 2], P('ep'), may hold values from 0 to 7, all different within a row; in each aligned block of 128 rows (0 to 127, 128 to 255, ...) at most 64 rows name the same one
- route_weight: float32 [1024, 2], P('ep'), may hold values from 0.2 to 1
- expert_gate: bfloat16 [8, 2048, 4096], P('ep', None, 'tp'), may hold values from -0.125 to 0.125
- expert_up: bfloat16 [8, 2048, 4096], P('ep', None, 'tp'), may hold values from -0.125 to 0.125
- expert_down: bfloat16 [8, 4096, 2048], P('ep', 'tp'), may hold values from -0.125 to 0.125
Outputs:
- mixer_output: bfloat16 [2048, 2048], P('ep', 'tp')
- expert_output: bfloat16 [1024, 2048], P('ep', 'tp')
The draws below stay inside these ranges and needn't reach their ends.
Inputs may be any that keep to these rules, and one draw needn't show every extreme that they name: `routes`: each row names 2 different experts. Among the 128 rows of one index of ep, no expert is named more than 64 times, a bound that some block reaches in some of them. `pole_real`: every rate is negative.
All inputs are finite; a program needn't handle non-finite values.
Results may differ from the reference program's by a relative error of at most 0.02.
Values may be sent and summed in bfloat16 or wider, within the bound.
No kernel may reach another device: no remote copies, remote signals or barrier semaphores. Data moves between devices by JAX's collectives and lax.ppermute only.
A program may use at most 128 MiB of HBM per device.

```python
import math
import jax
import jax.numpy as jnp
import numpy as np
from jax import lax

D = 2048
GROUP_CH = 16
GROUPS = 128
STATE = 32
FFE = 4096
EXPERTS = 8
TOP = 2
TOK_A = 256
TOK_B = 128
BLOCK = 128
SEQ_A = 2048
SEQ_B = 1024
CAP = 64
N_EP = 8
N_TP = 4


def scaled_rows(key, length):
    first, second, third = jax.random.split(key, 3)
    base = jnp.clip(jax.random.normal(first, (length, D), jnp.float32), -6.0, 6.0)
    levels = jnp.exp(jax.random.uniform(second, (16,), jnp.float32, -1.1, 1.1))
    column_scale = jnp.repeat(levels, D // 16)
    return base * column_scale[None, :]


def draw_mixer_input(key, part):
    return scaled_rows(jax.random.fold_in(key, 7), SEQ_A).astype(jnp.bfloat16)


def draw_expert_input(key, part):
    return scaled_rows(jax.random.fold_in(key, 8), SEQ_B).astype(jnp.bfloat16)


def draw_time_step(key, part):
    first, second = jax.random.split(jax.random.fold_in(key, 9))
    spans = SEQ_A // TOK_A
    fine = jax.random.uniform(first, (SEQ_A, GROUPS), jnp.float32, -0.5, 0.5)
    coarse = jax.random.uniform(second, (spans, 1, GROUPS), jnp.float32, -0.8, 0.8)
    coarse = jnp.broadcast_to(coarse, (spans, TOK_A, GROUPS)).reshape(SEQ_A, GROUPS)
    return jnp.exp(fine + coarse)


def rate_table(key):
    first, second, third = jax.random.split(jax.random.fold_in(key, 101), 3)
    share = 0.5
    slow = jax.random.uniform(first, (GROUPS, STATE), jnp.float32) < share
    slow_rate = jnp.exp(jax.random.uniform(second, (GROUPS, STATE), jnp.float32, math.log(0.1), math.log(0.6))) / SEQ_A
    fast_rate = jnp.exp(jax.random.uniform(third, (GROUPS, STATE), jnp.float32, math.log(0.03), math.log(0.1)))
    return jnp.where(slow, slow_rate, fast_rate)


def draw_pole_real(key, part):
    return -rate_table(key)


def read_table(key, salt):
    rates = rate_table(key)
    scale = jnp.sqrt(2.4 * rates / STATE) * 1.4
    noise = jnp.clip(jax.random.normal(jax.random.fold_in(key, salt), (GROUPS, GROUP_CH, STATE), jnp.float32), -4.0, 4.0)
    return noise * scale[:, None, :]


def draw_read_real(key, part):
    return read_table(key, 202)


def draw_read_imag(key, part):
    return read_table(key, 203)


def spiked(values, rng, source, target, parts, factor):
    owner, partner = [(jnp.arange(values.shape[dim]) // (values.shape[dim] // parts)).reshape([-1 if axis == dim else 1 for axis in range(values.ndim)]) for dim in (source, target)]
    chosen = jax.random.permutation(rng, parts)[partner]
    strong = (owner == chosen) | (owner == (partner + parts // 2) % parts)
    return jnp.where(strong, factor * values, values)


def block_scale(own_key, dims, cuts, low, top_value):
    level, own = 1.0, jax.random.fold_in(own_key, 6)
    for position, shards_of in cuts:
        steps = jnp.exp(jax.random.uniform(jax.random.fold_in(own, position), (shards_of,), jnp.float32, low / len(cuts), top_value / len(cuts)))
        level = level * jnp.repeat(steps, dims[position] // shards_of).reshape([-1 if axis == position else 1 for axis in range(len(dims))])
    return level


def deal_out(stream_key, own, number, rows, number_of, top, reach, skew):
    ranking = jax.random.permutation(stream_key, number_of)
    heavy_load, common = portions_of(number_of, rows * top, reach, skew, True), portions_of(number_of, rows * top, reach, skew, False)
    places = jnp.arange(number_of)

    def named(sizes, offset_by):
        used = int((sizes > 0).sum())
        fixed = max(1, used // 4)
        moved = fixed + (places - fixed + offset_by * (used - fixed)) % max(1, number_of - fixed)
        return jnp.zeros((number_of,), jnp.int32).at[ranking[jnp.where(places < fixed, places, moved)]].set(jnp.asarray(sizes, jnp.int32))

    sizes = jnp.where(number % 4 == 0, named(heavy_load, number // 4), named(common, number - number // 4 - 1))
    mixed = jax.random.permutation(jax.random.fold_in(own, 3), number_of)
    source_of, taker = mixed[0:number_of // 2 * 2:2], mixed[1:number_of // 2 * 2:2]
    margin = jnp.minimum(sizes[source_of] - 1, reach - sizes[taker]) // 2
    margin = jnp.where((source_of == ranking[0]) | (taker == ranking[0]) | (sizes[taker] == 0), 0, jnp.maximum(margin, 0))
    moved = jax.random.randint(jax.random.fold_in(own, 4), (number_of // 2,), 0, 1 << 20) % (margin + 1)
    sizes = sizes.at[source_of].add(-moved).at[taker].add(moved)
    items = jnp.searchsorted(jnp.cumsum(sizes), jnp.arange(rows * top), side="right").astype(jnp.int32)
    table = items.reshape(top, rows).T
    table = table[jax.random.permutation(jax.random.fold_in(own, 1), rows)]
    offset_by = jax.random.randint(jax.random.fold_in(own, 2), (rows, 1), 0, top)
    return jnp.take_along_axis(table, (jnp.arange(top)[None, :] + offset_by) % top, axis=1)


def portions_of(amount, total, most, slope, full):
    weights = [(1 << 20) // math.isqrt(rank ** slope) + 1 for rank in range(1, amount + 1)]
    largest = most if full else min(most, max(-(-total // amount), total * weights[0] // sum(weights)))
    least = 1 if total - largest >= amount - 1 else 0
    counts, rest = [largest] + [least] * (amount - 1), total - largest - least * (amount - 1)
    while rest > 0:
        movable = [i for i in range(1, amount) if counts[i] < largest] or [i for i in range(1, amount) if counts[i] < most]
        pool, budget = sum([weights[i] for i in movable]), rest
        for i in movable:
            more = min(most - counts[i], max(1, budget * weights[i] // pool), rest)
            counts[i] = counts[i] + more
            rest = rest - more
    return np.array(counts)


def scatter_about(key, shape, width, bound, shards=(), held_as=jnp.bfloat16):
    values = width * jax.random.normal(key, shape, jnp.float32)
    if shards:
        values = values * block_scale(key, shape, shards, -0.22, 0.18)
    return jnp.clip(values, -bound, bound).astype(held_as)


def bell_draw_with(rng, extent, spread, reach, shards, heavy, kind=jnp.bfloat16):
    array = spread * jax.random.normal(rng, extent, jnp.float32)
    if shards:
        array = array * block_scale(rng, extent, shards, -0.22, 0.18)
    return jnp.clip(spiked(array, jax.random.fold_in(rng, 3), *heavy), -reach, reach).astype(kind)


def setup_inputs(seed: int = 0) -> dict:
    keys = jax.random.split(jax.random.key(seed), 19)
    mixer_input = draw_mixer_input(jax.random.fold_in(keys[18], 71), 0)
    mixer_gain = jnp.clip(1.0 + 0.18 * jax.random.normal(keys[1], (D,), jnp.float32), 0.1, 1.9)
    time_step = draw_time_step(jax.random.fold_in(keys[18], 71), 0)
    pole_real = draw_pole_real(jax.random.fold_in(keys[18], 71), 0)
    pole_imag = jnp.clip(0.25 + 2.75 * jax.random.uniform(keys[4], (GROUPS, STATE), jnp.float32) ** block_scale(keys[4], (GROUPS, STATE), ((0, 4),), -0.2, 0.2), 0.25, 3.0)
    input_real = scatter_about(keys[5], (GROUPS, STATE, GROUP_CH), (2 * GROUP_CH) ** -0.5, 1.0, ((0, 4),), jnp.float32)
    input_imag = scatter_about(keys[6], (GROUPS, STATE, GROUP_CH), (2 * GROUP_CH) ** -0.5, 1.0, ((0, 4),), jnp.float32)
    read_real = draw_read_real(jax.random.fold_in(keys[18], 71), 0)
    read_imag = draw_read_imag(jax.random.fold_in(keys[18], 71), 0)
    out_value = scatter_about(keys[9], (D, D), D ** -0.5, 0.125, ((1, 4),))
    out_gate = scatter_about(keys[10], (D, D), D ** -0.5, 0.125, ((1, 4),))
    expert_input = draw_expert_input(jax.random.fold_in(keys[18], 71), 0)
    expert_gain = jnp.clip(1.0 + 0.18 * jax.random.normal(keys[12], (D,), jnp.float32), 0.1, 1.9)
    routes_keys = jax.random.split(jax.random.fold_in(keys[13], 1), SEQ_B // TOK_B)
    routes_turns = jax.random.permutation(jax.random.fold_in(keys[13], 3), SEQ_B // TOK_B)
    routes = jax.vmap(lambda own, number: deal_out(jax.random.fold_in(keys[13], 2), own, number, TOK_B, EXPERTS, TOP, CAP, 1))(routes_keys, routes_turns).reshape((SEQ_B, TOP))
    route_weight = jnp.clip(0.2 + 0.8 * jax.random.uniform(keys[14], (SEQ_B, TOP), jnp.float32) ** block_scale(keys[14], (SEQ_B, TOP), ((0, 8),), -0.2, 0.2), 0.2, 1.0)
    expert_gate = scatter_about(keys[15], (EXPERTS, D, FFE), D ** -0.5, 0.125, ((0, 8), (2, 4)))
    expert_up = scatter_about(keys[16], (EXPERTS, D, FFE), D ** -0.5, 0.125, ((0, 8), (2, 4)))
    expert_down = bell_draw_with(keys[17], (EXPERTS, FFE, D), FFE ** -0.5, 0.125, ((0, 8), (1, 4)), (1, 2, 4, 2.0))
    return dict(mixer_input=mixer_input, mixer_gain=mixer_gain, time_step=time_step, pole_real=pole_real, pole_imag=pole_imag, input_real=input_real, input_imag=input_imag, read_real=read_real, read_imag=read_imag, out_value=out_value, out_gate=out_gate, expert_input=expert_input, expert_gain=expert_gain, routes=routes, route_weight=route_weight, expert_gate=expert_gate, expert_up=expert_up, expert_down=expert_down)


def layer_norm(rows, gain):
    wide = rows.astype(jnp.float32)
    average = lax.optimization_barrier(jnp.mean(wide, axis=1, keepdims=True))
    variance = lax.optimization_barrier(jnp.mean(wide * wide, axis=1, keepdims=True)) - average * average
    return (wide - average) * lax.rsqrt(variance + 1e-05) * gain[None, :]

def compose(earlier, later):
    a1r, a1i, b1r, b1i = earlier
    a2r, a2i, b2r, b2i = later
    return (a2r * a1r - a2i * a1i, a2r * a1i + a2i * a1r, a2r * b1r - a2i * b1i + b2r, a2r * b1i + a2i * b1r + b2i)

def mixer_part(mixer_input, mixer_gain, time_step, pole_real, pole_imag, input_real, input_imag, read_real, read_imag, out_value, out_gate):
    normed = layer_norm(mixer_input, mixer_gain)
    blocks = SEQ_A // BLOCK
    rows_in = normed.reshape(blocks, BLOCK, GROUPS, GROUP_CH)
    steps_in = time_step.reshape(blocks, BLOCK, GROUPS)
    denom = pole_real * pole_real + pole_imag * pole_imag
    highest = lax.Precision.HIGHEST

    def advance(carried, inputs):
        state_re, state_im = carried
        rows_blk, step_blk = inputs
        drive_re = jnp.einsum('tgm,gpm->tgp', rows_blk, input_real, precision=highest)
        drive_im = jnp.einsum('tgm,gpm->tgp', rows_blk, input_imag, precision=highest)
        delta = step_blk[:, :, None]
        magnitude = jnp.exp(pole_real[None] * delta)
        angle = pole_imag[None] * delta
        abar_re = magnitude * jnp.cos(angle)
        abar_im = magnitude * jnp.sin(angle)
        numer_re = abar_re - 1.0
        coef_re = (numer_re * pole_real[None] + abar_im * pole_imag[None]) / denom[None]
        coef_im = (abar_im * pole_real[None] - numer_re * pole_imag[None]) / denom[None]
        push_re = coef_re * drive_re - coef_im * drive_im
        push_im = coef_re * drive_im + coef_im * drive_re
        cum_re, cum_im, acc_re, acc_im = lax.associative_scan(compose, (abar_re, abar_im, push_re, push_im), axis=0)
        new_re = cum_re * state_re[None] - cum_im * state_im[None] + acc_re
        new_im = cum_re * state_im[None] + cum_im * state_re[None] + acc_im
        response = jnp.einsum('gmp,tgp->tgm', read_real, new_re, precision=highest) - jnp.einsum('gmp,tgp->tgm', read_imag, new_im, precision=highest)
        mixed_blk = jax.nn.gelu(response.reshape(BLOCK, D)).astype(jnp.bfloat16)
        return ((new_re[-1], new_im[-1]), mixed_blk)
    zeros_state = jnp.zeros((GROUPS, STATE), jnp.float32)
    unused, mixed = lax.scan(advance, (zeros_state, zeros_state), (rows_in, steps_in))
    mixed = mixed.reshape(SEQ_A, D)
    value_sum = jnp.dot(mixed, out_value, preferred_element_type=jnp.float32)
    gate_sum = jnp.dot(mixed, out_gate, preferred_element_type=jnp.float32)
    return (value_sum * jax.nn.sigmoid(gate_sum)).astype(jnp.bfloat16)

def expert_part(expert_input, expert_gain, routes, route_weight, expert_gate, expert_up, expert_down):
    normed = layer_norm(expert_input, expert_gain).astype(jnp.bfloat16)
    tokens = normed.shape[0]
    flat_routes = routes.reshape(-1)
    flat_weights = route_weight.reshape(-1)
    owners = jnp.arange(flat_routes.shape[0], dtype=jnp.int32) // TOP
    padded = jnp.concatenate([normed, jnp.zeros((1, D), jnp.bfloat16)], axis=0)
    limit = N_EP * CAP
    blocks = FFE // N_TP

    def one_expert(totals, index):
        hits = flat_routes == index
        where_to = jnp.cumsum(hits.astype(jnp.int32)) - 1
        target = jnp.where(hits, where_to, limit).astype(jnp.int32)
        holder = jnp.full((limit,), tokens, jnp.int32).at[target].set(owners, mode='drop')
        share = jnp.zeros((limit,), jnp.float32).at[target].set(flat_weights, mode='drop')
        rows = padded[holder]
        gate_w = lax.dynamic_index_in_dim(expert_gate, index, 0, keepdims=False)
        up_w = lax.dynamic_index_in_dim(expert_up, index, 0, keepdims=False)
        down_w = lax.dynamic_index_in_dim(expert_down, index, 0, keepdims=False)
        gate_val = jnp.dot(rows, gate_w, preferred_element_type=jnp.float32)
        up_val = jnp.dot(rows, up_w, preferred_element_type=jnp.float32)
        hidden = (jax.nn.silu(gate_val) * up_val).astype(jnp.bfloat16)
        pieces = hidden.reshape(limit, N_TP, blocks).astype(jnp.float32)
        down_pieces = down_w.reshape(N_TP, blocks, D).astype(jnp.float32)
        partial_value = jnp.einsum('snk,nkd->nsd', pieces, down_pieces).astype(jnp.bfloat16)
        result = lax.optimization_barrier(jnp.sum(partial_value.astype(jnp.float32), axis=0)).astype(jnp.bfloat16)
        contrib = result.astype(jnp.float32) * share[:, None]
        return (totals.at[holder].add(contrib), None)
    totals, unused = lax.scan(one_expert, jnp.zeros((tokens + 1, D), jnp.float32), jnp.arange(EXPERTS, dtype=jnp.int32))
    return totals[:tokens].astype(jnp.bfloat16)

def reference(mixer_input, mixer_gain, time_step, pole_real, pole_imag, input_real, input_imag, read_real, read_imag, out_value, out_gate, expert_input, expert_gain, routes, route_weight, expert_gate, expert_up, expert_down):
    mixer_output = mixer_part(mixer_input, mixer_gain, time_step, pole_real, pole_imag, input_real, input_imag, read_real, read_imag, out_value, out_gate)
    expert_output = expert_part(expert_input, expert_gain, routes, route_weight, expert_gate, expert_up, expert_down)
    return (mixer_output, expert_output)
```

```python
import functools

import jax
import jax.numpy as jnp
from jax import lax
from jax.experimental import pallas as pl
from jax.experimental.pallas import tpu as pltpu
from jax.sharding import PartitionSpec as P

f32 = jnp.float32
bf16 = jnp.bfloat16
norm_eps = 1e-05
LANES = 8
NT = (((1,), (1,)), ((), ()))
TN = (((0,), (0,)), ((), ()))


def iota(shape, dim):
    return lax.broadcasted_iota(jnp.int32, shape, dim)


def ones_where(mask):
    return jnp.where(mask, 1.0, 0.0).astype(bf16)


def split2(value):
    high = value.astype(bf16)
    return high, (value - high.astype(f32)).astype(bf16)


def split3(value):
    high = value.astype(bf16)
    rest = value - high.astype(f32)
    mid = rest.astype(bf16)
    return high, mid, (rest - mid.astype(f32)).astype(bf16)


def mm(left, right, dims=(((1,), (0,)), ((), ()))):
    return lax.dot_general(left, right, dims, preferred_element_type=f32)


def mm3(left, right, dims):
    lh, ll = left
    rh, rl = right
    return mm(lh, rh, dims) + (mm(ll, rh, dims) + mm(lh, rl, dims))


def mul(ar, ai, br, bi):
    return ar * br - ai * bi, ar * bi + ai * br


def slot_keys(routes_t, experts):
    top, tokens = routes_t.shape
    number = iota((experts, tokens), 0)
    hit = routes_t[0:1, :] == number
    for k in range(1, top):
        hit = hit | (routes_t[k : k + 1, :] == number)
    before = ones_where(iota((tokens, tokens), 0) < iota((tokens, tokens), 1))
    place = mm(ones_where(hit), before)
    return jnp.where(hit, place, -1.0)


def send_kernel(experts, capacity, routes_ref, rows_ref, out_ref):
    keys = slot_keys(routes_ref[...], experts)
    tokens = keys.shape[1]
    slot = iota((capacity, tokens), 0).astype(f32)
    chosen = [ones_where(slot == keys[e : e + 1, :]) for e in range(experts)]
    out_ref[...] = mm(jnp.concatenate(chosen, axis=0), rows_ref[...]).astype(bf16)


def combine_kernel(experts, capacity, routes_ref, weight_ref, back_ref, out_ref):
    routes_t = routes_ref[...]
    weight_t = weight_ref[...]
    keys = slot_keys(routes_t, experts)
    tokens = keys.shape[1]
    number = iota((experts, tokens), 0)
    share = jnp.zeros((experts, tokens), f32)
    for k in range(routes_t.shape[0]):
        share = share + jnp.where(routes_t[k : k + 1, :] == number, weight_t[k : k + 1, :], 0.0)
    slot = iota((capacity, tokens), 0).astype(f32)
    spread = [
        jnp.where(slot == keys[e : e + 1, :], share[e : e + 1, :], 0.0) for e in range(experts)
    ]
    high, mid, low = split3(jnp.concatenate(spread, axis=0))
    back = back_ref[...]
    out_ref[...] = (mm(high, back, TN) + (mm(mid, back, TN) + mm(low, back, TN))).astype(bf16)


def hidden_kernel(parts, me_ref, gain_ref, *refs):
    blocks = refs[:parts]
    gate_ref, up_ref, out_ref, normed_ref = refs[parts:]
    rows, feats = blocks[0].shape
    width = parts * feats
    chunk = 64

    @pl.when(pl.program_id(0) == 0)
    def _():
        me = me_ref[0]

        def body(step, unused):
            at = pl.ds(pl.multiple_of(step * chunk, chunk), chunk)
            total = jnp.zeros((chunk, 1), f32)
            square = jnp.zeros((chunk, 1), f32)
            for block in blocks:
                wide = block[at, :].astype(f32)
                total = total + jnp.sum(wide, axis=1, keepdims=True)
                square = square + jnp.sum(wide * wide, axis=1, keepdims=True)
            mean = total / width
            scale = lax.rsqrt(square / width - mean * mean + norm_eps)
            for k, block in enumerate(blocks):
                which = me ^ k
                wide = block[at, :].astype(f32)
                value = (wide - mean) * scale * gain_ref[which]
                cols = pl.ds(pl.multiple_of(which * feats, feats), feats)
                normed_ref[at, cols] = value.astype(bf16)
            return unused

        lax.fori_loop(0, rows // chunk, body, 0)

    normed = normed_ref[...]
    gate = mm(normed, gate_ref[0])
    up = mm(normed, up_ref[0])
    out_ref[...] = (gate * jax.nn.sigmoid(gate) * up).astype(bf16)


def down_kernel(me_ref, hidden_ref, weight_ref, out_ref):
    out_ref[0] = mm(hidden_ref[...], weight_ref[0]).astype(bf16)


def reorder(rows, back):
    steps = rows // LANES
    row, col = iota((rows, rows), 1 if back else 0), iota((rows, rows), 0 if back else 1)
    return ones_where(col == (row % LANES) * steps + row // LANES)


def sin_cos(angle):
    turns = jnp.floor(angle * 0.6366197723675814 + 0.5)
    rest = angle - turns * 1.5703125
    rest = rest - turns * 4.83751296997070312e-4
    rest = rest - turns * 7.54978995489188e-8
    z = rest * rest
    sine = rest + rest * z * (
        -1.6666654611e-1 + z * (8.3321608736e-3 + z * -1.9515295891e-4)
    )
    cosine = 1.0 - 0.5 * z + z * z * (
        4.166664568298827e-2 + z * (-1.388731625493765e-3 + z * 2.443315711809948e-5)
    )
    quarter = turns.astype(jnp.int32)
    odd = (quarter & 1) != 0
    first = jnp.where(odd, cosine, sine)
    second = jnp.where(odd, sine, cosine)
    first = jnp.where((quarter & 2) != 0, -first, first)
    second = jnp.where(((quarter + 1) & 2) != 0, -second, second)
    return first, second


def spread_table(table, inner, outer_rows, outer_cols, width):
    rows = table.shape[0]
    pick = ones_where(iota((inner, width), 1) % inner == iota((inner, width), 0))
    high, mid, low = split3(table)
    wide = mm(high, pick) + (mm(mid, pick) + mm(low, pick))
    same = iota((rows, width), 0) // outer_rows == iota((rows, width), 1) // outer_cols
    return jnp.where(same, wide, 0.0)


def scan_kernel(
    total, x_ref, sums_ref, gain_ref, step_ref, pr_ref, pi_ref, ir_ref, ii_ref,
    hr_ref, hi_ref, cr_ref, ci_ref, end_ref, ar_ref, ai_ref,
):
    rows, feats = x_ref.shape
    groups = step_ref.shape[1]
    flat = pr_ref.shape[1]
    states = flat // groups
    inner = feats // groups
    steps = rows // LANES
    order = reorder(rows, False)
    sums = jnp.sum(sums_ref[...], axis=0)
    mean = sums[0:1, :] / total
    scale = lax.rsqrt(sums[1:2, :] / total - mean * mean + norm_eps)
    match = iota((rows, rows), 1) == (iota((rows, rows), 0) % LANES) * steps + iota(
        (rows, rows), 0
    ) // LANES
    mean_col = jnp.sum(jnp.where(match, mean, 0.0), axis=1, keepdims=True)
    scale_col = jnp.sum(jnp.where(match, scale, 0.0), axis=1, keepdims=True)
    d_high, d_mid, d_low = (
        mm(order, part).astype(bf16) for part in split3(step_ref[...])
    )
    piece = min(flat, 256)
    for at in range(0, flat, piece):
        cols = pl.ds(at, piece)
        expand = ones_where(
            iota((groups, piece), 0) == (iota((groups, piece), 1) + at) // states
        )
        delta = mm(d_high, expand) + (mm(d_mid, expand) + mm(d_low, expand))
        size = jnp.exp(pr_ref[:, cols] * delta)
        sine, cosine = sin_cos(pi_ref[:, cols] * delta)
        ar_ref[:, cols] = size * cosine
        ai_ref[:, cols] = size * sine
    cw = min(feats, 256)
    for b in range(feats // cw):
        chans = pl.ds(b * cw, cw)
        sw = cw // inner * states
        cols = pl.ds(b * sw, sw)
        rows_in = mm(order, x_ref[:, chans])
        normed = split2((rows_in - mean_col) * scale_col * gain_ref[:, chans])
        real = split2(spread_table(ir_ref[cols, :], inner, states, inner, cw))
        imag = split2(spread_table(ii_ref[cols, :], inner, states, inner, cw))
        drive_re = mm3(normed, real, NT)
        drive_im = mm3(normed, imag, NT)
        pr, pi = pr_ref[:, cols], pi_ref[:, cols]
        size = pr * pr + pi * pi
        hr_ref[:, cols], hi_ref[:, cols] = mul(drive_re, drive_im, pr / size, -pi / size)
    span = min(flat, 512)
    for at in range(0, flat, span):
        cols = pl.ds(at, span)

        def body(j, carry):
            h_re, h_im, c_re, c_im = carry
            here = pl.ds(pl.multiple_of(j * LANES, LANES), LANES)
            a_re, a_im = ar_ref[here, cols], ai_ref[here, cols]
            d_re, d_im = hr_ref[here, cols], hi_ref[here, cols]
            h_re, h_im = mul(a_re, a_im, h_re + d_re, h_im + d_im)
            h_re, h_im = h_re - d_re, h_im - d_im
            c_re, c_im = mul(a_re, a_im, c_re, c_im)
            hr_ref[here, cols], hi_ref[here, cols] = h_re, h_im
            cr_ref[here, cols], ci_ref[here, cols] = c_re, c_im
            return h_re, h_im, c_re, c_im

        zero = jnp.zeros((LANES, span), f32)
        lax.fori_loop(0, steps, body, (zero, zero, zero + 1.0, zero))
    last = pl.ds(rows - LANES, LANES)
    h_re, h_im, c_re, c_im = hr_ref[last, :], hi_ref[last, :], cr_ref[last, :], ci_ref[last, :]
    p_re, p_im = c_re[0:1], c_im[0:1]
    s_re, s_im = h_re[0:1], h_im[0:1]
    for c in range(1, LANES):
        k_re, k_im = c_re[c : c + 1], c_im[c : c + 1]
        p_re, p_im = mul(k_re, k_im, p_re, p_im)
        s_re, s_im = mul(k_re, k_im, s_re, s_im)
        s_re, s_im = s_re + h_re[c : c + 1], s_im + h_im[c : c + 1]
    end_ref[...] = jnp.concatenate([p_re, p_im, s_re, s_im], axis=0)


def read_kernel(
    me_ref, got_ref, hr_ref, hi_ref, cr_ref, ci_ref, rr_ref, ri_ref, out_ref,
):
    rows, flat = hr_ref.shape
    feats = out_ref.shape[1]
    states = rr_ref.shape[1]
    inner = feats // (flat // states)
    steps = rows // LANES
    me = me_ref[0]
    s_re = jnp.zeros((1, flat), f32)
    s_im = jnp.zeros((1, flat), f32)
    for i in range(got_ref.shape[0] - 1):
        ends = got_ref[i]
        n_re, n_im = mul(ends[0:1], ends[1:2], s_re, s_im)
        s_re = jnp.where(i < me, n_re + ends[2:3], s_re)
        s_im = jnp.where(i < me, n_im + ends[3:4], s_im)
    last = pl.ds(rows - LANES, LANES)
    h_re, h_im, c_re, c_im = hr_ref[last, :], hi_ref[last, :], cr_ref[last, :], ci_ref[last, :]
    in_re, in_im = [s_re], [s_im]
    for c in range(LANES - 1):
        n_re, n_im = mul(c_re[c : c + 1], c_im[c : c + 1], in_re[-1], in_im[-1])
        in_re.append(n_re + h_re[c : c + 1])
        in_im.append(n_im + h_im[c : c + 1])
    in_re = jnp.concatenate(in_re, axis=0)[None]
    in_im = jnp.concatenate(in_im, axis=0)[None]
    back = reorder(rows, True)
    cw = min(feats, 256)
    sw = cw // inner * states
    for b in range(feats // cw):
        chans = pl.ds(b * cw, cw)
        lo = b * sw
        cols = pl.ds(lo, sw)
        shape = (steps, LANES, sw)
        c_re, c_im = cr_ref[:, cols].reshape(shape), ci_ref[:, cols].reshape(shape)
        g_re, g_im = in_re[:, :, lo : lo + sw], in_im[:, :, lo : lo + sw]
        f_re = hr_ref[:, cols].reshape(shape) + (c_re * g_re - c_im * g_im)
        f_im = hi_ref[:, cols].reshape(shape) + (c_re * g_im + c_im * g_re)
        real = split2(spread_table(rr_ref[chans, :], states, inner, states, sw))
        imag = split2(spread_table(ri_ref[chans, :], states, inner, states, sw))
        response = mm3(split2(f_re.reshape(rows, sw)), real, NT) - mm3(
            split2(f_im.reshape(rows, sw)), imag, NT
        )
        cube = response + 0.044715 * (response * response * response)
        mixed = 0.5 * response * (1.0 + jnp.tanh(0.7978845608028654 * cube))
        out_ref[:, chans] = mm(back, mixed.astype(bf16)).astype(bf16)


def output_kernel(parts, me_ref, *refs):
    pieces = refs[:parts]
    value_ref, gate_ref, out_ref = refs[parts:]
    feats = pieces[0].shape[1]
    value = gate = None
    for k, piece in enumerate(pieces):
        at = pl.ds(pl.multiple_of((me_ref[0] ^ k) * feats, feats), feats)
        rows = piece[...]
        v, g = mm(rows, value_ref[at, :]), mm(rows, gate_ref[at, :])
        value, gate = (v, g) if value is None else (value + v, gate + g)
    out_ref[...] = (value * jax.nn.sigmoid(gate)).astype(bf16)


vmem = pl.BlockSpec(memory_space=pltpu.VMEM)
smem = pl.BlockSpec(memory_space=pltpu.SMEM)
params = pltpu.CompilerParams(vmem_limit_bytes=56 << 20)


def swap(value, bit):
    count = lax.axis_size("tp")
    return lax.ppermute(value, "tp", [(i, i ^ bit) for i in range(count)])


def gather_tp(value):
    count = lax.axis_size("tp")
    blocks = {0: value}
    bit = count // 2
    while bit >= 1:
        blocks.update({k ^ bit: swap(block, bit) for k, block in list(blocks.items())})
        bit //= 2
    return [blocks[k] for k in range(count)]


def shards(
    mixer_input, mixer_gain, time_step, pole_real, pole_imag, input_real, input_imag,
    read_real, read_imag, out_value, out_gate, expert_input, expert_gain, routes,
    route_weight, expert_gate, expert_up, expert_down,
):
    n_tp, n_ep = lax.axis_size("tp"), lax.axis_size("ep")
    tp_at = lax.axis_index("tp").astype(jnp.int32).reshape(1)
    ep_at = lax.axis_index("ep").astype(jnp.int32).reshape(1)
    tokens, feats = expert_input.shape
    top = routes.shape[1]
    capacity = 2 * top * tokens // n_ep
    slots = n_ep * capacity
    routes_t = routes.T
    weight_t = route_weight.T

    send = pl.pallas_call(
        functools.partial(send_kernel, n_ep, capacity),
        out_shape=jax.ShapeDtypeStruct((slots, feats), bf16),
        in_specs=[vmem, vmem], out_specs=vmem, compiler_params=params, name="send_rows",
    )(routes_t, expert_input)
    arrived = lax.all_to_all(send, "ep", split_axis=0, concat_axis=0, tiled=True)

    rows, chans = mixer_input.shape
    wide = mixer_input.astype(f32)
    packed = jnp.concatenate(
        [jnp.sum(wide, axis=1), jnp.sum(wide * wide, axis=1), expert_gain]
    )
    packed = lax.all_gather(packed, "tp")
    sums = packed[:, : 2 * rows].reshape(n_tp, 2, rows)
    gains = packed[:, 2 * rows :].reshape(n_tp, 1, feats)

    groups, states = pole_real.shape
    flat = groups * states
    inner = input_real.shape[2]
    big = jax.ShapeDtypeStruct((rows, flat), f32)
    h_re, h_im, c_re, c_im, ends = pl.pallas_call(
        functools.partial(scan_kernel, float(chans * n_tp)),
        out_shape=(big, big, big, big, jax.ShapeDtypeStruct((4, flat), f32)),
        in_specs=[vmem] * 8, out_specs=(vmem,) * 5,
        scratch_shapes=[pltpu.VMEM((rows, flat), f32)] * 2,
        compiler_params=params, name="mixer_scan",
    )(
        mixer_input, sums, mixer_gain.reshape(1, chans), time_step,
        pole_real.reshape(1, flat), pole_imag.reshape(1, flat),
        input_real.reshape(flat, inner), input_imag.reshape(flat, inner),
    )
    got = lax.all_to_all(
        jnp.broadcast_to(ends[None], (n_ep, 4, flat)), "ep", split_axis=0, concat_axis=0
    )
    mixed = pl.pallas_call(
        read_kernel,
        out_shape=jax.ShapeDtypeStruct((rows, chans), bf16),
        in_specs=[smem] + [vmem] * 7, out_specs=vmem, compiler_params=params,
        name="mixer_read",
    )(
        ep_at, got, h_re, h_im, c_re, c_im,
        read_real.reshape(chans, states), read_imag.reshape(chans, states),
    )
    pieces = gather_tp(mixed)
    mixer_output = pl.pallas_call(
        functools.partial(output_kernel, n_tp),
        out_shape=jax.ShapeDtypeStruct((rows, out_value.shape[1]), bf16),
        in_specs=[smem] + [vmem] * (n_tp + 2), out_specs=vmem, compiler_params=params,
        name="mixer_out",
    )(tp_at, *pieces, out_value, out_gate)

    blocks = gather_tp(arrived)
    units = expert_gate.shape[2]
    unit_block = min(units, 256)
    hidden = pl.pallas_call(
        functools.partial(hidden_kernel, n_tp),
        grid=(units // unit_block,),
        out_shape=jax.ShapeDtypeStruct((slots, units), bf16),
        in_specs=[smem, vmem] + [vmem] * n_tp + [
            pl.BlockSpec((1, n_tp * feats, unit_block), lambda j: (0, 0, j)),
            pl.BlockSpec((1, n_tp * feats, unit_block), lambda j: (0, 0, j)),
        ],
        out_specs=pl.BlockSpec((slots, unit_block), lambda j: (0, j)),
        scratch_shapes=[pltpu.VMEM((slots, n_tp * feats), bf16)],
        compiler_params=params, name="expert_hidden",
    )(tp_at, gains, *blocks, expert_gate, expert_up)

    def down(odd):
        return pl.pallas_call(
            down_kernel,
            grid_spec=pltpu.PrefetchScalarGridSpec(
                num_scalar_prefetch=1,
                grid=(n_tp // 2,),
                in_specs=[
                    pl.BlockSpec((slots, units), lambda i, me: (0, 0)),
                    pl.BlockSpec((1, units, feats), lambda i, me: (0, 0, me[0] ^ (2 * i + odd))),
                ],
                out_specs=pl.BlockSpec((1, slots, feats), lambda i, me: (i, 0, 0)),
            ),
            out_shape=jax.ShapeDtypeStruct((n_tp // 2, slots, feats), bf16),
            compiler_params=params, name="expert_down",
        )(tp_at, hidden, expert_down)

    theirs = swap(down(1), 1)
    total = down(0).astype(f32) + theirs.astype(f32)
    bit = 2
    while bit < n_tp:
        total = total.reshape((-1, 2) + total.shape[1:])
        total = total[:, 0] + swap(total[:, 1].astype(bf16), bit).astype(f32)
        bit *= 2
    result = total[0].astype(bf16)
    back = lax.all_to_all(result, "ep", split_axis=0, concat_axis=0, tiled=True)
    expert_output = pl.pallas_call(
        functools.partial(combine_kernel, n_ep, capacity),
        out_shape=jax.ShapeDtypeStruct((tokens, feats), bf16),
        in_specs=[vmem] * 3, out_specs=vmem, compiler_params=params, name="combine",
    )(routes_t, weight_t, back)
    return mixer_output, expert_output


def solution(mesh):
    return jax.shard_map(
        shards,
        mesh=mesh,
        in_specs=(
            P("ep", "tp"), P("tp"), P("ep", "tp"), P("tp", None), P("tp", None),
            P("tp", None, None), P("tp", None, None), P("tp", None, None), P("tp", None, None),
            P(None, "tp"), P(None, "tp"), P("ep", "tp"), P("tp"), P("ep", None), P("ep", None),
            P("ep", None, "tp"), P("ep", None, "tp"), P("ep", "tp", None),
        ),
        out_specs=(P("ep", "tp"), P("ep", "tp")),
        check_vma=False,
    )
```

```python
import functools

import jax
import jax.numpy as jnp
from jax import lax
from jax.experimental import pallas as pl
from jax.experimental.pallas import tpu as pltpu
from jax.sharding import PartitionSpec as P


f32 = jnp.float32
bf16 = jnp.bfloat16
norm_eps = 1e-05
LANES = 8
NN = (((1,), (0,)), ((), ()))
NT = (((1,), (1,)), ((), ()))
TN = (((0,), (0,)), ((), ()))


def iota(shape, dim):
    return lax.broadcasted_iota(jnp.int32, shape, dim)


def ones_where(mask):
    return jnp.where(mask, 1.0, 0.0).astype(bf16)


def split2(value):
    high = value.astype(bf16)
    return high, (value - high.astype(f32)).astype(bf16)


def split3(value):
    high = value.astype(bf16)
    rest = value - high.astype(f32)
    mid = rest.astype(bf16)
    return high, mid, (rest - mid.astype(f32)).astype(bf16)


def mm(left, right, dims=NN):
    return lax.dot_general(left, right, dims, preferred_element_type=f32)


def mm3(left, right, dims):
    lh, ll = left
    rh, rl = right
    return mm(lh, rh, dims) + (mm(ll, rh, dims) + mm(lh, rl, dims))


def mul(ar, ai, br, bi):
    return ar * br - ai * bi, ar * bi + ai * br


def slot_keys(routes_t, experts):
    top, tokens = routes_t.shape
    number = iota((experts, tokens), 0)
    hit = routes_t[0:1, :] == number
    for k in range(1, top):
        hit = hit | (routes_t[k : k + 1, :] == number)
    before = ones_where(iota((tokens, tokens), 0) < iota((tokens, tokens), 1))
    place = mm(ones_where(hit), before)
    return jnp.where(hit, place, -1.0)


def send_kernel(experts, capacity, routes_ref, rows_ref, out_ref):
    keys = slot_keys(routes_ref[...], experts)
    tokens = keys.shape[1]
    slot = iota((capacity, tokens), 0).astype(f32)
    chosen = [ones_where(slot == keys[e : e + 1, :]) for e in range(experts)]
    out_ref[...] = mm(jnp.concatenate(chosen, axis=0), rows_ref[...]).astype(bf16)


def share_kernel(experts, capacity, routes_ref, weight_ref, out_ref):
    routes_t = routes_ref[...]
    weight_t = weight_ref[...]
    keys = slot_keys(routes_t, experts)
    tokens = keys.shape[1]
    number = iota((experts, tokens), 0)
    share = jnp.zeros((experts, tokens), f32)
    for k in range(routes_t.shape[0]):
        share = share + jnp.where(routes_t[k : k + 1, :] == number, weight_t[k : k + 1, :], 0.0)
    slot = iota((capacity, tokens), 0).astype(f32)
    spread = [
        jnp.where(slot == keys[e : e + 1, :], share[e : e + 1, :], 0.0) for e in range(experts)
    ]
    same = ones_where(iota((tokens, tokens), 0) == iota((tokens, tokens), 1))
    for n, term in enumerate(split3(jnp.concatenate(spread, axis=0))):
        out_ref[n] = mm(same, term, NT).astype(bf16)


def combine_kernel(share_ref, back_ref, out_ref):
    back = back_ref[...]
    out = mm(share_ref[0], back) + (mm(share_ref[1], back) + mm(share_ref[2], back))
    out_ref[...] = out.astype(bf16)


def hidden_kernel(parts, blocks_of, me_ref, packed_ref, *refs):
    blocks = refs[:parts]
    gate_ref, up_ref, down_ref, hidden_ref, far_ref, normed_ref = refs[parts:]
    rows, feats = blocks[0].shape
    width = parts * feats
    chunk = 64
    step = pl.program_id(0)

    @pl.when(step == 0)
    def _():
        me = me_ref[0]
        lead = packed_ref.shape[1] - feats
        number = iota((parts, feats), 0)
        gains = [
            jnp.sum(jnp.where(number == me ^ k, packed_ref[:, lead:], 0.0), axis=0, keepdims=True)
            for k in range(parts)
        ]

        def body(step, unused):
            at = pl.ds(pl.multiple_of(step * chunk, chunk), chunk)
            total = jnp.zeros((chunk, 1), f32)
            square = jnp.zeros((chunk, 1), f32)
            for block in blocks:
                wide = block[at, :].astype(f32)
                total = total + jnp.sum(wide, axis=1, keepdims=True)
                square = square + jnp.sum(wide * wide, axis=1, keepdims=True)
            mean = total / width
            scale = lax.rsqrt(square / width - mean * mean + norm_eps)
            for k, block in enumerate(blocks):
                which = me ^ k
                value = (block[at, :].astype(f32) - mean) * scale * gains[k]
                cols = pl.ds(pl.multiple_of(which * feats, feats), feats)
                normed_ref[at, cols] = value.astype(bf16)
            return unused

        lax.fori_loop(0, rows // chunk, body, 0, unroll=2)

    @pl.when(step < blocks_of)
    def _():
        normed = normed_ref[...]
        gate = mm(normed, gate_ref[0])
        up = mm(normed, up_ref[0])
        size = gate_ref.shape[2]
        cols = pl.ds(pl.multiple_of(step * size, size), size)
        hidden_ref[:, cols] = (gate * jax.nn.sigmoid(gate) * up).astype(bf16)

    @pl.when(step >= blocks_of)
    def _():
        far_ref[0] = mm(hidden_ref[...], down_ref[0]).astype(bf16)


def down_kernel(me_ref, hidden_ref, weight_ref, out_ref):
    out_ref[0] = mm(hidden_ref[...], weight_ref[0]).astype(bf16)


def reorder(rows, back):
    steps = rows // LANES
    row, col = iota((rows, rows), 1 if back else 0), iota((rows, rows), 0 if back else 1)
    return ones_where(col == (row % LANES) * steps + row // LANES)


def sums_kernel(x_ref, gain_ref, out_ref):
    rows = x_ref[...]
    count = rows.shape[0]
    ones = jnp.ones((8, rows.shape[1]), bf16)
    wide = rows.astype(f32)
    high, low = split2(wide * wide)
    out_ref[:, :count] = mm(ones, rows, NT)[0:1]
    out_ref[:, count : 2 * count] = (mm(ones, high, NT) + mm(ones, low, NT))[0:1]
    out_ref[:, 2 * count :] = gain_ref[...]


def in_line(table, width):
    states = table.shape[1]
    wide = spread_table(table, states, 1, states, width)
    return jnp.sum(wide, axis=0, keepdims=True)


def sin_cos(angle):
    turns = jnp.floor(angle * 0.6366197723675814 + 0.5)
    rest = angle - turns * 1.5703125
    rest = rest - turns * 4.83751296997070312e-4
    rest = rest - turns * 7.54978995489188e-8
    z = rest * rest
    sine = rest + rest * z * (
        -1.6666654611e-1 + z * (8.3321608736e-3 + z * -1.9515295891e-4)
    )
    cosine = 1.0 - 0.5 * z + z * z * (
        4.166664568298827e-2 + z * (-1.388731625493765e-3 + z * 2.443315711809948e-5)
    )
    quarter = turns.astype(jnp.int32)
    odd = (quarter & 1) != 0
    first = jnp.where(odd, cosine, sine)
    second = jnp.where(odd, sine, cosine)
    first = jnp.where((quarter & 2) != 0, -first, first)
    second = jnp.where(((quarter + 1) & 2) != 0, -second, second)
    return first, second


def spread_table(table, inner, outer_rows, outer_cols, width):
    rows = table.shape[0]
    pick = ones_where(iota((inner, width), 1) % inner == iota((inner, width), 0))
    high, mid, low = split3(table)
    wide = mm(high, pick) + (mm(mid, pick) + mm(low, pick))
    same = iota((rows, width), 0) // outer_rows == iota((rows, width), 1) // outer_cols
    return jnp.where(same, wide, 0.0)


def scan_kernel(
    total, x_ref, packed_ref, gain_ref, step_ref, pr_ref, pi_ref, ir_ref, ii_ref,
    hr_ref, hi_ref, cr_ref, ci_ref, end_ref, ar_ref, ai_ref,
):
    rows, feats = x_ref.shape
    groups, states = pr_ref.shape
    flat = groups * states
    inner = feats // groups
    steps = rows // LANES
    order = reorder(rows, False)
    mean = jnp.sum(packed_ref[:, :rows], axis=0, keepdims=True) / total
    square = jnp.sum(packed_ref[:, rows : 2 * rows], axis=0, keepdims=True) / total
    scale = lax.rsqrt(square - mean * mean + norm_eps)
    match = iota((rows, rows), 1) == (iota((rows, rows), 0) % LANES) * steps + iota(
        (rows, rows), 0
    ) // LANES
    mean_col = jnp.sum(jnp.where(match, mean, 0.0), axis=1, keepdims=True)
    scale_col = jnp.sum(jnp.where(match, scale, 0.0), axis=1, keepdims=True)
    poles_re = in_line(pr_ref[...], flat)
    poles_im = in_line(pi_ref[...], flat)
    size = poles_re * poles_re + poles_im * poles_im
    over_re, over_im = poles_re / size, -poles_im / size
    d_high, d_mid, d_low = (
        mm(part, order, NT).astype(bf16) for part in split3(step_ref[...])
    )
    piece = min(flat, 256)
    for at in range(0, flat, piece):
        cols = pl.ds(at, piece)
        expand = ones_where(
            iota((groups, piece), 0) == (iota((groups, piece), 1) + at) // states
        )
        delta = mm(d_high, expand, TN) + (mm(d_mid, expand, TN) + mm(d_low, expand, TN))
        size = jnp.exp(poles_re[:, at : at + piece] * delta)
        sine, cosine = sin_cos(poles_im[:, at : at + piece] * delta)
        ar_ref[:, cols] = size * cosine
        ai_ref[:, cols] = size * sine
    cw = min(feats, 256)
    sw = cw // inner * states
    for b in range(feats // cw):
        chans = pl.ds(b * cw, cw)
        cols = pl.ds(b * sw, sw)
        rows_in = mm(order, x_ref[:, chans])
        normed = split2((rows_in - mean_col) * scale_col * gain_ref[:, chans])
        real = split2(spread_table(ir_ref[chans, :], states, inner, states, sw))
        imag = split2(spread_table(ii_ref[chans, :], states, inner, states, sw))
        hr_ref[:, cols], hi_ref[:, cols] = mul(
            mm3(normed, real, NN), mm3(normed, imag, NN),
            over_re[:, b * sw : b * sw + sw], over_im[:, b * sw : b * sw + sw],
        )
    span = min(flat, 512)
    for at in range(0, flat, span):
        cols = pl.ds(at, span)

        def body(j, carry):
            h_re, h_im, c_re, c_im = carry
            here = pl.ds(pl.multiple_of(j * LANES, LANES), LANES)
            a_re, a_im = ar_ref[here, cols], ai_ref[here, cols]
            d_re, d_im = hr_ref[here, cols], hi_ref[here, cols]
            h_re, h_im = mul(a_re, a_im, h_re + d_re, h_im + d_im)
            h_re, h_im = h_re - d_re, h_im - d_im
            c_re, c_im = mul(a_re, a_im, c_re, c_im)
            hr_ref[here, cols], hi_ref[here, cols] = h_re, h_im
            cr_ref[here, cols], ci_ref[here, cols] = c_re, c_im
            return h_re, h_im, c_re, c_im

        zero = jnp.zeros((LANES, span), f32)
        lax.fori_loop(0, steps, body, (zero, zero, zero + 1.0, zero))
    last = pl.ds(rows - LANES, LANES)
    h_re, h_im, c_re, c_im = hr_ref[last, :], hi_ref[last, :], cr_ref[last, :], ci_ref[last, :]
    p_re, p_im = c_re[0:1], c_im[0:1]
    s_re, s_im = h_re[0:1], h_im[0:1]
    for c in range(1, LANES):
        k_re, k_im = c_re[c : c + 1], c_im[c : c + 1]
        p_re, p_im = mul(k_re, k_im, p_re, p_im)
        s_re, s_im = mul(k_re, k_im, s_re, s_im)
        s_re, s_im = s_re + h_re[c : c + 1], s_im + h_im[c : c + 1]
    ends = jnp.concatenate([p_re, p_im, s_re, s_im], axis=0)
    for i in range(end_ref.shape[0]):
        end_ref[i] = ends


def read_kernel(
    me_ref, got_ref, hr_ref, hi_ref, cr_ref, ci_ref, rr_ref, ri_ref, out_ref,
):
    rows, flat = hr_ref.shape
    feats = out_ref.shape[1]
    states = rr_ref.shape[1]
    inner = feats // (flat // states)
    steps = rows // LANES
    me = me_ref[0]
    s_re = jnp.zeros((1, flat), f32)
    s_im = jnp.zeros((1, flat), f32)
    for i in range(got_ref.shape[0] - 1):
        ends = got_ref[i]
        n_re, n_im = mul(ends[0:1], ends[1:2], s_re, s_im)
        s_re = jnp.where(i < me, n_re + ends[2:3], s_re)
        s_im = jnp.where(i < me, n_im + ends[3:4], s_im)
    last = pl.ds(rows - LANES, LANES)
    h_re, h_im, c_re, c_im = hr_ref[last, :], hi_ref[last, :], cr_ref[last, :], ci_ref[last, :]
    in_re, in_im = [s_re], [s_im]
    for c in range(LANES - 1):
        n_re, n_im = mul(c_re[c : c + 1], c_im[c : c + 1], in_re[-1], in_im[-1])
        in_re.append(n_re + h_re[c : c + 1])
        in_im.append(n_im + h_im[c : c + 1])
    in_re = jnp.concatenate(in_re, axis=0)[None]
    in_im = jnp.concatenate(in_im, axis=0)[None]
    back = reorder(rows, True)
    cw = min(feats, 256)
    sw = cw // inner * states
    for b in range(feats // cw):
        chans = pl.ds(b * cw, cw)
        lo = b * sw
        cols = pl.ds(lo, sw)
        shape = (steps, LANES, sw)
        c_re, c_im = cr_ref[:, cols].reshape(shape), ci_ref[:, cols].reshape(shape)
        g_re, g_im = in_re[:, :, lo : lo + sw], in_im[:, :, lo : lo + sw]
        f_re = hr_ref[:, cols].reshape(shape) + (c_re * g_re - c_im * g_im)
        f_im = hi_ref[:, cols].reshape(shape) + (c_re * g_im + c_im * g_re)
        real = split2(spread_table(rr_ref[chans, :], states, inner, states, sw))
        imag = split2(spread_table(ri_ref[chans, :], states, inner, states, sw))
        response = mm3(split2(f_re.reshape(rows, sw)), real, NT) - mm3(
            split2(f_im.reshape(rows, sw)), imag, NT
        )
        cube = response + 0.044715 * (response * response * response)
        mixed = 0.5 * response * (1.0 + jnp.tanh(0.7978845608028654 * cube))
        out_ref[:, chans] = mm(back, mixed.astype(bf16)).astype(bf16)


def output_kernel(parts, me_ref, *refs):
    pieces = refs[:parts]
    value_ref, gate_ref, out_ref = refs[parts:]
    feats = pieces[0].shape[1]
    value = gate = None
    for k, piece in enumerate(pieces):
        at = pl.ds(pl.multiple_of((me_ref[0] ^ k) * feats, feats), feats)
        rows = piece[...]
        v, g = mm(rows, value_ref[at, :]), mm(rows, gate_ref[at, :])
        value, gate = (v, g) if value is None else (value + v, gate + g)
    out_ref[...] = (value * jax.nn.sigmoid(gate)).astype(bf16)


vmem = pl.BlockSpec(memory_space=pltpu.VMEM)
smem = pl.BlockSpec(memory_space=pltpu.SMEM)


def params(mib):
    return pltpu.CompilerParams(vmem_limit_bytes=mib << 20)


def swap(value, bit):
    count = lax.axis_size("tp")
    return lax.ppermute(value, "tp", [(i, i ^ bit) for i in range(count)])


def gather_tp(value):
    count = lax.axis_size("tp")
    blocks = {0: value}
    bit = count // 2
    while bit >= 1:
        blocks.update({k ^ bit: swap(block, bit) for k, block in list(blocks.items())})
        bit //= 2
    return [blocks[k] for k in range(count)]


def shards(
    mixer_input, mixer_gain, time_step, pole_real, pole_imag, input_real, input_imag,
    read_real, read_imag, out_value, out_gate, expert_input, expert_gain, routes,
    route_weight, expert_gate, expert_up, expert_down,
):
    n_tp, n_ep = lax.axis_size("tp"), lax.axis_size("ep")
    tp_at = lax.axis_index("tp").astype(jnp.int32).reshape(1)
    ep_at = lax.axis_index("ep").astype(jnp.int32).reshape(1)
    tokens, feats = expert_input.shape
    top = routes.shape[1]
    capacity = 2 * top * tokens // n_ep
    slots = n_ep * capacity
    routes_t = routes.T
    weight_t = route_weight.T

    send = pl.pallas_call(
        functools.partial(send_kernel, n_ep, capacity),
        out_shape=jax.ShapeDtypeStruct((slots, feats), bf16),
        in_specs=[vmem, vmem], out_specs=vmem, compiler_params=params(8), name="send_rows",
    )(routes_t, expert_input)
    arrived = lax.all_to_all(send, "ep", split_axis=0, concat_axis=0, tiled=True)

    rows, chans = mixer_input.shape
    mixer_input, send = lax.optimization_barrier((mixer_input, send))
    packed = pl.pallas_call(
        sums_kernel,
        out_shape=jax.ShapeDtypeStruct((1, 2 * rows + feats), f32),
        in_specs=[vmem, vmem], out_specs=vmem, compiler_params=params(8), name="mixer_sums",
    )(mixer_input, expert_gain.reshape(1, feats))
    packed = lax.all_gather(packed, "tp", axis=0, tiled=True)

    groups, states = pole_real.shape
    flat = groups * states
    big = jax.ShapeDtypeStruct((rows, flat), f32)
    h_re, h_im, c_re, c_im, ends = pl.pallas_call(
        functools.partial(scan_kernel, float(chans * n_tp)),
        out_shape=(big, big, big, big, jax.ShapeDtypeStruct((n_ep, 4, flat), f32)),
        in_specs=[vmem] * 8, out_specs=(vmem,) * 5,
        scratch_shapes=[pltpu.VMEM((rows, flat), f32)] * 2,
        compiler_params=params(28), name="mixer_scan",
    )(
        mixer_input, packed, mixer_gain.reshape(1, chans), time_step.T,
        pole_real, pole_imag,
        jnp.swapaxes(input_real, 1, 2).reshape(chans, states),
        jnp.swapaxes(input_imag, 1, 2).reshape(chans, states),
    )
    got = lax.all_to_all(ends, "ep", split_axis=0, concat_axis=0)

    blocks = gather_tp(arrived)
    share = pl.pallas_call(
        functools.partial(share_kernel, n_ep, capacity),
        out_shape=jax.ShapeDtypeStruct((3, tokens, slots), bf16),
        in_specs=[vmem, vmem], out_specs=vmem, compiler_params=params(8), name="route_share",
    )(routes_t, weight_t)
    units = expert_gate.shape[2]
    unit_block = min(units, 256)
    n_unit = units // unit_block
    n_far = n_tp // 2 - 1
    hidden, odd_far = pl.pallas_call(
        functools.partial(hidden_kernel, n_tp, n_unit),
        grid_spec=pltpu.PrefetchScalarGridSpec(
            num_scalar_prefetch=1,
            grid=(n_unit + n_far,),
            in_specs=[vmem] * (n_tp + 1) + [
                pl.BlockSpec(
                    (1, n_tp * feats, unit_block),
                    lambda j, me: (0, 0, jnp.minimum(j, n_unit - 1)),
                ),
                pl.BlockSpec(
                    (1, n_tp * feats, unit_block),
                    lambda j, me: (0, 0, jnp.minimum(j, n_unit - 1)),
                ),
                pl.BlockSpec(
                    (1, units, feats),
                    lambda j, me: (0, 0, me[0] ^ (2 * jnp.maximum(j - n_unit, 0) + 3)),
                ),
            ],
            out_specs=(
                pl.BlockSpec((slots, units), lambda j, me: (0, 0)),
                pl.BlockSpec(
                    (1, slots, feats), lambda j, me: (jnp.maximum(j - n_unit, 0), 0, 0)
                ),
            ),
            scratch_shapes=[pltpu.VMEM((slots, n_tp * feats), bf16)],
        ),
        out_shape=(
            jax.ShapeDtypeStruct((slots, units), bf16),
            jax.ShapeDtypeStruct((n_far, slots, feats), bf16),
        ),
        compiler_params=params(28), name="expert_hidden",
    )(tp_at, packed, *blocks, expert_gate, expert_up, expert_down)

    def down(count, offset):
        return pl.pallas_call(
            down_kernel,
            grid_spec=pltpu.PrefetchScalarGridSpec(
                num_scalar_prefetch=1,
                grid=(count,),
                in_specs=[
                    pl.BlockSpec((slots, units), lambda i, me: (0, 0)),
                    pl.BlockSpec((1, units, feats), lambda i, me: (0, 0, me[0] ^ offset(i))),
                ],
                out_specs=pl.BlockSpec((1, slots, feats), lambda i, me: (i, 0, 0)),
            ),
            out_shape=jax.ShapeDtypeStruct((count, slots, feats), bf16),
            compiler_params=params(10),
        )(tp_at, hidden, expert_down)

    theirs = swap(odd_far, 1)
    far = down(n_far, lambda i: 2 * i + 2).astype(f32) + theirs.astype(f32)
    parts = [swap(down(1, lambda i: i + 1)[0], 1), down(1, lambda i: i)[0]]
    bit = n_tp // 4
    while bit >= 1:
        come = swap(far[bit - 1 :].astype(bf16), 2 * bit).astype(f32)
        parts.append(come[0])
        far = far[: bit - 1] + come[1:]
        bit //= 2
    result = sum(part.astype(f32) for part in parts).astype(bf16)
    back = lax.all_to_all(result, "ep", split_axis=0, concat_axis=0, tiled=True)

    mixed = pl.pallas_call(
        read_kernel,
        out_shape=jax.ShapeDtypeStruct((rows, chans), bf16),
        in_specs=[smem] + [vmem] * 7, out_specs=vmem, compiler_params=params(28),
        name="mixer_read",
    )(
        ep_at, got, h_re, h_im, c_re, c_im,
        read_real.reshape(chans, states), read_imag.reshape(chans, states),
    )
    pieces = gather_tp(mixed)
    mixer_output = pl.pallas_call(
        functools.partial(output_kernel, n_tp),
        out_shape=jax.ShapeDtypeStruct((rows, out_value.shape[1]), bf16),
        in_specs=[smem] + [vmem] * (n_tp + 2), out_specs=vmem, compiler_params=params(20),
        name="mixer_out",
    )(tp_at, *pieces, out_value, out_gate)
    expert_output = pl.pallas_call(
        combine_kernel,
        out_shape=jax.ShapeDtypeStruct((tokens, feats), bf16),
        in_specs=[vmem] * 2, out_specs=vmem, compiler_params=params(8), name="combine",
    )(share, back)
    return mixer_output, expert_output


def solution(mesh):
    return jax.shard_map(
        shards,
        mesh=mesh,
        in_specs=(
            P("ep", "tp"), P("tp"), P("ep", "tp"), P("tp", None), P("tp", None),
            P("tp", None, None), P("tp", None, None), P("tp", None, None), P("tp", None, None),
            P(None, "tp"), P(None, "tp"), P("ep", "tp"), P("tp"), P("ep", None), P("ep", None),
            P("ep", None, "tp"), P("ep", None, "tp"), P("ep", "tp", None),
        ),
        out_specs=(P("ep", "tp"), P("ep", "tp")),
        check_vma=False,
    )
```

```python
import functools

import jax
import jax.numpy as jnp
from jax import lax
from jax.experimental import pallas as pl
from jax.experimental.pallas import tpu as pltpu
from jax.sharding import PartitionSpec as P


f32 = jnp.float32
bf16 = jnp.bfloat16
norm_eps = 1e-05
LANES = 8
NN = (((1,), (0,)), ((), ()))
NT = (((1,), (1,)), ((), ()))
TN = (((0,), (0,)), ((), ()))


def iota(shape, dim):
    return lax.broadcasted_iota(jnp.int32, shape, dim)


def ones_where(mask):
    return jnp.where(mask, 1.0, 0.0).astype(bf16)


def split2(value):
    high = value.astype(bf16)
    return high, (value - high.astype(f32)).astype(bf16)


def split3(value):
    high = value.astype(bf16)
    rest = value - high.astype(f32)
    mid = rest.astype(bf16)
    return high, mid, (rest - mid.astype(f32)).astype(bf16)


def mm(left, right, dims=NN):
    return lax.dot_general(left, right, dims, preferred_element_type=f32)


def mm3(left, right, dims):
    lh, ll = left
    rh, rl = right
    return mm(lh, rh, dims) + (mm(ll, rh, dims) + mm(lh, rl, dims))


def mul(ar, ai, br, bi):
    return ar * br - ai * bi, ar * bi + ai * br


def slot_keys(routes_t, experts):
    top, tokens = routes_t.shape
    number = iota((experts, tokens), 0)
    hit = routes_t[0:1, :] == number
    for k in range(1, top):
        hit = hit | (routes_t[k : k + 1, :] == number)
    before = ones_where(iota((tokens, tokens), 0) < iota((tokens, tokens), 1))
    place = mm(ones_where(hit), before)
    return jnp.where(hit, place, -1.0)


def send_kernel(experts, capacity, routes_ref, rows_ref, out_ref):
    keys = slot_keys(routes_ref[...], experts)
    tokens = keys.shape[1]
    slot = iota((capacity, tokens), 0).astype(f32)
    chosen = [ones_where(slot == keys[e : e + 1, :]) for e in range(experts)]
    out_ref[...] = mm(jnp.concatenate(chosen, axis=0), rows_ref[...]).astype(bf16)


def share_kernel(
    experts, capacity, routes_ref, weight_ref, value_ref, gate_ref,
    out_ref, value_out, gate_out, sems,
):
    copies = [
        pltpu.make_async_copy(value_ref, value_out, sems.at[0]),
        pltpu.make_async_copy(gate_ref, gate_out, sems.at[1]),
    ]
    for copy in copies:
        copy.start()
    routes_t = routes_ref[...]
    weight_t = weight_ref[...]
    keys = slot_keys(routes_t, experts)
    tokens = keys.shape[1]
    number = iota((experts, tokens), 0)
    share = jnp.zeros((experts, tokens), f32)
    for k in range(routes_t.shape[0]):
        share = share + jnp.where(routes_t[k : k + 1, :] == number, weight_t[k : k + 1, :], 0.0)
    slot = iota((capacity, tokens), 0).astype(f32)
    spread = [
        jnp.where(slot == keys[e : e + 1, :], share[e : e + 1, :], 0.0) for e in range(experts)
    ]
    same = ones_where(iota((tokens, tokens), 0) == iota((tokens, tokens), 1))
    for n, term in enumerate(split3(jnp.concatenate(spread, axis=0))):
        out_ref[n] = mm(same, term, NT).astype(bf16)
    for copy in copies:
        copy.wait()


def fetch_kernel(*refs):
    count = (len(refs) - 1) // 2
    sems = refs[-1]
    copies = [
        pltpu.make_async_copy(refs[n], refs[count + n], sems.at[n]) for n in range(count)
    ]
    for copy in copies:
        copy.start()
    for copy in copies:
        copy.wait()


def combine_kernel(share_ref, back_ref, out_ref):
    back = back_ref[...]
    out = mm(share_ref[0], back) + (mm(share_ref[1], back) + mm(share_ref[2], back))
    out_ref[...] = out.astype(bf16)


def hidden_kernel(parts, me_ref, packed_ref, *refs):
    blocks = refs[:parts]
    gate_ref, up_ref, down_ref, hidden_ref, far_ref, normed_ref = refs[parts:]
    rows, feats = blocks[0].shape
    width = parts * feats
    chunk = 64
    me = me_ref[0]
    lead = packed_ref.shape[1] - feats
    number = iota((parts, feats), 0)
    gains = [
        jnp.sum(jnp.where(number == me ^ k, packed_ref[:, lead:], 0.0), axis=0, keepdims=True)
        for k in range(parts)
    ]

    def body(step, unused):
        at = pl.ds(pl.multiple_of(step * chunk, chunk), chunk)
        total = jnp.zeros((chunk, 1), f32)
        square = jnp.zeros((chunk, 1), f32)
        for block in blocks:
            wide = block[at, :].astype(f32)
            total = total + jnp.sum(wide, axis=1, keepdims=True)
            square = square + jnp.sum(wide * wide, axis=1, keepdims=True)
        mean = total / width
        scale = lax.rsqrt(square / width - mean * mean + norm_eps)
        for k, block in enumerate(blocks):
            value = (block[at, :].astype(f32) - mean) * scale * gains[k]
            cols = pl.ds(pl.multiple_of((me ^ k) * feats, feats), feats)
            normed_ref[at, cols] = value.astype(bf16)
        return unused

    lax.fori_loop(0, rows // chunk, body, 0, unroll=2)
    units = gate_ref.shape[2]
    size = min(units, 256)
    for at in range(0, units, size):
        cols = pl.ds(at, size)
        normed = normed_ref[...]
        gate = mm(normed, gate_ref[0, :, cols])
        up = mm(normed, up_ref[0, :, cols])
        hidden_ref[:, cols] = (gate * jax.nn.sigmoid(gate) * up).astype(bf16)
    for n in range(far_ref.shape[0]):
        far_ref[n] = down_part(me ^ (2 * n + 3), hidden_ref, down_ref, feats)


def down_part(which, hidden_ref, weight_ref, feats):
    cols = pl.ds(pl.multiple_of(which * feats, feats), feats)
    return mm(hidden_ref[...], weight_ref[0, :, cols]).astype(bf16)


def down_kernel(offsets, me_ref, hidden_ref, weight_ref, out_ref):
    for n, offset in enumerate(offsets):
        out_ref[n] = down_part(
            me_ref[0] ^ offset, hidden_ref, weight_ref, out_ref.shape[2]
        )


def reorder(rows, back):
    steps = rows // LANES
    row, col = iota((rows, rows), 1 if back else 0), iota((rows, rows), 0 if back else 1)
    return ones_where(col == (row % LANES) * steps + row // LANES)


def sums_kernel(x_ref, gain_ref, out_ref):
    rows = x_ref[...]
    count = rows.shape[0]
    ones = jnp.ones((8, rows.shape[1]), bf16)
    wide = rows.astype(f32)
    high, low = split2(wide * wide)
    out_ref[:, :count] = mm(ones, rows, NT)[0:1]
    out_ref[:, count : 2 * count] = (mm(ones, high, NT) + mm(ones, low, NT))[0:1]
    out_ref[:, 2 * count :] = gain_ref[...]


def in_line(table, width):
    states = table.shape[1]
    wide = spread_table(table, states, 1, states, width)
    return jnp.sum(wide, axis=0, keepdims=True)


def sin_cos(angle):
    turns = jnp.floor(angle * 0.6366197723675814 + 0.5)
    rest = angle - turns * 1.5703125
    rest = rest - turns * 4.83751296997070312e-4
    rest = rest - turns * 7.54978995489188e-8
    z = rest * rest
    sine = rest + rest * z * (
        -1.6666654611e-1 + z * (8.3321608736e-3 + z * -1.9515295891e-4)
    )
    cosine = 1.0 - 0.5 * z + z * z * (
        4.166664568298827e-2 + z * (-1.388731625493765e-3 + z * 2.443315711809948e-5)
    )
    quarter = turns.astype(jnp.int32)
    odd = (quarter & 1) != 0
    first = jnp.where(odd, cosine, sine)
    second = jnp.where(odd, sine, cosine)
    first = jnp.where((quarter & 2) != 0, -first, first)
    second = jnp.where(((quarter + 1) & 2) != 0, -second, second)
    return first, second


def spread_table(table, inner, outer_rows, outer_cols, width):
    rows = table.shape[0]
    pick = ones_where(iota((inner, width), 1) % inner == iota((inner, width), 0))
    high, mid, low = split3(table)
    wide = mm(high, pick) + (mm(mid, pick) + mm(low, pick))
    same = iota((rows, width), 0) // outer_rows == iota((rows, width), 1) // outer_cols
    return jnp.where(same, wide, 0.0)


def scan_kernel(
    total, x_ref, packed_ref, gain_ref, step_ref, pr_ref, pi_ref, ir_ref, ii_ref,
    hr_ref, hi_ref, cr_ref, ci_ref, end_ref, ar_ref, ai_ref,
):
    rows, feats = x_ref.shape
    groups, states = pr_ref.shape
    flat = groups * states
    inner = feats // groups
    steps = rows // LANES
    order = reorder(rows, False)
    mean = jnp.sum(packed_ref[:, :rows], axis=0, keepdims=True) / total
    square = jnp.sum(packed_ref[:, rows : 2 * rows], axis=0, keepdims=True) / total
    scale = lax.rsqrt(square - mean * mean + norm_eps)
    match = iota((rows, rows), 1) == (iota((rows, rows), 0) % LANES) * steps + iota(
        (rows, rows), 0
    ) // LANES
    mean_col = jnp.sum(jnp.where(match, mean, 0.0), axis=1, keepdims=True)
    scale_col = jnp.sum(jnp.where(match, scale, 0.0), axis=1, keepdims=True)
    poles_re = in_line(pr_ref[...], flat)
    poles_im = in_line(pi_ref[...], flat)
    size = poles_re * poles_re + poles_im * poles_im
    over_re, over_im = poles_re / size, -poles_im / size
    d_high, d_mid, d_low = (
        mm(part, order, NT).astype(bf16) for part in split3(step_ref[...])
    )
    piece = min(flat, 256)
    for at in range(0, flat, piece):
        cols = pl.ds(at, piece)
        expand = ones_where(
            iota((groups, piece), 0) == (iota((groups, piece), 1) + at) // states
        )
        delta = mm(d_high, expand, TN) + (mm(d_mid, expand, TN) + mm(d_low, expand, TN))
        size = jnp.exp(poles_re[:, at : at + piece] * delta)
        sine, cosine = sin_cos(poles_im[:, at : at + piece] * delta)
        ar_ref[:, cols] = size * cosine
        ai_ref[:, cols] = size * sine
    cw = min(feats, 256)
    sw = cw // inner * states
    for b in range(feats // cw):
        chans = pl.ds(b * cw, cw)
        cols = pl.ds(b * sw, sw)
        rows_in = mm(order, x_ref[:, chans])
        normed = split2((rows_in - mean_col) * scale_col * gain_ref[:, chans])
        real = split2(spread_table(ir_ref[chans, :], states, inner, states, sw))
        imag = split2(spread_table(ii_ref[chans, :], states, inner, states, sw))
        hr_ref[:, cols], hi_ref[:, cols] = mul(
            mm3(normed, real, NN), mm3(normed, imag, NN),
            over_re[:, b * sw : b * sw + sw], over_im[:, b * sw : b * sw + sw],
        )
    span = min(flat, 512)
    for at in range(0, flat, span):
        cols = pl.ds(at, span)

        def body(j, carry):
            h_re, h_im, c_re, c_im = carry
            here = pl.ds(pl.multiple_of(j * LANES, LANES), LANES)
            a_re, a_im = ar_ref[here, cols], ai_ref[here, cols]
            d_re, d_im = hr_ref[here, cols], hi_ref[here, cols]
            h_re, h_im = mul(a_re, a_im, h_re + d_re, h_im + d_im)
            h_re, h_im = h_re - d_re, h_im - d_im
            c_re, c_im = mul(a_re, a_im, c_re, c_im)
            hr_ref[here, cols], hi_ref[here, cols] = h_re, h_im
            cr_ref[here, cols], ci_ref[here, cols] = c_re, c_im
            return h_re, h_im, c_re, c_im

        zero = jnp.zeros((LANES, span), f32)
        lax.fori_loop(0, steps, body, (zero, zero, zero + 1.0, zero))
    last = pl.ds(rows - LANES, LANES)
    h_re, h_im, c_re, c_im = hr_ref[last, :], hi_ref[last, :], cr_ref[last, :], ci_ref[last, :]
    p_re, p_im = c_re[0:1], c_im[0:1]
    s_re, s_im = h_re[0:1], h_im[0:1]
    for c in range(1, LANES):
        k_re, k_im = c_re[c : c + 1], c_im[c : c + 1]
        p_re, p_im = mul(k_re, k_im, p_re, p_im)
        s_re, s_im = mul(k_re, k_im, s_re, s_im)
        s_re, s_im = s_re + h_re[c : c + 1], s_im + h_im[c : c + 1]
    ends = jnp.concatenate([p_re, p_im, s_re, s_im], axis=0)
    for i in range(end_ref.shape[0]):
        end_ref[i] = ends


def read_kernel(
    me_ref, got_ref, hr_ref, hi_ref, cr_ref, ci_ref, rr_ref, ri_ref, out_ref,
):
    rows, flat = hr_ref.shape
    feats = out_ref.shape[1]
    states = rr_ref.shape[1]
    inner = feats // (flat // states)
    steps = rows // LANES
    me = me_ref[0]
    s_re = jnp.zeros((1, flat), f32)
    s_im = jnp.zeros((1, flat), f32)
    for i in range(got_ref.shape[0] - 1):
        ends = got_ref[i]
        n_re, n_im = mul(ends[0:1], ends[1:2], s_re, s_im)
        s_re = jnp.where(i < me, n_re + ends[2:3], s_re)
        s_im = jnp.where(i < me, n_im + ends[3:4], s_im)
    last = pl.ds(rows - LANES, LANES)
    h_re, h_im, c_re, c_im = hr_ref[last, :], hi_ref[last, :], cr_ref[last, :], ci_ref[last, :]
    in_re, in_im = [s_re], [s_im]
    for c in range(LANES - 1):
        n_re, n_im = mul(c_re[c : c + 1], c_im[c : c + 1], in_re[-1], in_im[-1])
        in_re.append(n_re + h_re[c : c + 1])
        in_im.append(n_im + h_im[c : c + 1])
    in_re = jnp.concatenate(in_re, axis=0)[None]
    in_im = jnp.concatenate(in_im, axis=0)[None]
    back = reorder(rows, True)
    cw = min(feats, 256)
    sw = cw // inner * states
    for b in range(feats // cw):
        chans = pl.ds(b * cw, cw)
        lo = b * sw
        cols = pl.ds(lo, sw)
        shape = (steps, LANES, sw)
        c_re, c_im = cr_ref[:, cols].reshape(shape), ci_ref[:, cols].reshape(shape)
        g_re, g_im = in_re[:, :, lo : lo + sw], in_im[:, :, lo : lo + sw]
        f_re = hr_ref[:, cols].reshape(shape) + (c_re * g_re - c_im * g_im)
        f_im = hi_ref[:, cols].reshape(shape) + (c_re * g_im + c_im * g_re)
        real = split2(spread_table(rr_ref[chans, :], states, inner, states, sw))
        imag = split2(spread_table(ri_ref[chans, :], states, inner, states, sw))
        response = mm3(split2(f_re.reshape(rows, sw)), real, NT) - mm3(
            split2(f_im.reshape(rows, sw)), imag, NT
        )
        cube = response + 0.044715 * (response * response * response)
        mixed = 0.5 * response * (1.0 + jnp.tanh(0.7978845608028654 * cube))
        out_ref[:, chans] = mm(back, mixed.astype(bf16)).astype(bf16)


def output_kernel(parts, me_ref, *refs):
    pieces = refs[:parts]
    value_ref, gate_ref, out_ref = refs[parts:]
    feats = pieces[0].shape[1]
    value = gate = None
    for k, piece in enumerate(pieces):
        at = pl.ds(pl.multiple_of((me_ref[0] ^ k) * feats, feats), feats)
        rows = piece[...]
        v, g = mm(rows, value_ref[at, :]), mm(rows, gate_ref[at, :])
        value, gate = (v, g) if value is None else (value + v, gate + g)
    out_ref[...] = (value * jax.nn.sigmoid(gate)).astype(bf16)


vmem = pl.BlockSpec(memory_space=pltpu.VMEM)
hbm = pl.BlockSpec(memory_space=pltpu.HBM)
smem = pl.BlockSpec(memory_space=pltpu.SMEM)


def stay(value):
    return pltpu.with_memory_space_constraint(value, pltpu.HBM)


def params(mib):
    return pltpu.CompilerParams(vmem_limit_bytes=mib << 20)


def swap(value, bit):
    count = lax.axis_size("tp")
    return lax.ppermute(value, "tp", [(i, i ^ bit) for i in range(count)])


def gather_tp(value):
    count = lax.axis_size("tp")
    blocks = {0: value}
    bit = count // 2
    while bit >= 1:
        blocks.update({k ^ bit: swap(block, bit) for k, block in list(blocks.items())})
        bit //= 2
    return [blocks[k] for k in range(count)]


def shards(
    mixer_input, mixer_gain, time_step, pole_real, pole_imag, input_real, input_imag,
    read_real, read_imag, out_value, out_gate, expert_input, expert_gain, routes,
    route_weight, expert_gate, expert_up, expert_down,
):
    n_tp, n_ep = lax.axis_size("tp"), lax.axis_size("ep")
    tp_at = lax.axis_index("tp").astype(jnp.int32).reshape(1)
    ep_at = lax.axis_index("ep").astype(jnp.int32).reshape(1)
    tokens, feats = expert_input.shape
    top = routes.shape[1]
    capacity = 2 * top * tokens // n_ep
    slots = n_ep * capacity
    routes_t = routes.T
    weight_t = route_weight.T

    send = pl.pallas_call(
        functools.partial(send_kernel, n_ep, capacity),
        out_shape=jax.ShapeDtypeStruct((slots, feats), bf16),
        in_specs=[vmem, vmem], out_specs=vmem, compiler_params=params(60), name="send_rows",
    )(routes_t, expert_input)
    arrived = lax.all_to_all(send, "ep", split_axis=0, concat_axis=0, tiled=True)

    rows, chans = mixer_input.shape
    mixer_input, send, tp_at, ep_at = lax.optimization_barrier(
        (mixer_input, send, tp_at, ep_at)
    )
    packed = pl.pallas_call(
        sums_kernel,
        out_shape=jax.ShapeDtypeStruct((1, 2 * rows + feats), f32),
        in_specs=[vmem, vmem], out_specs=vmem, compiler_params=params(60), name="mixer_sums",
    )(mixer_input, expert_gain.reshape(1, feats))
    packed = lax.all_gather(packed, "tp", axis=0, tiled=True)

    groups, states = pole_real.shape
    flat = groups * states
    big = jax.ShapeDtypeStruct((rows, flat), f32)
    h_re, h_im, c_re, c_im, ends = pl.pallas_call(
        functools.partial(scan_kernel, float(chans * n_tp)),
        out_shape=(big, big, big, big, jax.ShapeDtypeStruct((n_ep, 4, flat), f32)),
        in_specs=[vmem] * 8, out_specs=(vmem,) * 5,
        scratch_shapes=[pltpu.VMEM((rows, flat), f32)] * 2,
        compiler_params=params(60), name="mixer_scan",
    )(
        mixer_input, packed, mixer_gain.reshape(1, chans), time_step.T,
        pole_real, pole_imag,
        jnp.swapaxes(input_real, 1, 2).reshape(chans, states),
        jnp.swapaxes(input_imag, 1, 2).reshape(chans, states),
    )
    got = lax.all_to_all(ends, "ep", split_axis=0, concat_axis=0)

    blocks = gather_tp(arrived)
    weights = tuple(stay(w) for w in (expert_gate, expert_up, expert_down))
    gate_w, up_w, down_w = pl.pallas_call(
        fetch_kernel,
        out_shape=tuple(jax.ShapeDtypeStruct(w.shape, w.dtype) for w in weights),
        in_specs=[hbm] * 3, out_specs=(vmem,) * 3,
        scratch_shapes=[pltpu.SemaphoreType.DMA((3,))],
        compiler_params=params(16), name="expert_fetch",
    )(*weights)
    units = expert_gate.shape[2]
    n_far = n_tp // 2 - 1
    hidden, odd_far = pl.pallas_call(
        functools.partial(hidden_kernel, n_tp),
        in_specs=[smem] + [vmem] * (n_tp + 4), out_specs=(vmem, vmem),
        scratch_shapes=[pltpu.VMEM((slots, n_tp * feats), bf16)],
        out_shape=(
            jax.ShapeDtypeStruct((slots, units), bf16),
            jax.ShapeDtypeStruct((n_far, slots, feats), bf16),
        ),
        compiler_params=params(16), name="expert_hidden",
    )(tp_at, packed, *blocks, gate_w, up_w, down_w)

    def down(offsets):
        return pl.pallas_call(
            functools.partial(down_kernel, offsets),
            in_specs=[smem, vmem, vmem], out_specs=vmem,
            out_shape=jax.ShapeDtypeStruct((len(offsets), slots, feats), bf16),
            compiler_params=params(10),
        )(tp_at, hidden, down_w)

    theirs = swap(odd_far, 1)
    even_far = down(tuple(range(2, n_tp, 2)))
    far = even_far.astype(f32) + theirs.astype(f32)
    parts = [swap(down((1,))[0], 1), down((0,))[0]]
    bit = n_tp // 4
    while bit >= 1:
        come = swap(far[bit - 1 :].astype(bf16), 2 * bit).astype(f32)
        parts.append(come[0])
        far = far[: bit - 1] + come[1:]
        bit //= 2
    result = sum(part.astype(f32) for part in parts).astype(bf16)
    back = lax.all_to_all(result, "ep", split_axis=0, concat_axis=0, tiled=True)

    mixed = pl.pallas_call(
        read_kernel,
        out_shape=jax.ShapeDtypeStruct((rows, chans), bf16),
        in_specs=[smem] + [vmem] * 7, out_specs=vmem, compiler_params=params(60),
        name="mixer_read",
    )(
        ep_at, got, h_re, h_im, c_re, c_im,
        read_real.reshape(chans, states), read_imag.reshape(chans, states),
    )
    pieces = gather_tp(mixed)
    share, value_w, gate_w = pl.pallas_call(
        functools.partial(share_kernel, n_ep, capacity),
        out_shape=(
            jax.ShapeDtypeStruct((3, tokens, slots), bf16),
            jax.ShapeDtypeStruct(out_value.shape, bf16),
            jax.ShapeDtypeStruct(out_gate.shape, bf16),
        ),
        in_specs=[vmem, vmem, hbm, hbm], out_specs=(vmem,) * 3,
        scratch_shapes=[pltpu.SemaphoreType.DMA((2,))],
        compiler_params=params(10), name="out_fetch",
    )(routes_t, weight_t, stay(out_value), stay(out_gate))
    mixer_output = pl.pallas_call(
        functools.partial(output_kernel, n_tp),
        out_shape=jax.ShapeDtypeStruct((rows, out_value.shape[1]), bf16),
        in_specs=[smem] + [vmem] * (n_tp + 2), out_specs=vmem, compiler_params=params(10),
        name="mixer_out",
    )(tp_at, *pieces, value_w, gate_w)
    expert_output = pl.pallas_call(
        combine_kernel,
        out_shape=jax.ShapeDtypeStruct((tokens, feats), bf16),
        in_specs=[vmem] * 2, out_specs=vmem, compiler_params=params(8), name="combine",
    )(share, back)
    return mixer_output, expert_output


def solution(mesh):
    return jax.shard_map(
        shards,
        mesh=mesh,
        in_specs=(
            P("ep", "tp"), P("tp"), P("ep", "tp"), P("tp", None), P("tp", None),
            P("tp", None, None), P("tp", None, None), P("tp", None, None), P("tp", None, None),
            P(None, "tp"), P(None, "tp"), P("ep", "tp"), P("tp"), P("ep", None), P("ep", None),
            P("ep", None, "tp"), P("ep", None, "tp"), P("ep", "tp", None),
        ),
        out_specs=(P("ep", "tp"), P("ep", "tp")),
        check_vma=False,
    )
```

```python
import functools

import jax
import jax.numpy as jnp
from jax import lax
from jax.experimental import pallas as pl
from jax.experimental.pallas import tpu as pltpu
from jax.sharding import PartitionSpec as P


f32 = jnp.float32
bf16 = jnp.bfloat16
norm_eps = 1e-05
LANES = 8
NN = (((1,), (0,)), ((), ()))
NT = (((1,), (1,)), ((), ()))
TN = (((0,), (0,)), ((), ()))


def iota(shape, dim):
    return lax.broadcasted_iota(jnp.int32, shape, dim)


def ones_where(mask):
    return jnp.where(mask, 1.0, 0.0).astype(bf16)


def split2(value):
    high = value.astype(bf16)
    return high, (value - high.astype(f32)).astype(bf16)


def split3(value):
    high = value.astype(bf16)
    rest = value - high.astype(f32)
    mid = rest.astype(bf16)
    return high, mid, (rest - mid.astype(f32)).astype(bf16)


def mm(left, right, dims=NN):
    return lax.dot_general(left, right, dims, preferred_element_type=f32)


def mm3(left, right, dims):
    lh, ll = left
    rh, rl = right
    return mm(lh, rh, dims) + (mm(ll, rh, dims) + mm(lh, rl, dims))


def mul(ar, ai, br, bi):
    return ar * br - ai * bi, ar * bi + ai * br


def slot_keys(routes_t, experts):
    top, tokens = routes_t.shape
    number = iota((experts, tokens), 0)
    hit = routes_t[0:1, :] == number
    for k in range(1, top):
        hit = hit | (routes_t[k : k + 1, :] == number)
    before = ones_where(iota((tokens, tokens), 0) < iota((tokens, tokens), 1))
    place = mm(ones_where(hit), before)
    return jnp.where(hit, place, -1.0)


def send_kernel(experts, capacity, routes_ref, rows_ref, out_ref):
    keys = slot_keys(routes_ref[...], experts)
    tokens = keys.shape[1]
    slot = iota((capacity, tokens), 0).astype(f32)
    chosen = [ones_where(slot == keys[e : e + 1, :]) for e in range(experts)]
    out_ref[...] = mm(jnp.concatenate(chosen, axis=0), rows_ref[...]).astype(bf16)


def share_kernel(
    experts, capacity, routes_ref, weight_ref, value_ref, gate_ref,
    out_ref, value_out, gate_out, sems,
):
    copies = [
        pltpu.make_async_copy(value_ref, value_out, sems.at[0]),
        pltpu.make_async_copy(gate_ref, gate_out, sems.at[1]),
    ]
    for copy in copies:
        copy.start()
    routes_t = routes_ref[...]
    weight_t = weight_ref[...]
    keys = slot_keys(routes_t, experts)
    tokens = keys.shape[1]
    number = iota((experts, tokens), 0)
    share = jnp.zeros((experts, tokens), f32)
    for k in range(routes_t.shape[0]):
        share = share + jnp.where(routes_t[k : k + 1, :] == number, weight_t[k : k + 1, :], 0.0)
    slot = iota((capacity, tokens), 0).astype(f32)
    spread = [
        jnp.where(slot == keys[e : e + 1, :], share[e : e + 1, :], 0.0) for e in range(experts)
    ]
    same = ones_where(iota((tokens, tokens), 0) == iota((tokens, tokens), 1))
    for n, term in enumerate(split3(jnp.concatenate(spread, axis=0))):
        out_ref[n] = mm(same, term, NT).astype(bf16)
    for copy in copies:
        copy.wait()


def combine_kernel(share_ref, back_ref, out_ref):
    back = back_ref[...]
    out = mm(share_ref[0], back) + (mm(share_ref[1], back) + mm(share_ref[2], back))
    out_ref[...] = out.astype(bf16)


def row_gain(packed_ref, which, lead):
    gain = jnp.zeros_like(packed_ref[0][:, lead:])
    for q in range(packed_ref.shape[0]):
        gain = jnp.where(which == q, packed_ref[q][:, lead:], gain)
    return gain


def hidden_kernel(parts, senders, start, me_ref, packed_ref, *refs):
    blocks = refs[:parts]
    gate_hbm, up_hbm, down_hbm, hidden_ref, odd_ref, even_ref = refs[parts : parts + 6]
    normed_ref, gate_ref, up_ref, down_ref, unit_sems, down_sems = refs[parts + 6 :]
    rows = hidden_ref.shape[0]
    full, feats = blocks[0].shape
    width = parts * feats
    chunk = rows // senders
    me = me_ref[0]
    units = gate_ref.shape[1]
    size = units // unit_sems.shape[1]
    loads = []
    for n in range(unit_sems.shape[1]):
        cols = pl.ds(n * size, size)
        loads.append([
            pltpu.make_async_copy(hbm.at[0, :, cols], ref.at[:, cols], unit_sems.at[m, n])
            for m, (hbm, ref) in enumerate(((gate_hbm, gate_ref), (up_hbm, up_ref)))
        ])
    downs = []
    for n in range(down_ref.shape[0]):
        which = me ^ (n + 2)
        cols = pl.ds(pl.multiple_of(which * feats, feats), feats)
        downs.append(
            pltpu.make_async_copy(down_hbm.at[0, :, cols], down_ref.at[n], down_sems.at[n])
        )
    for pair in loads:
        for copy in pair:
            copy.start()
    for copy in downs:
        copy.start()
    gains = [row_gain(packed_ref, me ^ k, packed_ref.shape[2] - feats) for k in range(parts)]

    def body(sender, unused):
        here = pl.ds(pl.multiple_of(sender * chunk, chunk), chunk)
        there = pl.ds(pl.multiple_of(sender * (full // senders) + start, chunk), chunk)
        at = [there if k < 2 else here for k in range(parts)]
        total = jnp.zeros((chunk, 1), f32)
        square = jnp.zeros((chunk, 1), f32)
        for k, block in enumerate(blocks):
            wide = block[at[k], :].astype(f32)
            total = total + jnp.sum(wide, axis=1, keepdims=True)
            square = square + jnp.sum(wide * wide, axis=1, keepdims=True)
        mean = total / width
        scale = lax.rsqrt(square / width - mean * mean + norm_eps)
        for k, block in enumerate(blocks):
            value = (block[at[k], :].astype(f32) - mean) * scale * gains[k]
            cols = pl.ds(pl.multiple_of((me ^ k) * feats, feats), feats)
            normed_ref[here, cols] = value.astype(bf16)
        return unused

    lax.fori_loop(0, senders, body, 0, unroll=2)
    for n, pair in enumerate(loads):
        cols = pl.ds(n * size, size)
        for copy in pair:
            copy.wait()
        normed = normed_ref[...]
        gate = mm(normed, gate_ref[:, cols])
        up = mm(normed, up_ref[:, cols])
        hidden_ref[:, cols] = (gate * jax.nn.sigmoid(gate) * up).astype(bf16)
    order = [*range(1, len(downs), 2), *range(0, len(downs), 2)]
    for copy in downs:
        copy.wait()
    for n in order:
        out = odd_ref if n % 2 else even_ref
        out[n // 2] = mm(hidden_ref[...], down_ref[n]).astype(bf16)


def near_kernel(count, me_ref, *refs):
    hiddens = refs[:count]
    down_hbm, near_ref, *owns = refs[count : 2 * count + 2]
    down_ref, sems = refs[2 * count + 2 :]
    feats = near_ref.shape[1]
    copies = []
    for n in range(2):
        cols = pl.ds(pl.multiple_of((me_ref[0] ^ n) * feats, feats), feats)
        copies.append(
            pltpu.make_async_copy(down_hbm.at[0, :, cols], down_ref.at[n], sems.at[n])
        )
    for copy in copies:
        copy.start()
    for copy in copies:
        copy.wait()
    rows = near_ref.shape[0] // count
    for c, hidden in enumerate(hiddens):
        near_ref[pl.ds(c * rows, rows), :] = mm(hidden[...], down_ref[1]).astype(bf16)
    for own, hidden in zip(owns, hiddens):
        own[...] = mm(hidden[...], down_ref[0]).astype(bf16)


def join_kernel(count, senders, near_ref, *refs):
    out_ref = refs[-1]
    terms = (len(refs) - 1) // count
    part = near_ref.shape[0] // count
    chunk = part // senders
    for c in range(count):
        for e in range(senders):
            total = near_ref[pl.ds(c * part + e * chunk, chunk), :].astype(f32)
            for ref in refs[c * terms : (c + 1) * terms]:
                total = total + ref[pl.ds(e * chunk, chunk), :].astype(f32)
            out_ref[pl.ds((e * count + c) * chunk, chunk), :] = total.astype(bf16)


def reorder(rows, back):
    steps = rows // LANES
    row, col = iota((rows, rows), 1 if back else 0), iota((rows, rows), 0 if back else 1)
    return ones_where(col == (row % LANES) * steps + row // LANES)


def sums_kernel(x_ref, gain_ref, out_ref):
    rows = x_ref[...]
    count = rows.shape[0]
    ones = jnp.ones((8, rows.shape[1]), bf16)
    wide = rows.astype(f32)
    high, low = split2(wide * wide)
    out_ref[:, :count] = mm(ones, rows, NT)[0:1]
    out_ref[:, count : 2 * count] = (mm(ones, high, NT) + mm(ones, low, NT))[0:1]
    out_ref[:, 2 * count :] = gain_ref[...]


def in_line(table, width):
    states = table.shape[1]
    wide = spread_table(table, states, 1, states, width)
    return jnp.sum(wide, axis=0, keepdims=True)


def sin_cos(angle):
    turns = jnp.floor(angle * 0.6366197723675814 + 0.5)
    rest = angle - turns * 1.5703125
    rest = rest - turns * 4.83751296997070312e-4
    rest = rest - turns * 7.54978995489188e-8
    z = rest * rest
    sine = rest + rest * z * (
        -1.6666654611e-1 + z * (8.3321608736e-3 + z * -1.9515295891e-4)
    )
    cosine = 1.0 - 0.5 * z + z * z * (
        4.166664568298827e-2 + z * (-1.388731625493765e-3 + z * 2.443315711809948e-5)
    )
    quarter = turns.astype(jnp.int32)
    odd = (quarter & 1) != 0
    first = jnp.where(odd, cosine, sine)
    second = jnp.where(odd, sine, cosine)
    first = jnp.where((quarter & 2) != 0, -first, first)
    second = jnp.where(((quarter + 1) & 2) != 0, -second, second)
    return first, second


def spread_table(table, inner, outer_rows, outer_cols, width):
    rows = table.shape[0]
    pick = ones_where(iota((inner, width), 1) % inner == iota((inner, width), 0))
    high, mid, low = split3(table)
    wide = mm(high, pick) + (mm(mid, pick) + mm(low, pick))
    same = iota((rows, width), 0) // outer_rows == iota((rows, width), 1) // outer_cols
    return jnp.where(same, wide, 0.0)


def scan_kernel(
    total, x_ref, packed_ref, gain_ref, step_ref, pr_ref, pi_ref, ir_ref, ii_ref,
    hr_ref, hi_ref, cr_ref, ci_ref, end_ref, ar_ref, ai_ref,
):
    rows, feats = x_ref.shape
    groups, states = pr_ref.shape
    flat = groups * states
    inner = feats // groups
    steps = rows // LANES
    order = reorder(rows, False)
    packed = packed_ref[0]
    for q in range(1, packed_ref.shape[0]):
        packed = packed + packed_ref[q]
    mean = packed[:, :rows] / total
    square = packed[:, rows : 2 * rows] / total
    scale = lax.rsqrt(square - mean * mean + norm_eps)
    match = iota((rows, rows), 1) == (iota((rows, rows), 0) % LANES) * steps + iota(
        (rows, rows), 0
    ) // LANES
    mean_col = jnp.sum(jnp.where(match, mean, 0.0), axis=1, keepdims=True)
    scale_col = jnp.sum(jnp.where(match, scale, 0.0), axis=1, keepdims=True)
    poles_re = in_line(pr_ref[...], flat)
    poles_im = in_line(pi_ref[...], flat)
    size = poles_re * poles_re + poles_im * poles_im
    over_re, over_im = poles_re / size, -poles_im / size
    d_high, d_mid, d_low = (
        mm(part, order, NT).astype(bf16) for part in split3(step_ref[...])
    )
    piece = min(flat, 256)
    for at in range(0, flat, piece):
        cols = pl.ds(at, piece)
        expand = ones_where(
            iota((groups, piece), 0) == (iota((groups, piece), 1) + at) // states
        )
        delta = mm(d_high, expand, TN) + (mm(d_mid, expand, TN) + mm(d_low, expand, TN))
        size = jnp.exp(poles_re[:, at : at + piece] * delta)
        sine, cosine = sin_cos(poles_im[:, at : at + piece] * delta)
        ar_ref[:, cols] = size * cosine
        ai_ref[:, cols] = size * sine
    cw = min(feats, 256)
    sw = cw // inner * states
    for b in range(feats // cw):
        chans = pl.ds(b * cw, cw)
        cols = pl.ds(b * sw, sw)
        rows_in = mm(order, x_ref[:, chans])
        normed = split2((rows_in - mean_col) * scale_col * gain_ref[:, chans])
        real = split2(spread_table(ir_ref[chans, :], states, inner, states, sw))
        imag = split2(spread_table(ii_ref[chans, :], states, inner, states, sw))
        hr_ref[:, cols], hi_ref[:, cols] = mul(
            mm3(normed, real, NN), mm3(normed, imag, NN),
            over_re[:, b * sw : b * sw + sw], over_im[:, b * sw : b * sw + sw],
        )
    span = min(flat, 512)
    for at in range(0, flat, span):
        cols = pl.ds(at, span)

        def body(j, carry):
            h_re, h_im, c_re, c_im = carry
            here = pl.ds(pl.multiple_of(j * LANES, LANES), LANES)
            a_re, a_im = ar_ref[here, cols], ai_ref[here, cols]
            d_re, d_im = hr_ref[here, cols], hi_ref[here, cols]
            h_re, h_im = mul(a_re, a_im, h_re + d_re, h_im + d_im)
            h_re, h_im = h_re - d_re, h_im - d_im
            c_re, c_im = mul(a_re, a_im, c_re, c_im)
            hr_ref[here, cols], hi_ref[here, cols] = h_re, h_im
            cr_ref[here, cols], ci_ref[here, cols] = c_re, c_im
            return h_re, h_im, c_re, c_im

        zero = jnp.zeros((LANES, span), f32)
        lax.fori_loop(0, steps, body, (zero, zero, zero + 1.0, zero))
    last = pl.ds(rows - LANES, LANES)
    h_re, h_im, c_re, c_im = hr_ref[last, :], hi_ref[last, :], cr_ref[last, :], ci_ref[last, :]
    p_re, p_im = c_re[0:1], c_im[0:1]
    s_re, s_im = h_re[0:1], h_im[0:1]
    for c in range(1, LANES):
        k_re, k_im = c_re[c : c + 1], c_im[c : c + 1]
        p_re, p_im = mul(k_re, k_im, p_re, p_im)
        s_re, s_im = mul(k_re, k_im, s_re, s_im)
        s_re, s_im = s_re + h_re[c : c + 1], s_im + h_im[c : c + 1]
    ends = jnp.concatenate([p_re, p_im, s_re, s_im], axis=0)
    for i in range(end_ref.shape[0]):
        end_ref[i] = ends


def read_kernel(
    me_ref, got_ref, hr_ref, hi_ref, cr_ref, ci_ref, rr_ref, ri_ref, out_ref,
):
    rows, flat = hr_ref.shape
    feats = out_ref.shape[1]
    states = rr_ref.shape[1]
    inner = feats // (flat // states)
    steps = rows // LANES
    me = me_ref[0]
    s_re = jnp.zeros((1, flat), f32)
    s_im = jnp.zeros((1, flat), f32)
    for i in range(got_ref.shape[0] - 1):
        ends = got_ref[i]
        n_re, n_im = mul(ends[0:1], ends[1:2], s_re, s_im)
        s_re = jnp.where(i < me, n_re + ends[2:3], s_re)
        s_im = jnp.where(i < me, n_im + ends[3:4], s_im)
    last = pl.ds(rows - LANES, LANES)
    h_re, h_im, c_re, c_im = hr_ref[last, :], hi_ref[last, :], cr_ref[last, :], ci_ref[last, :]
    in_re, in_im = [s_re], [s_im]
    for c in range(LANES - 1):
        n_re, n_im = mul(c_re[c : c + 1], c_im[c : c + 1], in_re[-1], in_im[-1])
        in_re.append(n_re + h_re[c : c + 1])
        in_im.append(n_im + h_im[c : c + 1])
    in_re = jnp.concatenate(in_re, axis=0)[None]
    in_im = jnp.concatenate(in_im, axis=0)[None]
    back = reorder(rows, True)
    cw = min(feats, 256)
    sw = cw // inner * states
    for b in range(feats // cw):
        chans = pl.ds(b * cw, cw)
        lo = b * sw
        cols = pl.ds(lo, sw)
        shape = (steps, LANES, sw)
        c_re, c_im = cr_ref[:, cols].reshape(shape), ci_ref[:, cols].reshape(shape)
        g_re, g_im = in_re[:, :, lo : lo + sw], in_im[:, :, lo : lo + sw]
        f_re = hr_ref[:, cols].reshape(shape) + (c_re * g_re - c_im * g_im)
        f_im = hi_ref[:, cols].reshape(shape) + (c_re * g_im + c_im * g_re)
        real = split2(spread_table(rr_ref[chans, :], states, inner, states, sw))
        imag = split2(spread_table(ri_ref[chans, :], states, inner, states, sw))
        response = mm3(split2(f_re.reshape(rows, sw)), real, NT) - mm3(
            split2(f_im.reshape(rows, sw)), imag, NT
        )
        cube = response + 0.044715 * (response * response * response)
        mixed = 0.5 * response * (1.0 + jnp.tanh(0.7978845608028654 * cube))
        out_ref[:, chans] = mm(back, mixed.astype(bf16)).astype(bf16)


def output_kernel(parts, me_ref, *refs):
    pieces = refs[:parts]
    value_ref, gate_ref, out_ref = refs[parts:]
    feats = pieces[0].shape[1]
    value = gate = None
    for k, piece in enumerate(pieces):
        at = pl.ds(pl.multiple_of((me_ref[0] ^ k) * feats, feats), feats)
        rows = piece[...]
        v, g = mm(rows, value_ref[at, :]), mm(rows, gate_ref[at, :])
        value, gate = (v, g) if value is None else (value + v, gate + g)
    out_ref[...] = (value * jax.nn.sigmoid(gate)).astype(bf16)


vmem = pl.BlockSpec(memory_space=pltpu.VMEM)
hbm = pl.BlockSpec(memory_space=pltpu.HBM)
smem = pl.BlockSpec(memory_space=pltpu.SMEM)


def stay(value):
    return pltpu.with_memory_space_constraint(value, pltpu.HBM)


def params(mib):
    return pltpu.CompilerParams(vmem_limit_bytes=mib << 20)


def swap(value, bit):
    count = lax.axis_size("tp")
    return lax.ppermute(value, "tp", [(i, i ^ bit) for i in range(count)])


def gather_tp(value):
    count = lax.axis_size("tp")
    blocks = {0: value}
    bit = count // 2
    while bit >= 1:
        blocks.update({k ^ bit: swap(block, bit) for k, block in list(blocks.items())})
        bit //= 2
    return [blocks[k] for k in range(count)]


def shards(
    mixer_input, mixer_gain, time_step, pole_real, pole_imag, input_real, input_imag,
    read_real, read_imag, out_value, out_gate, expert_input, expert_gain, routes,
    route_weight, expert_gate, expert_up, expert_down,
):
    n_tp, n_ep = lax.axis_size("tp"), lax.axis_size("ep")
    tp_at = lax.axis_index("tp").astype(jnp.int32).reshape(1)
    ep_at = lax.axis_index("ep").astype(jnp.int32).reshape(1)
    tokens, feats = expert_input.shape
    top = routes.shape[1]
    capacity = 2 * top * tokens // n_ep
    slots = n_ep * capacity
    routes_t = routes.T
    weight_t = route_weight.T

    send = pl.pallas_call(
        functools.partial(send_kernel, n_ep, capacity),
        out_shape=jax.ShapeDtypeStruct((slots, feats), bf16),
        in_specs=[vmem, vmem], out_specs=vmem, compiler_params=params(60), name="send_rows",
    )(routes_t, expert_input)
    arrived = lax.all_to_all(send, "ep", split_axis=0, concat_axis=0, tiled=True)

    rows, chans = mixer_input.shape
    mixer_input, send, tp_at, ep_at = lax.optimization_barrier(
        (mixer_input, send, tp_at, ep_at)
    )
    packed = pl.pallas_call(
        sums_kernel,
        out_shape=jax.ShapeDtypeStruct((1, 2 * rows + feats), f32),
        in_specs=[vmem, vmem], out_specs=vmem, compiler_params=params(60), name="mixer_sums",
    )(mixer_input, expert_gain.reshape(1, feats))
    packed = lax.all_gather(packed, "tp")

    groups, states = pole_real.shape
    flat = groups * states
    big = jax.ShapeDtypeStruct((rows, flat), f32)
    h_re, h_im, c_re, c_im, ends = pl.pallas_call(
        functools.partial(scan_kernel, float(chans * n_tp)),
        out_shape=(big, big, big, big, jax.ShapeDtypeStruct((n_ep, 4, flat), f32)),
        in_specs=[vmem] * 8, out_specs=(vmem,) * 5,
        scratch_shapes=[pltpu.VMEM((rows, flat), f32)] * 2,
        compiler_params=params(60), name="mixer_scan",
    )(
        mixer_input, packed, mixer_gain.reshape(1, chans), time_step.T,
        pole_real, pole_imag,
        jnp.swapaxes(input_real, 1, 2).reshape(chans, states),
        jnp.swapaxes(input_imag, 1, 2).reshape(chans, states),
    )
    got = lax.all_to_all(ends, "ep", split_axis=0, concat_axis=0)

    units = expert_gate.shape[2]
    n_far = n_tp // 2 - 1
    n_half = 2 if capacity % 32 == 0 else 1
    half = capacity // n_half
    part = n_ep * half
    by_sender = arrived.reshape(n_ep, capacity, feats)
    halves = [by_sender[:, c * half : (c + 1) * half].reshape(part, feats) for c in range(n_half)]
    far_blocks = []
    for c in range(n_half):
        evens = {0: halves[c]}
        bit = n_tp // 2
        while bit > 1:
            evens.update({k ^ bit: swap(b, bit) for k, b in list(evens.items())})
            bit //= 2
        far_blocks.append(evens)
    partner = swap(arrived, 1)
    weights = [stay(w) for w in (expert_gate, expert_up, expert_down)]
    n_unit = max(1, units // 256)
    hiddens, sums = [], []
    for c in range(n_half):
        blocks = [arrived, partner]
        for k in range(2, n_tp, 2):
            blocks += [far_blocks[c][k], swap(far_blocks[c][k], 1)]
        far_shape = jax.ShapeDtypeStruct((n_far, part, feats), bf16)
        hidden, odd_far, even_far = pl.pallas_call(
            functools.partial(hidden_kernel, n_tp, n_ep, c * half),
            in_specs=[smem] + [vmem] * (n_tp + 1) + [hbm] * 3, out_specs=(vmem,) * 3,
            scratch_shapes=[
                pltpu.VMEM((part, n_tp * feats), bf16),
                pltpu.VMEM((n_tp * feats, units), bf16),
                pltpu.VMEM((n_tp * feats, units), bf16),
                pltpu.VMEM((2 * n_far, units, feats), bf16),
                pltpu.SemaphoreType.DMA((2, n_unit)),
                pltpu.SemaphoreType.DMA((2 * n_far,)),
            ],
            out_shape=(jax.ShapeDtypeStruct((part, units), bf16), far_shape, far_shape),
            compiler_params=params(20),
        )(tp_at, packed, *blocks, *weights)
        hiddens.append(hidden)
        theirs = swap(odd_far, 1)
        far = even_far.astype(f32) + theirs.astype(f32)
        come = []
        bit = n_tp // 4
        while bit >= 1:
            got_far = swap(far[bit - 1 :].astype(bf16), 2 * bit)
            come.append(got_far[0])
            far = far[: bit - 1] + got_far[1:].astype(f32)
            bit //= 2
        sums.append(come)
    near, *owns = pl.pallas_call(
        functools.partial(near_kernel, n_half),
        in_specs=[smem] + [vmem] * n_half + [hbm], out_specs=(vmem,) * (n_half + 1),
        out_shape=(jax.ShapeDtypeStruct((slots, feats), bf16),)
        + (jax.ShapeDtypeStruct((part, feats), bf16),) * n_half,
        scratch_shapes=[
            pltpu.VMEM((2, units, feats), bf16), pltpu.SemaphoreType.DMA((2,)),
        ],
        compiler_params=params(10), name="expert_near",
    )(tp_at, *hiddens, weights[2])
    near = swap(near, 1)
    terms = [term for own, come in zip(owns, sums) for term in (own, *come)]
    result = pl.pallas_call(
        functools.partial(join_kernel, n_half, n_ep),
        out_shape=jax.ShapeDtypeStruct((slots, feats), bf16),
        in_specs=[vmem] * (len(terms) + 1), out_specs=vmem, compiler_params=params(8),
        name="expert_join",
    )(near, *terms)
    back = lax.all_to_all(result, "ep", split_axis=0, concat_axis=0, tiled=True)

    mixed = pl.pallas_call(
        read_kernel,
        out_shape=jax.ShapeDtypeStruct((rows, chans), bf16),
        in_specs=[smem] + [vmem] * 7, out_specs=vmem, compiler_params=params(60),
        name="mixer_read",
    )(
        ep_at, got, h_re, h_im, c_re, c_im,
        read_real.reshape(chans, states), read_imag.reshape(chans, states),
    )
    pieces = gather_tp(mixed)
    share, value_w, gate_w = pl.pallas_call(
        functools.partial(share_kernel, n_ep, capacity),
        out_shape=(
            jax.ShapeDtypeStruct((3, tokens, slots), bf16),
            jax.ShapeDtypeStruct(out_value.shape, bf16),
            jax.ShapeDtypeStruct(out_gate.shape, bf16),
        ),
        in_specs=[vmem, vmem, hbm, hbm], out_specs=(vmem,) * 3,
        scratch_shapes=[pltpu.SemaphoreType.DMA((2,))],
        compiler_params=params(10), name="out_fetch",
    )(routes_t, weight_t, stay(out_value), stay(out_gate))
    mixer_output = pl.pallas_call(
        functools.partial(output_kernel, n_tp),
        out_shape=jax.ShapeDtypeStruct((rows, out_value.shape[1]), bf16),
        in_specs=[smem] + [vmem] * (n_tp + 2), out_specs=vmem, compiler_params=params(10),
        name="mixer_out",
    )(tp_at, *pieces, value_w, gate_w)
    expert_output = pl.pallas_call(
        combine_kernel,
        out_shape=jax.ShapeDtypeStruct((tokens, feats), bf16),
        in_specs=[vmem] * 2, out_specs=vmem, compiler_params=params(8), name="combine",
    )(share, back)
    return mixer_output, expert_output


def solution(mesh):
    return jax.shard_map(
        shards,
        mesh=mesh,
        in_specs=(
            P("ep", "tp"), P("tp"), P("ep", "tp"), P("tp", None), P("tp", None),
            P("tp", None, None), P("tp", None, None), P("tp", None, None), P("tp", None, None),
            P(None, "tp"), P(None, "tp"), P("ep", "tp"), P("tp"), P("ep", None), P("ep", None),
            P("ep", None, "tp"), P("ep", None, "tp"), P("ep", "tp", None),
        ),
        out_specs=(P("ep", "tp"), P("ep", "tp")),
        check_vma=False,
    )
```

```python
import functools

import jax
import jax.numpy as jnp
from jax import lax
from jax.experimental import pallas as pl
from jax.experimental.pallas import tpu as pltpu
from jax.sharding import PartitionSpec as P


f32 = jnp.float32
bf16 = jnp.bfloat16
norm_eps = 1e-05
LANES = 8
NN = (((1,), (0,)), ((), ()))
NT = (((1,), (1,)), ((), ()))
TN = (((0,), (0,)), ((), ()))


def iota(shape, dim):
    return lax.broadcasted_iota(jnp.int32, shape, dim)


def ones_where(mask):
    return jnp.where(mask, 1.0, 0.0).astype(bf16)


def split2(value):
    high = value.astype(bf16)
    return high, (value - high.astype(f32)).astype(bf16)


def split3(value):
    high = value.astype(bf16)
    rest = value - high.astype(f32)
    mid = rest.astype(bf16)
    return high, mid, (rest - mid.astype(f32)).astype(bf16)


def mm(left, right, dims=NN):
    return lax.dot_general(left, right, dims, preferred_element_type=f32)


def mm3(left, right, dims):
    lh, ll = left
    rh, rl = right
    return mm(lh, rh, dims) + (mm(ll, rh, dims) + mm(lh, rl, dims))


def mul(ar, ai, br, bi):
    return ar * br - ai * bi, ar * bi + ai * br


def slot_keys(routes_t, experts):
    top, tokens = routes_t.shape
    number = iota((experts, tokens), 0)
    hit = routes_t[0:1, :] == number
    for k in range(1, top):
        hit = hit | (routes_t[k : k + 1, :] == number)
    before = ones_where(iota((tokens, tokens), 0) < iota((tokens, tokens), 1))
    place = mm(ones_where(hit), before)
    return jnp.where(hit, place, -1.0)


def send_kernel(experts, capacity, routes_ref, rows_ref, x_ref, gain_ref, out_ref, sums_ref):
    keys = slot_keys(routes_ref[...], experts)
    tokens = keys.shape[1]
    slot = iota((capacity, tokens), 0).astype(f32)
    chosen = [ones_where(slot == keys[e : e + 1, :]) for e in range(experts)]
    out_ref[...] = mm(jnp.concatenate(chosen, axis=0), rows_ref[...]).astype(bf16)
    rows = x_ref[...]
    count = rows.shape[0]
    ones = jnp.ones((8, rows.shape[1]), bf16)
    wide = rows.astype(f32)
    high, low = split2(wide * wide)
    sums_ref[:, :count] = mm(ones, rows, NT)[0:1]
    sums_ref[:, count : 2 * count] = (mm(ones, high, NT) + mm(ones, low, NT))[0:1]
    sums_ref[:, 2 * count :] = gain_ref[...]


def share_kernel(experts, capacity, routes_ref, weight_ref, out_ref):
    routes_t = routes_ref[...]
    weight_t = weight_ref[...]
    keys = slot_keys(routes_t, experts)
    tokens = keys.shape[1]
    number = iota((experts, tokens), 0)
    share = jnp.zeros((experts, tokens), f32)
    for k in range(routes_t.shape[0]):
        share = share + jnp.where(routes_t[k : k + 1, :] == number, weight_t[k : k + 1, :], 0.0)
    slot = iota((capacity, tokens), 0).astype(f32)
    spread = [
        jnp.where(slot == keys[e : e + 1, :], share[e : e + 1, :], 0.0)
        for e in range(experts)
    ]
    same = ones_where(iota((tokens, tokens), 0) == iota((tokens, tokens), 1))
    for n, term in enumerate(split3(jnp.concatenate(spread, axis=0))):
        out_ref[n] = mm(same, term, NT).astype(bf16)


def fetch_kernel(*refs):
    count = (len(refs) - 1) // 2
    sems = refs[-1]
    copies = [
        pltpu.make_async_copy(refs[n], refs[count + n], sems.at[n]) for n in range(count)
    ]
    for copy in copies:
        copy.start()
    for copy in copies:
        copy.wait()


def combine_kernel(share_ref, back_ref, out_ref):
    back = back_ref[...]
    out = mm(share_ref[0], back) + (mm(share_ref[1], back) + mm(share_ref[2], back))
    out_ref[...] = out.astype(bf16)


def hidden_kernel(parts, senders, start, load, me_ref, *refs):
    packs = refs[:parts]
    blocks = refs[parts : 2 * parts]
    if load:
        sources = refs[2 * parts : 2 * parts + 3]
        hidden_ref, odd_ref, even_ref, gate_ref, up_ref, down_ref = refs[
            2 * parts + 3 : 2 * parts + 9
        ]
        normed_ref, sems = refs[2 * parts + 9 :]
    else:
        gate_ref, up_ref, down_ref, hidden_ref, odd_ref, even_ref, normed_ref = refs[
            2 * parts :
        ]
    rows, units = hidden_ref.shape
    full, feats = blocks[0].shape
    width = parts * feats
    chunk = rows // senders
    me = me_ref[0]
    lead = packs[0].shape[1] - feats
    size = min(units, 256)
    loads = []
    if load:
        for n in range(units // size):
            cols = pl.ds(n * size, size)
            loads.append([
                pltpu.make_async_copy(
                    sources[m].at[0, :, cols], ref.at[0, :, cols], sems.at[m, n]
                )
                for m, ref in enumerate((gate_ref, up_ref))
            ])
        loads.append([pltpu.make_async_copy(sources[2], down_ref, sems.at[2, 0])])
        for group in loads:
            for copy in group:
                copy.start()

    def body(sender, unused):
        here = pl.ds(pl.multiple_of(sender * chunk, chunk), chunk)
        there = pl.ds(pl.multiple_of(sender * (full // senders) + start, chunk), chunk)
        at = [there if k < 2 else here for k in range(parts)]
        total = jnp.zeros((chunk, 1), f32)
        square = jnp.zeros((chunk, 1), f32)
        for k, block in enumerate(blocks):
            wide = block[at[k], :].astype(f32)
            total = total + jnp.sum(wide, axis=1, keepdims=True)
            square = square + jnp.sum(wide * wide, axis=1, keepdims=True)
        mean = total / width
        scale = lax.rsqrt(square / width - mean * mean + norm_eps)
        for k, block in enumerate(blocks):
            gain = packs[k][:, lead:]
            value = (block[at[k], :].astype(f32) - mean) * scale * gain
            cols = pl.ds(pl.multiple_of((me ^ k) * feats, feats), feats)
            normed_ref[here, cols] = value.astype(bf16)
        return unused

    lax.fori_loop(0, senders, body, 0, unroll=2)
    for at in range(0, units, size):
        cols = pl.ds(at, size)
        if load:
            for copy in loads[at // size]:
                copy.wait()
        normed = normed_ref[...]
        gate = mm(normed, gate_ref[0, :, cols])
        up = mm(normed, up_ref[0, :, cols])
        hidden_ref[:, cols] = (gate * jax.nn.sigmoid(gate) * up).astype(bf16)
    if load:
        loads[-1][0].wait()
    for first, out in ((3, odd_ref), (2, even_ref)):
        for n in range(out.shape[0]):
            out[n] = down_part(me ^ (2 * n + first), hidden_ref, down_ref, feats)


def down_part(which, hidden_ref, weight_ref, feats):
    cols = pl.ds(pl.multiple_of(which * feats, feats), feats)
    return mm(hidden_ref[...], weight_ref[0, :, cols]).astype(bf16)


def near_kernel(count, me_ref, *refs):
    hiddens = refs[:count]
    down_ref, near_ref, *owns = refs[count:]
    feats = near_ref.shape[1]
    rows = near_ref.shape[0] // count
    for c, hidden in enumerate(hiddens):
        near_ref[pl.ds(c * rows, rows), :] = down_part(me_ref[0] ^ 1, hidden, down_ref, feats)
    for own, hidden in zip(owns, hiddens):
        own[...] = down_part(me_ref[0], hidden, down_ref, feats)


def join_kernel(count, senders, near_ref, *refs):
    out_ref = refs[-1]
    terms = (len(refs) - 1) // count
    part = near_ref.shape[0] // count
    chunk = part // senders
    for c in range(count):
        for e in range(senders):
            total = near_ref[pl.ds(c * part + e * chunk, chunk), :].astype(f32)
            for ref in refs[c * terms : (c + 1) * terms]:
                total = total + ref[pl.ds(e * chunk, chunk), :].astype(f32)
            out_ref[pl.ds((e * count + c) * chunk, chunk), :] = total.astype(bf16)


def reorder(rows, back):
    steps = rows // LANES
    row, col = iota((rows, rows), 1 if back else 0), iota((rows, rows), 0 if back else 1)
    return ones_where(col == (row % LANES) * steps + row // LANES)


def in_line(table, width):
    states = table.shape[1]
    wide = spread_table(table, states, 1, states, width)
    return jnp.sum(wide, axis=0, keepdims=True)


def sin_cos(angle):
    turns = jnp.floor(angle * 0.6366197723675814 + 0.5)
    rest = angle - turns * 1.5703125
    rest = rest - turns * 4.83751296997070312e-4
    rest = rest - turns * 7.54978995489188e-8
    z = rest * rest
    sine = rest + rest * z * (
        -1.6666654611e-1 + z * (8.3321608736e-3 + z * -1.9515295891e-4)
    )
    cosine = 1.0 - 0.5 * z + z * z * (
        4.166664568298827e-2 + z * (-1.388731625493765e-3 + z * 2.443315711809948e-5)
    )
    quarter = turns.astype(jnp.int32)
    odd = (quarter & 1) != 0
    first = jnp.where(odd, cosine, sine)
    second = jnp.where(odd, sine, cosine)
    first = jnp.where((quarter & 2) != 0, -first, first)
    second = jnp.where(((quarter + 1) & 2) != 0, -second, second)
    return first, second


def spread_table(table, inner, outer_rows, outer_cols, width):
    rows = table.shape[0]
    pick = ones_where(iota((inner, width), 1) % inner == iota((inner, width), 0))
    high, mid, low = split3(table)
    wide = mm(high, pick) + (mm(mid, pick) + mm(low, pick))
    same = iota((rows, width), 0) // outer_rows == iota((rows, width), 1) // outer_cols
    return jnp.where(same, wide, 0.0)


def poles_kernel(step_ref, pr_ref, pi_ref, ar_ref, ai_ref, over_ref):
    groups, states = pr_ref.shape
    rows, flat = ar_ref.shape
    order = reorder(rows, False)
    poles_re = in_line(pr_ref[...], flat)
    poles_im = in_line(pi_ref[...], flat)
    size = poles_re * poles_re + poles_im * poles_im
    over_ref[0:1, :] = poles_re / size
    over_ref[1:2, :] = -poles_im / size
    d_high, d_mid, d_low = (
        mm(part, order, NT).astype(bf16) for part in split3(step_ref[...])
    )
    piece = min(flat, 256)
    for at in range(0, flat, piece):
        cols = pl.ds(at, piece)
        expand = ones_where(
            iota((groups, piece), 0) == (iota((groups, piece), 1) + at) // states
        )
        delta = mm(d_high, expand, TN) + (mm(d_mid, expand, TN) + mm(d_low, expand, TN))
        size = jnp.exp(poles_re[:, at : at + piece] * delta)
        sine, cosine = sin_cos(poles_im[:, at : at + piece] * delta)
        ar_ref[:, cols] = size * cosine
        ai_ref[:, cols] = size * sine


def scan_kernel(
    total, parts, x_ref, gain_ref, ar_ref, ai_ref, over_ref, ir_ref, ii_ref, *refs,
):
    packs = refs[:parts]
    h_re_out, h_im_out, c_re_out, c_im_out, end_ref = refs[parts : parts + 5]
    hr_ref, hi_ref, cr_ref, ci_ref, sems = refs[parts + 5 :]
    rows, feats = x_ref.shape
    flat = ar_ref.shape[1]
    states = ir_ref.shape[1]
    inner = feats // (flat // states)
    steps = rows // LANES
    order = reorder(rows, False)
    packed = packs[0][:, : 2 * rows]
    for other in packs[1:]:
        packed = packed + other[:, : 2 * rows]
    mean = packed[:, :rows] / total
    scale = lax.rsqrt(packed[:, rows:] / total - mean * mean + norm_eps)
    match = iota((rows, rows), 1) == (iota((rows, rows), 0) % LANES) * steps + iota(
        (rows, rows), 0
    ) // LANES
    mean_col = jnp.sum(jnp.where(match, mean, 0.0), axis=1, keepdims=True)
    scale_col = jnp.sum(jnp.where(match, scale, 0.0), axis=1, keepdims=True)
    cw = min(feats, 256)
    sw = cw // inner * states
    copies = []
    for b in range(feats // cw):
        chans = pl.ds(b * cw, cw)
        cols = pl.ds(b * sw, sw)
        rows_in = mm(order, x_ref[:, chans])
        normed = split2((rows_in - mean_col) * scale_col * gain_ref[:, chans])
        real = split2(spread_table(ir_ref[chans, :], states, inner, states, sw))
        imag = split2(spread_table(ii_ref[chans, :], states, inner, states, sw))
        hr_ref[:, cols], hi_ref[:, cols] = mul(
            mm3(normed, real, NN), mm3(normed, imag, NN), over_ref[0:1, cols], over_ref[1:2, cols]
        )

        def body(j, carry):
            h_re, h_im, c_re, c_im = carry
            here = pl.ds(pl.multiple_of(j * LANES, LANES), LANES)
            a_re, a_im = ar_ref[here, cols], ai_ref[here, cols]
            d_re, d_im = hr_ref[here, cols], hi_ref[here, cols]
            h_re, h_im = mul(a_re, a_im, h_re + d_re, h_im + d_im)
            h_re, h_im = h_re - d_re, h_im - d_im
            c_re, c_im = mul(a_re, a_im, c_re, c_im)
            hr_ref[here, cols], hi_ref[here, cols] = h_re, h_im
            cr_ref[here, cols], ci_ref[here, cols] = c_re, c_im
            return h_re, h_im, c_re, c_im

        zero = jnp.zeros((LANES, sw), f32)
        lax.fori_loop(0, steps, body, (zero, zero, zero + 1.0, zero), unroll=2)
        for n, (ref, out) in enumerate((
            (hr_ref, h_re_out), (hi_ref, h_im_out), (cr_ref, c_re_out), (ci_ref, c_im_out),
        )):
            copies.append(
                pltpu.make_async_copy(ref.at[:, cols], out.at[:, cols], sems.at[b, n])
            )
            copies[-1].start()
    last = pl.ds(rows - LANES, LANES)
    h_re, h_im, c_re, c_im = hr_ref[last, :], hi_ref[last, :], cr_ref[last, :], ci_ref[last, :]
    p_re, p_im = c_re[0:1], c_im[0:1]
    s_re, s_im = h_re[0:1], h_im[0:1]
    for c in range(1, LANES):
        k_re, k_im = c_re[c : c + 1], c_im[c : c + 1]
        p_re, p_im = mul(k_re, k_im, p_re, p_im)
        s_re, s_im = mul(k_re, k_im, s_re, s_im)
        s_re, s_im = s_re + h_re[c : c + 1], s_im + h_im[c : c + 1]
    ends = jnp.concatenate([p_re, p_im, s_re, s_im], axis=0)
    for i in range(end_ref.shape[0]):
        end_ref[i] = ends
    for copy in copies:
        copy.wait()


def read_kernel(
    me_ref, got_ref, h_re_in, h_im_in, c_re_in, c_im_in, rr_ref, ri_ref, out_ref,
    hr_ref, hi_ref, cr_ref, ci_ref, sems,
):
    rows, flat = hr_ref.shape
    feats = out_ref.shape[1]
    states = rr_ref.shape[1]
    inner = feats // (flat // states)
    steps = rows // LANES
    me = me_ref[0]
    cw = min(feats, 256)
    sw = cw // inner * states
    last = pl.ds(rows - LANES, LANES)
    pairs = ((h_re_in, hr_ref), (h_im_in, hi_ref), (c_re_in, cr_ref), (c_im_in, ci_ref))
    loads = []
    for b in range(feats // cw):
        cols = pl.ds(b * sw, sw)
        loads.append([
            pltpu.make_async_copy(src.at[:, cols], ref.at[:, cols], sems.at[b, n])
            for n, (src, ref) in enumerate(pairs)
        ])
        for copy in loads[-1]:
            copy.start()
    s_re = jnp.zeros((1, flat), f32)
    s_im = jnp.zeros((1, flat), f32)
    for i in range(got_ref.shape[0] - 1):
        ends = got_ref[i]
        n_re, n_im = mul(ends[0:1], ends[1:2], s_re, s_im)
        s_re = jnp.where(i < me, n_re + ends[2:3], s_re)
        s_im = jnp.where(i < me, n_im + ends[3:4], s_im)
    back = reorder(rows, True)
    for b in range(feats // cw):
        chans = pl.ds(b * cw, cw)
        lo = b * sw
        cols = pl.ds(lo, sw)
        real = split2(spread_table(rr_ref[chans, :], states, inner, states, sw))
        imag = split2(spread_table(ri_ref[chans, :], states, inner, states, sw))
        for copy in loads[b]:
            copy.wait()
        h_re, h_im, c_re, c_im = (
            ref[last, cols] for ref in (hr_ref, hi_ref, cr_ref, ci_ref)
        )
        in_re, in_im = [s_re[:, lo : lo + sw]], [s_im[:, lo : lo + sw]]
        for c in range(LANES - 1):
            n_re, n_im = mul(c_re[c : c + 1], c_im[c : c + 1], in_re[-1], in_im[-1])
            in_re.append(n_re + h_re[c : c + 1])
            in_im.append(n_im + h_im[c : c + 1])
        g_re = jnp.concatenate(in_re, axis=0)[None]
        g_im = jnp.concatenate(in_im, axis=0)[None]
        shape = (steps, LANES, sw)
        c_re, c_im = cr_ref[:, cols].reshape(shape), ci_ref[:, cols].reshape(shape)
        f_re = hr_ref[:, cols].reshape(shape) + (c_re * g_re - c_im * g_im)
        f_im = hi_ref[:, cols].reshape(shape) + (c_re * g_im + c_im * g_re)
        response = mm3(split2(f_re.reshape(rows, sw)), real, NT) - mm3(
            split2(f_im.reshape(rows, sw)), imag, NT
        )
        cube = response + 0.044715 * (response * response * response)
        mixed = 0.5 * response * (1.0 + jnp.tanh(0.7978845608028654 * cube))
        out_ref[:, chans] = mm(back, mixed.astype(bf16)).astype(bf16)


def output_kernel(parts, me_ref, *refs):
    pieces = refs[:parts]
    value_ref, gate_ref, out_ref = refs[parts:]
    feats = pieces[0].shape[1]
    value = gate = None
    for k, piece in enumerate(pieces):
        at = pl.ds(pl.multiple_of((me_ref[0] ^ k) * feats, feats), feats)
        rows = piece[...]
        v, g = mm(rows, value_ref[at, :]), mm(rows, gate_ref[at, :])
        value, gate = (v, g) if value is None else (value + v, gate + g)
    out_ref[...] = (value * jax.nn.sigmoid(gate)).astype(bf16)


vmem = pl.BlockSpec(memory_space=pltpu.VMEM)
hbm = pl.BlockSpec(memory_space=pltpu.HBM)
smem = pl.BlockSpec(memory_space=pltpu.SMEM)


def stay(value):
    return pltpu.with_memory_space_constraint(value, pltpu.HBM)


def params(mib):
    return pltpu.CompilerParams(vmem_limit_bytes=mib << 20)


def swap(value, bit):
    count = lax.axis_size("tp")
    return lax.ppermute(value, "tp", [(i, i ^ bit) for i in range(count)])


def gather_tp(value):
    count = lax.axis_size("tp")
    blocks = {0: value}
    bit = count // 2
    while bit >= 1:
        blocks.update({k ^ bit: swap(block, bit) for k, block in list(blocks.items())})
        bit //= 2
    return [blocks[k] for k in range(count)]


def shards(
    mixer_input, mixer_gain, time_step, pole_real, pole_imag, input_real, input_imag,
    read_real, read_imag, out_value, out_gate, expert_input, expert_gain, routes,
    route_weight, expert_gate, expert_up, expert_down,
):
    n_tp, n_ep = lax.axis_size("tp"), lax.axis_size("ep")
    tp_at = lax.axis_index("tp").astype(jnp.int32).reshape(1)
    ep_at = lax.axis_index("ep").astype(jnp.int32).reshape(1)
    tokens, feats = expert_input.shape
    top = routes.shape[1]
    capacity = 2 * top * tokens // n_ep
    slots = n_ep * capacity
    routes_t = routes.T
    weight_t = route_weight.T

    rows, chans = mixer_input.shape
    send, packed = pl.pallas_call(
        functools.partial(send_kernel, n_ep, capacity),
        out_shape=(
            jax.ShapeDtypeStruct((slots, feats), bf16),
            jax.ShapeDtypeStruct((1, 2 * rows + feats), f32),
        ),
        in_specs=[vmem] * 4, out_specs=(vmem, vmem), compiler_params=params(60),
        name="send_rows",
    )(routes_t, expert_input, mixer_input, expert_gain.reshape(1, feats))
    arrived = lax.all_to_all(send, "ep", split_axis=0, concat_axis=0, tiled=True)
    packed, tp_at, ep_at = lax.optimization_barrier((packed, tp_at, ep_at))
    packs = gather_tp(packed)
    packs[0] = stay(packed)

    groups, states = pole_real.shape
    flat = groups * states
    big = jax.ShapeDtypeStruct((rows, flat), f32)
    a_re, a_im, over = pl.pallas_call(
        poles_kernel,
        out_shape=(big, big, jax.ShapeDtypeStruct((2, flat), f32)),
        in_specs=[vmem] * 3, out_specs=(vmem,) * 3, compiler_params=params(20),
        name="mixer_poles",
    )(stay(time_step.T), stay(pole_real), stay(pole_imag))
    n_block = max(1, chans // 256)
    far_big = pltpu.HBM((rows, flat), f32)
    *carried, ends = pl.pallas_call(
        functools.partial(scan_kernel, float(chans * n_tp), n_tp),
        out_shape=(far_big,) * 4 + (jax.ShapeDtypeStruct((n_ep, 4, flat), f32),),
        in_specs=[vmem] * (7 + n_tp), out_specs=(hbm,) * 4 + (vmem,),
        scratch_shapes=[pltpu.VMEM((rows, flat), f32)] * 4
        + [pltpu.SemaphoreType.DMA((n_block, 4))],
        compiler_params=params(24), name="mixer_scan",
    )(
        stay(mixer_input), stay(mixer_gain.reshape(1, chans)), a_re, a_im, over,
        stay(jnp.swapaxes(input_real, 1, 2).reshape(chans, states)),
        stay(jnp.swapaxes(input_imag, 1, 2).reshape(chans, states)),
        *packs,
    )
    n_half = 2 if capacity % 32 == 0 else 1
    half = capacity // n_half
    share = pl.pallas_call(
        functools.partial(share_kernel, n_ep, capacity),
        out_shape=jax.ShapeDtypeStruct((3, tokens, slots), bf16),
        in_specs=[vmem, vmem], out_specs=vmem, compiler_params=params(8), name="route_share",
    )(stay(routes_t), stay(weight_t))
    got = lax.all_to_all(ends, "ep", split_axis=0, concat_axis=0)

    units = expert_gate.shape[2]
    n_far = n_tp // 2 - 1
    part = n_ep * half
    by_sender = arrived.reshape(n_ep, capacity, feats)
    halves = [by_sender[:, c * half : (c + 1) * half].reshape(part, feats) for c in range(n_half)]
    far_blocks = []
    for c in range(n_half):
        evens = {0: halves[c]}
        bit = n_tp // 2
        while bit > 1:
            evens.update({k ^ bit: swap(b, bit) for k, b in list(evens.items())})
            bit //= 2
        far_blocks.append(evens)
    partner = swap(arrived, 1)
    weights = tuple(stay(w) for w in (expert_gate, expert_up, expert_down))
    n_unit = max(1, units // 256)
    hiddens, sums = [], []
    for c in range(n_half):
        blocks = [arrived, partner]
        for k in range(2, n_tp, 2):
            blocks += [far_blocks[c][k], swap(far_blocks[c][k], 1)]
        far_shape = jax.ShapeDtypeStruct((n_far, part, feats), bf16)
        load = c == 0
        kept = tuple(jax.ShapeDtypeStruct(w.shape, w.dtype) for w in weights) if load else ()
        hidden, odd_far, even_far, *held = pl.pallas_call(
            functools.partial(hidden_kernel, n_tp, n_ep, c * half, load),
            in_specs=[smem] + [vmem] * (2 * n_tp) + [hbm if load else vmem] * 3,
            out_specs=(vmem,) * (3 + len(kept)),
            scratch_shapes=[pltpu.VMEM((part, n_tp * feats), bf16)]
            + ([pltpu.SemaphoreType.DMA((3, n_unit))] if load else []),
            out_shape=(jax.ShapeDtypeStruct((part, units), bf16), far_shape, far_shape, *kept),
            compiler_params=params(12),
        )(tp_at, *packs, *blocks, *weights)
        weights = held or weights
        hiddens.append(hidden)
        theirs = swap(odd_far, 1)
        far = even_far.astype(f32) + theirs.astype(f32)
        come = []
        bit = n_tp // 4
        while bit >= 1:
            got_far = swap(far[bit - 1 :].astype(bf16), 2 * bit)
            come.append(got_far[0])
            far = far[: bit - 1] + got_far[1:].astype(f32)
            bit //= 2
        sums.append(come)
    near, *owns = pl.pallas_call(
        functools.partial(near_kernel, n_half),
        in_specs=[smem] + [vmem] * (n_half + 1), out_specs=(vmem,) * (n_half + 1),
        out_shape=(jax.ShapeDtypeStruct((slots, feats), bf16),)
        + (jax.ShapeDtypeStruct((part, feats), bf16),) * n_half,
        compiler_params=params(8), name="expert_near",
    )(tp_at, *hiddens, weights[2])
    near = swap(near, 1)
    terms = [term for own, come in zip(owns, sums) for term in (own, *come)]
    result = pl.pallas_call(
        functools.partial(join_kernel, n_half, n_ep),
        out_shape=jax.ShapeDtypeStruct((slots, feats), bf16),
        in_specs=[vmem] * (len(terms) + 1), out_specs=vmem, compiler_params=params(8),
        name="expert_join",
    )(near, *terms)
    back = lax.all_to_all(result, "ep", split_axis=0, concat_axis=0, tiled=True)

    mixed = pl.pallas_call(
        read_kernel,
        out_shape=jax.ShapeDtypeStruct((rows, chans), bf16),
        in_specs=[smem, vmem] + [hbm] * 4 + [vmem] * 2, out_specs=vmem,
        scratch_shapes=[pltpu.VMEM((rows, flat), f32)] * 4
        + [pltpu.SemaphoreType.DMA((n_block, 4))],
        compiler_params=params(20), name="mixer_read",
    )(
        ep_at, got, *(stay(x) for x in carried),
        stay(read_real.reshape(chans, states)), stay(read_imag.reshape(chans, states)),
    )
    pieces = gather_tp(mixed)
    value_w, gate_w = pl.pallas_call(
        fetch_kernel,
        out_shape=tuple(jax.ShapeDtypeStruct(w.shape, bf16) for w in (out_value, out_gate)),
        in_specs=[hbm] * 2, out_specs=(vmem,) * 2,
        scratch_shapes=[pltpu.SemaphoreType.DMA((2,))],
        compiler_params=params(10), name="out_fetch",
    )(stay(out_value), stay(out_gate))
    mixer_output = pl.pallas_call(
        functools.partial(output_kernel, n_tp),
        out_shape=jax.ShapeDtypeStruct((rows, out_value.shape[1]), bf16),
        in_specs=[smem] + [vmem] * (n_tp + 2), out_specs=vmem, compiler_params=params(10),
        name="mixer_out",
    )(tp_at, *pieces, value_w, gate_w)
    expert_output = pl.pallas_call(
        combine_kernel,
        out_shape=jax.ShapeDtypeStruct((tokens, feats), bf16),
        in_specs=[vmem] * 2, out_specs=vmem, compiler_params=params(8), name="combine",
    )(share, back)
    return mixer_output, expert_output


def solution(mesh):
    return jax.shard_map(
        shards,
        mesh=mesh,
        in_specs=(
            P("ep", "tp"), P("tp"), P("ep", "tp"), P("tp", None), P("tp", None),
            P("tp", None, None), P("tp", None, None), P("tp", None, None), P("tp", None, None),
            P(None, "tp"), P(None, "tp"), P("ep", "tp"), P("tp"), P("ep", None), P("ep", None),
            P("ep", None, "tp"), P("ep", None, "tp"), P("ep", "tp", None),
        ),
        out_specs=(P("ep", "tp"), P("ep", "tp")),
        check_vma=False,
    )
```

```python
import functools

import jax
import jax.numpy as jnp
from jax import lax
from jax.experimental import pallas as pl
from jax.experimental.pallas import tpu as pltpu
from jax.sharding import PartitionSpec as P


f32 = jnp.float32
bf16 = jnp.bfloat16
norm_eps = 1e-05
LANES = 8
NN = (((1,), (0,)), ((), ()))
NT = (((1,), (1,)), ((), ()))
TN = (((0,), (0,)), ((), ()))


def iota(shape, dim):
    return lax.broadcasted_iota(jnp.int32, shape, dim)


def ones_where(mask):
    return jnp.where(mask, 1.0, 0.0).astype(bf16)


def split2(value):
    high = value.astype(bf16)
    return high, (value - high.astype(f32)).astype(bf16)


def split3(value):
    high = value.astype(bf16)
    rest = value - high.astype(f32)
    mid = rest.astype(bf16)
    return high, mid, (rest - mid.astype(f32)).astype(bf16)


def mm(left, right, dims=NN):
    return lax.dot_general(left, right, dims, preferred_element_type=f32)


def mm3(left, right, dims):
    lh, ll = left
    rh, rl = right
    return mm(lh, rh, dims) + (mm(ll, rh, dims) + mm(lh, rl, dims))


def mul(ar, ai, br, bi):
    return ar * br - ai * bi, ar * bi + ai * br


def slot_keys(routes_t, experts):
    top, tokens = routes_t.shape
    number = iota((experts, tokens), 0)
    hit = routes_t[0:1, :] == number
    for k in range(1, top):
        hit = hit | (routes_t[k : k + 1, :] == number)
    before = ones_where(iota((tokens, tokens), 0) < iota((tokens, tokens), 1))
    place = mm(ones_where(hit), before)
    return jnp.where(hit, place, -1.0)


def send_kernel(experts, capacity, routes_ref, rows_ref, x_ref, gain_ref, out_ref, sums_ref):
    keys = slot_keys(routes_ref[...], experts)
    tokens = keys.shape[1]
    slot = iota((capacity, tokens), 0).astype(f32)
    chosen = [ones_where(slot == keys[e : e + 1, :]) for e in range(experts)]
    out_ref[...] = mm(jnp.concatenate(chosen, axis=0), rows_ref[...]).astype(bf16)
    rows = x_ref[...]
    count = rows.shape[0]
    ones = jnp.ones((8, rows.shape[1]), bf16)
    wide = rows.astype(f32)
    high, low = split2(wide * wide)
    sums_ref[:, :count] = mm(ones, rows, NT)[0:1]
    sums_ref[:, count : 2 * count] = (mm(ones, high, NT) + mm(ones, low, NT))[0:1]
    sums_ref[:, 2 * count :] = gain_ref[...]


def share_kernel(experts, capacity, routes_ref, weight_ref, out_ref):
    routes_t = routes_ref[...]
    weight_t = weight_ref[...]
    keys = slot_keys(routes_t, experts)
    tokens = keys.shape[1]
    number = iota((experts, tokens), 0)
    share = jnp.zeros((experts, tokens), f32)
    for k in range(routes_t.shape[0]):
        share = share + jnp.where(routes_t[k : k + 1, :] == number, weight_t[k : k + 1, :], 0.0)
    slot = iota((capacity, tokens), 0).astype(f32)
    spread = [
        jnp.where(slot == keys[e : e + 1, :], share[e : e + 1, :], 0.0)
        for e in range(experts)
    ]
    same = ones_where(iota((tokens, tokens), 0) == iota((tokens, tokens), 1))
    for n, term in enumerate(split3(jnp.concatenate(spread, axis=0))):
        out_ref[n] = mm(same, term, NT).astype(bf16)


def fetch_kernel(*refs):
    count = (len(refs) - 1) // 2
    sems = refs[-1]
    copies = [
        pltpu.make_async_copy(refs[n], refs[count + n], sems.at[n]) for n in range(count)
    ]
    for copy in copies:
        copy.start()
    for copy in copies:
        copy.wait()


def combine_kernel(share_ref, back_ref, out_ref):
    back = back_ref[...]
    out = mm(share_ref[0], back) + (mm(share_ref[1], back) + mm(share_ref[2], back))
    out_ref[...] = out.astype(bf16)


def hidden_kernel(parts, senders, start, me_ref, *refs):
    packs = refs[:parts]
    blocks = refs[parts : 2 * parts]
    gate_ref, up_ref, down_ref, hidden_ref, odd_ref, normed_ref = refs[2 * parts :]
    rows, units = hidden_ref.shape
    full, feats = blocks[0].shape
    width = parts * feats
    chunk = rows // senders
    me = me_ref[0]
    lead = packs[0].shape[1] - feats
    size = min(units, 256)

    def body(sender, unused):
        here = pl.ds(pl.multiple_of(sender * chunk, chunk), chunk)
        there = pl.ds(pl.multiple_of(sender * (full // senders) + start, chunk), chunk)
        at = [there if k < 2 else here for k in range(parts)]
        total = jnp.zeros((chunk, 1), f32)
        square = jnp.zeros((chunk, 1), f32)
        for k, block in enumerate(blocks):
            wide = block[at[k], :].astype(f32)
            total = total + jnp.sum(wide, axis=1, keepdims=True)
            square = square + jnp.sum(wide * wide, axis=1, keepdims=True)
        mean = total / width
        scale = lax.rsqrt(square / width - mean * mean + norm_eps)
        for k, block in enumerate(blocks):
            gain = packs[k][:, lead:]
            value = (block[at[k], :].astype(f32) - mean) * scale * gain
            cols = pl.ds(pl.multiple_of((me ^ k) * feats, feats), feats)
            normed_ref[here, cols] = value.astype(bf16)
        return unused

    lax.fori_loop(0, senders, body, 0, unroll=4)
    for at in range(0, units, size):
        cols = pl.ds(at, size)
        normed = normed_ref[...]
        gate = mm(normed, gate_ref[0, :, cols])
        up = mm(normed, up_ref[0, :, cols])
        hidden_ref[:, cols] = (gate * jax.nn.sigmoid(gate) * up).astype(bf16)
    for n in range(odd_ref.shape[0]):
        odd_ref[n] = down_part(me ^ (2 * n + 3), hidden_ref, down_ref, feats)


def down_part(which, hidden_ref, weight_ref, feats):
    cols = pl.ds(pl.multiple_of(which * feats, feats), feats)
    return mm(hidden_ref[...], weight_ref[0, :, cols]).astype(bf16)


def rest_kernel(me_ref, hidden_ref, down_ref, even_ref, near_ref, own_ref):
    me = me_ref[0]
    feats = near_ref.shape[1]
    for n in range(even_ref.shape[0]):
        even_ref[n] = down_part(me ^ (2 * n + 2), hidden_ref, down_ref, feats)
    near_ref[...] = down_part(me ^ 1, hidden_ref, down_ref, feats)
    own_ref[...] = down_part(me, hidden_ref, down_ref, feats)


def join_kernel(count, senders, *refs):
    out_ref = refs[-1]
    terms = (len(refs) - 1) // count
    chunk = refs[0].shape[0] // senders
    for c in range(count):
        for e in range(senders):
            total = None
            for ref in refs[c * terms : (c + 1) * terms]:
                term = ref[pl.ds(e * chunk, chunk), :].astype(f32)
                total = term if total is None else total + term
            out_ref[pl.ds((e * count + c) * chunk, chunk), :] = total.astype(bf16)


def reorder(rows, back):
    steps = rows // LANES
    row, col = iota((rows, rows), 1 if back else 0), iota((rows, rows), 0 if back else 1)
    return ones_where(col == (row % LANES) * steps + row // LANES)


def in_line(table, width):
    states = table.shape[1]
    wide = spread_table(table, states, 1, states, width)
    return jnp.sum(wide, axis=0, keepdims=True)


def sin_cos(angle):
    turns = jnp.floor(angle * 0.6366197723675814 + 0.5)
    rest = angle - turns * 1.5703125
    rest = rest - turns * 4.83751296997070312e-4
    rest = rest - turns * 7.54978995489188e-8
    z = rest * rest
    sine = rest + rest * z * (
        -1.6666654611e-1 + z * (8.3321608736e-3 + z * -1.9515295891e-4)
    )
    cosine = 1.0 - 0.5 * z + z * z * (
        4.166664568298827e-2 + z * (-1.388731625493765e-3 + z * 2.443315711809948e-5)
    )
    quarter = turns.astype(jnp.int32)
    odd = (quarter & 1) != 0
    first = jnp.where(odd, cosine, sine)
    second = jnp.where(odd, sine, cosine)
    first = jnp.where((quarter & 2) != 0, -first, first)
    second = jnp.where(((quarter + 1) & 2) != 0, -second, second)
    return first, second


def spread_table(table, inner, outer_rows, outer_cols, width):
    rows = table.shape[0]
    pick = ones_where(iota((inner, width), 1) % inner == iota((inner, width), 0))
    high, mid, low = split3(table)
    wide = mm(high, pick) + (mm(mid, pick) + mm(low, pick))
    same = iota((rows, width), 0) // outer_rows == iota((rows, width), 1) // outer_cols
    return jnp.where(same, wide, 0.0)


def poles_kernel(step_ref, pr_ref, pi_ref, ar_ref, ai_ref, over_ref):
    groups, states = pr_ref.shape
    rows, flat = ar_ref.shape
    order = reorder(rows, False)
    poles_re = in_line(pr_ref[...], flat)
    poles_im = in_line(pi_ref[...], flat)
    size = poles_re * poles_re + poles_im * poles_im
    over_ref[0:1, :] = poles_re / size
    over_ref[1:2, :] = -poles_im / size
    d_high, d_mid, d_low = (
        mm(part, order, NT).astype(bf16) for part in split3(step_ref[...])
    )
    piece = min(flat, 256)
    for at in range(0, flat, piece):
        cols = pl.ds(at, piece)
        expand = ones_where(
            iota((groups, piece), 0) == (iota((groups, piece), 1) + at) // states
        )
        delta = mm(d_high, expand, TN) + (mm(d_mid, expand, TN) + mm(d_low, expand, TN))
        size = jnp.exp(poles_re[:, at : at + piece] * delta)
        sine, cosine = sin_cos(poles_im[:, at : at + piece] * delta)
        ar_ref[:, cols] = size * cosine
        ai_ref[:, cols] = size * sine


def scan_kernel(
    total, parts, x_ref, gain_ref, ar_ref, ai_ref, over_ref, ir_ref, ii_ref, *refs,
):
    packs = refs[:parts]
    h_re_out, h_im_out, c_re_out, c_im_out, end_ref = refs[parts : parts + 5]
    hr_ref, hi_ref, cr_ref, ci_ref, sems = refs[parts + 5 :]
    rows, feats = x_ref.shape
    flat = ar_ref.shape[1]
    states = ir_ref.shape[1]
    inner = feats // (flat // states)
    steps = rows // LANES
    order = reorder(rows, False)
    packed = packs[0][:, : 2 * rows]
    for other in packs[1:]:
        packed = packed + other[:, : 2 * rows]
    mean = packed[:, :rows] / total
    scale = lax.rsqrt(packed[:, rows:] / total - mean * mean + norm_eps)
    match = iota((rows, rows), 1) == (iota((rows, rows), 0) % LANES) * steps + iota(
        (rows, rows), 0
    ) // LANES
    mean_col = jnp.sum(jnp.where(match, mean, 0.0), axis=1, keepdims=True)
    scale_col = jnp.sum(jnp.where(match, scale, 0.0), axis=1, keepdims=True)
    cw = min(feats, 256)
    sw = cw // inner * states
    copies = []
    for b in range(feats // cw):
        chans = pl.ds(b * cw, cw)
        cols = pl.ds(b * sw, sw)
        rows_in = mm(order, x_ref[:, chans])
        normed = split2((rows_in - mean_col) * scale_col * gain_ref[:, chans])
        real = split2(spread_table(ir_ref[chans, :], states, inner, states, sw))
        imag = split2(spread_table(ii_ref[chans, :], states, inner, states, sw))
        hr_ref[:, cols], hi_ref[:, cols] = mul(
            mm3(normed, real, NN), mm3(normed, imag, NN), over_ref[0:1, cols], over_ref[1:2, cols]
        )

        def body(j, carry):
            h_re, h_im, c_re, c_im = carry
            here = pl.ds(pl.multiple_of(j * LANES, LANES), LANES)
            a_re, a_im = ar_ref[here, cols], ai_ref[here, cols]
            d_re, d_im = hr_ref[here, cols], hi_ref[here, cols]
            h_re, h_im = mul(a_re, a_im, h_re + d_re, h_im + d_im)
            h_re, h_im = h_re - d_re, h_im - d_im
            c_re, c_im = mul(a_re, a_im, c_re, c_im)
            hr_ref[here, cols], hi_ref[here, cols] = h_re, h_im
            cr_ref[here, cols], ci_ref[here, cols] = c_re, c_im
            return h_re, h_im, c_re, c_im

        zero = jnp.zeros((LANES, sw), f32)
        lax.fori_loop(0, steps, body, (zero, zero, zero + 1.0, zero), unroll=2)
        for n, (ref, out) in enumerate((
            (hr_ref, h_re_out), (hi_ref, h_im_out), (cr_ref, c_re_out), (ci_ref, c_im_out),
        )):
            copies.append(
                pltpu.make_async_copy(ref.at[:, cols], out.at[:, cols], sems.at[b, n])
            )
            copies[-1].start()
    last = pl.ds(rows - LANES, LANES)
    h_re, h_im, c_re, c_im = hr_ref[last, :], hi_ref[last, :], cr_ref[last, :], ci_ref[last, :]
    p_re, p_im = c_re[0:1], c_im[0:1]
    s_re, s_im = h_re[0:1], h_im[0:1]
    for c in range(1, LANES):
        k_re, k_im = c_re[c : c + 1], c_im[c : c + 1]
        p_re, p_im = mul(k_re, k_im, p_re, p_im)
        s_re, s_im = mul(k_re, k_im, s_re, s_im)
        s_re, s_im = s_re + h_re[c : c + 1], s_im + h_im[c : c + 1]
    ends = jnp.concatenate([p_re, p_im, s_re, s_im], axis=0)
    for i in range(end_ref.shape[0]):
        end_ref[i] = ends
    for copy in copies:
        copy.wait()


def read_kernel(
    me_ref, got_ref, h_re_in, h_im_in, c_re_in, c_im_in, rr_ref, ri_ref, out_ref,
    hr_ref, hi_ref, cr_ref, ci_ref, sems,
):
    rows, flat = hr_ref.shape
    feats = out_ref.shape[1]
    states = rr_ref.shape[1]
    inner = feats // (flat // states)
    steps = rows // LANES
    me = me_ref[0]
    cw = min(feats, 256)
    sw = cw // inner * states
    last = pl.ds(rows - LANES, LANES)
    pairs = ((h_re_in, hr_ref), (h_im_in, hi_ref), (c_re_in, cr_ref), (c_im_in, ci_ref))
    loads = []
    for b in range(feats // cw):
        cols = pl.ds(b * sw, sw)
        loads.append([
            pltpu.make_async_copy(src.at[:, cols], ref.at[:, cols], sems.at[b, n])
            for n, (src, ref) in enumerate(pairs)
        ])
        for copy in loads[-1]:
            copy.start()
    s_re = jnp.zeros((1, flat), f32)
    s_im = jnp.zeros((1, flat), f32)
    for i in range(got_ref.shape[0] - 1):
        ends = got_ref[i]
        n_re, n_im = mul(ends[0:1], ends[1:2], s_re, s_im)
        s_re = jnp.where(i < me, n_re + ends[2:3], s_re)
        s_im = jnp.where(i < me, n_im + ends[3:4], s_im)
    back = reorder(rows, True)
    for b in range(feats // cw):
        chans = pl.ds(b * cw, cw)
        lo = b * sw
        cols = pl.ds(lo, sw)
        real = split2(spread_table(rr_ref[chans, :], states, inner, states, sw))
        imag = split2(spread_table(ri_ref[chans, :], states, inner, states, sw))
        for copy in loads[b]:
            copy.wait()
        h_re, h_im, c_re, c_im = (
            ref[last, cols] for ref in (hr_ref, hi_ref, cr_ref, ci_ref)
        )
        in_re, in_im = [s_re[:, lo : lo + sw]], [s_im[:, lo : lo + sw]]
        for c in range(LANES - 1):
            n_re, n_im = mul(c_re[c : c + 1], c_im[c : c + 1], in_re[-1], in_im[-1])
            in_re.append(n_re + h_re[c : c + 1])
            in_im.append(n_im + h_im[c : c + 1])
        g_re = jnp.concatenate(in_re, axis=0)[None]
        g_im = jnp.concatenate(in_im, axis=0)[None]
        shape = (steps, LANES, sw)
        c_re, c_im = cr_ref[:, cols].reshape(shape), ci_ref[:, cols].reshape(shape)
        f_re = hr_ref[:, cols].reshape(shape) + (c_re * g_re - c_im * g_im)
        f_im = hi_ref[:, cols].reshape(shape) + (c_re * g_im + c_im * g_re)
        response = mm3(split2(f_re.reshape(rows, sw)), real, NT) - mm3(
            split2(f_im.reshape(rows, sw)), imag, NT
        )
        cube = response + 0.044715 * (response * response * response)
        mixed = 0.5 * response * (1.0 + jnp.tanh(0.7978845608028654 * cube))
        out_ref[:, chans] = mm(back, mixed.astype(bf16)).astype(bf16)


def output_kernel(parts, me_ref, *refs):
    pieces = refs[:parts]
    value_ref, gate_ref, out_ref = refs[parts:]
    feats = pieces[0].shape[1]
    value = gate = None
    for k, piece in enumerate(pieces):
        at = pl.ds(pl.multiple_of((me_ref[0] ^ k) * feats, feats), feats)
        rows = piece[...]
        v, g = mm(rows, value_ref[at, :]), mm(rows, gate_ref[at, :])
        value, gate = (v, g) if value is None else (value + v, gate + g)
    out_ref[...] = (value * jax.nn.sigmoid(gate)).astype(bf16)


vmem = pl.BlockSpec(memory_space=pltpu.VMEM)
hbm = pl.BlockSpec(memory_space=pltpu.HBM)
smem = pl.BlockSpec(memory_space=pltpu.SMEM)


def stay(value):
    return pltpu.with_memory_space_constraint(value, pltpu.HBM)


def params(mib):
    return pltpu.CompilerParams(vmem_limit_bytes=mib << 20)


def swap(value, bit):
    count = lax.axis_size("tp")
    return lax.ppermute(value, "tp", [(i, i ^ bit) for i in range(count)])


def gather_tp(value):
    count = lax.axis_size("tp")
    blocks = {0: value}
    bit = count // 2
    while bit >= 1:
        blocks.update({k ^ bit: swap(block, bit) for k, block in list(blocks.items())})
        bit //= 2
    return [blocks[k] for k in range(count)]


def shards(
    mixer_input, mixer_gain, time_step, pole_real, pole_imag, input_real, input_imag,
    read_real, read_imag, out_value, out_gate, expert_input, expert_gain, routes,
    route_weight, expert_gate, expert_up, expert_down,
):
    n_tp, n_ep = lax.axis_size("tp"), lax.axis_size("ep")
    tp_at = lax.axis_index("tp").astype(jnp.int32).reshape(1)
    ep_at = lax.axis_index("ep").astype(jnp.int32).reshape(1)
    tokens, feats = expert_input.shape
    top = routes.shape[1]
    capacity = 2 * top * tokens // n_ep
    slots = n_ep * capacity
    routes_t = routes.T
    weight_t = route_weight.T

    rows, chans = mixer_input.shape
    send, packed = pl.pallas_call(
        functools.partial(send_kernel, n_ep, capacity),
        out_shape=(
            jax.ShapeDtypeStruct((slots, feats), bf16),
            jax.ShapeDtypeStruct((1, 2 * rows + feats), f32),
        ),
        in_specs=[vmem] * 4, out_specs=(vmem, vmem), compiler_params=params(60),
        name="send_rows",
    )(routes_t, expert_input, mixer_input, expert_gain.reshape(1, feats))
    arrived = lax.all_to_all(send, "ep", split_axis=0, concat_axis=0, tiled=True)
    packed, tp_at, ep_at = lax.optimization_barrier((packed, tp_at, ep_at))
    packs = gather_tp(packed)
    packs[0] = stay(packed)

    groups, states = pole_real.shape
    flat = groups * states
    big = jax.ShapeDtypeStruct((rows, flat), f32)
    a_re, a_im, over = pl.pallas_call(
        poles_kernel,
        out_shape=(big, big, jax.ShapeDtypeStruct((2, flat), f32)),
        in_specs=[vmem] * 3, out_specs=(vmem,) * 3, compiler_params=params(20),
        name="mixer_poles",
    )(stay(time_step.T), stay(pole_real), stay(pole_imag))
    n_block = max(1, chans // 256)
    far_big = pltpu.HBM((rows, flat), f32)
    *carried, ends = pl.pallas_call(
        functools.partial(scan_kernel, float(chans * n_tp), n_tp),
        out_shape=(far_big,) * 4 + (jax.ShapeDtypeStruct((n_ep, 4, flat), f32),),
        in_specs=[vmem] * (7 + n_tp), out_specs=(hbm,) * 4 + (vmem,),
        scratch_shapes=[pltpu.VMEM((rows, flat), f32)] * 4
        + [pltpu.SemaphoreType.DMA((n_block, 4))],
        compiler_params=params(24), name="mixer_scan",
    )(
        stay(mixer_input), stay(mixer_gain.reshape(1, chans)), a_re, a_im, over,
        stay(jnp.swapaxes(input_real, 1, 2).reshape(chans, states)),
        stay(jnp.swapaxes(input_imag, 1, 2).reshape(chans, states)),
        *packs,
    )
    n_half = 2 if capacity % 32 == 0 else 1
    half = capacity // n_half
    share = pl.pallas_call(
        functools.partial(share_kernel, n_ep, capacity),
        out_shape=jax.ShapeDtypeStruct((3, tokens, slots), bf16),
        in_specs=[vmem, vmem], out_specs=vmem, compiler_params=params(8), name="route_share",
    )(stay(routes_t), stay(weight_t))
    got = lax.all_to_all(ends, "ep", split_axis=0, concat_axis=0)

    units = expert_gate.shape[2]
    n_far = n_tp // 2 - 1
    part = n_ep * half
    by_sender = arrived.reshape(n_ep, capacity, feats)
    halves = [by_sender[:, c * half : (c + 1) * half].reshape(part, feats) for c in range(n_half)]
    far_blocks = []
    for c in range(n_half):
        evens = {0: halves[c]}
        bit = n_tp // 2
        while bit > 1:
            evens.update({k ^ bit: swap(b, bit) for k, b in list(evens.items())})
            bit //= 2
        far_blocks.append(evens)
    partner = swap(arrived, 1)

    def fetch(*weights):
        return pl.pallas_call(
            fetch_kernel,
            out_shape=tuple(jax.ShapeDtypeStruct(w.shape, w.dtype) for w in weights),
            in_specs=[hbm] * len(weights), out_specs=(vmem,) * len(weights),
            scratch_shapes=[pltpu.SemaphoreType.DMA((len(weights),))],
            compiler_params=params(10),
        )(*(stay(w) for w in weights))

    gate_w, up_w = fetch(expert_gate, expert_up)
    (down_w,) = fetch(expert_down)
    terms = []
    for c in range(n_half):
        blocks = [arrived, partner]
        for k in range(2, n_tp, 2):
            blocks += [far_blocks[c][k], swap(far_blocks[c][k], 1)]
        far_shape = jax.ShapeDtypeStruct((n_far, part, feats), bf16)
        part_shape = jax.ShapeDtypeStruct((part, feats), bf16)
        hidden, odd_far = pl.pallas_call(
            functools.partial(hidden_kernel, n_tp, n_ep, c * half),
            in_specs=[smem] + [vmem] * (2 * n_tp + 3), out_specs=(vmem,) * 2,
            scratch_shapes=[pltpu.VMEM((part, n_tp * feats), bf16)],
            out_shape=(jax.ShapeDtypeStruct((part, units), bf16), far_shape),
            compiler_params=params(12),
        )(tp_at, *packs, *blocks, gate_w, up_w, down_w)
        theirs = swap(odd_far, 1)
        even_far, near, own = pl.pallas_call(
            rest_kernel,
            in_specs=[smem] + [vmem] * 2, out_specs=(vmem,) * 3,
            out_shape=(far_shape, part_shape, part_shape),
            compiler_params=params(8),
        )(tp_at, hidden, down_w)
        far = even_far.astype(f32) + theirs.astype(f32)
        terms += [own, swap(near, 1)]
        bit = n_tp // 4
        while bit >= 1:
            come = swap(far[bit - 1 :].astype(bf16), 2 * bit)
            terms.append(come[0])
            far = far[: bit - 1] + come[1:].astype(f32)
            bit //= 2
    result = pl.pallas_call(
        functools.partial(join_kernel, n_half, n_ep),
        out_shape=jax.ShapeDtypeStruct((slots, feats), bf16),
        in_specs=[vmem] * len(terms), out_specs=vmem, compiler_params=params(8),
        name="expert_join",
    )(*terms)
    back = lax.all_to_all(result, "ep", split_axis=0, concat_axis=0, tiled=True)

    mixed = pl.pallas_call(
        read_kernel,
        out_shape=jax.ShapeDtypeStruct((rows, chans), bf16),
        in_specs=[smem, vmem] + [hbm] * 4 + [vmem] * 2, out_specs=vmem,
        scratch_shapes=[pltpu.VMEM((rows, flat), f32)] * 4
        + [pltpu.SemaphoreType.DMA((n_block, 4))],
        compiler_params=params(20), name="mixer_read",
    )(
        ep_at, got, *(stay(x) for x in carried),
        stay(read_real.reshape(chans, states)), stay(read_imag.reshape(chans, states)),
    )
    pieces = gather_tp(mixed)
    value_w, gate_w = fetch(out_value, out_gate)
    mixer_output = pl.pallas_call(
        functools.partial(output_kernel, n_tp),
        out_shape=jax.ShapeDtypeStruct((rows, out_value.shape[1]), bf16),
        in_specs=[smem] + [vmem] * (n_tp + 2), out_specs=vmem, compiler_params=params(10),
        name="mixer_out",
    )(tp_at, *pieces, value_w, gate_w)
    expert_output = pl.pallas_call(
        combine_kernel,
        out_shape=jax.ShapeDtypeStruct((tokens, feats), bf16),
        in_specs=[vmem] * 2, out_specs=vmem, compiler_params=params(8), name="combine",
    )(share, back)
    return mixer_output, expert_output


def solution(mesh):
    return jax.shard_map(
        shards,
        mesh=mesh,
        in_specs=(
            P("ep", "tp"), P("tp"), P("ep", "tp"), P("tp", None), P("tp", None),
            P("tp", None, None), P("tp", None, None), P("tp", None, None), P("tp", None, None),
            P(None, "tp"), P(None, "tp"), P("ep", "tp"), P("tp"), P("ep", None), P("ep", None),
            P("ep", None, "tp"), P("ep", None, "tp"), P("ep", "tp", None),
        ),
        out_specs=(P("ep", "tp"), P("ep", "tp")),
        check_vma=False,
    )
```

```python
import functools

import jax
import jax.numpy as jnp
from jax import lax
from jax.experimental import pallas as pl
from jax.experimental.pallas import tpu as pltpu
from jax.sharding import PartitionSpec as P


f32 = jnp.float32
bf16 = jnp.bfloat16
norm_eps = 1e-05
LANES = 8
NN = (((1,), (0,)), ((), ()))
NT = (((1,), (1,)), ((), ()))
TN = (((0,), (0,)), ((), ()))


def iota(shape, dim):
    return lax.broadcasted_iota(jnp.int32, shape, dim)


def ones_where(mask):
    return jnp.where(mask, 1.0, 0.0).astype(bf16)


def split2(value):
    high = value.astype(bf16)
    return high, (value - high.astype(f32)).astype(bf16)


def split3(value):
    high = value.astype(bf16)
    rest = value - high.astype(f32)
    mid = rest.astype(bf16)
    return high, mid, (rest - mid.astype(f32)).astype(bf16)


def mm(left, right, dims=NN):
    return lax.dot_general(left, right, dims, preferred_element_type=f32)


def mm3(left, right, dims):
    lh, ll = left
    rh, rl = right
    return mm(lh, rh, dims) + (mm(ll, rh, dims) + mm(lh, rl, dims))


def mul(ar, ai, br, bi):
    return ar * br - ai * bi, ar * bi + ai * br


def slot_keys(routes_t, experts):
    top, tokens = routes_t.shape
    number = iota((experts, tokens), 0)
    hit = routes_t[0:1, :] == number
    for k in range(1, top):
        hit = hit | (routes_t[k : k + 1, :] == number)
    before = ones_where(iota((tokens, tokens), 0) < iota((tokens, tokens), 1))
    place = mm(ones_where(hit), before)
    return jnp.where(hit, place, -1.0)


def send_kernel(experts, capacity, routes_ref, rows_ref, x_ref, gain_ref, out_ref, sums_ref):
    keys = slot_keys(routes_ref[...], experts)
    tokens = keys.shape[1]
    slot = iota((capacity, tokens), 0).astype(f32)
    chosen = [ones_where(slot == keys[e : e + 1, :]) for e in range(experts)]
    out_ref[...] = mm(jnp.concatenate(chosen, axis=0), rows_ref[...]).astype(bf16)
    rows = x_ref[...]
    count = rows.shape[0]
    ones = jnp.ones((8, rows.shape[1]), bf16)
    wide = rows.astype(f32)
    high, low = split2(wide * wide)
    sums_ref[:, :count] = mm(ones, rows, NT)[0:1]
    sums_ref[:, count : 2 * count] = (mm(ones, high, NT) + mm(ones, low, NT))[0:1]
    sums_ref[:, 2 * count :] = gain_ref[...]


def share_kernel(experts, capacity, routes_ref, weight_ref, out_ref):
    routes_t = routes_ref[...]
    weight_t = weight_ref[...]
    keys = slot_keys(routes_t, experts)
    tokens = keys.shape[1]
    number = iota((experts, tokens), 0)
    share = jnp.zeros((experts, tokens), f32)
    for k in range(routes_t.shape[0]):
        share = share + jnp.where(routes_t[k : k + 1, :] == number, weight_t[k : k + 1, :], 0.0)
    slot = iota((capacity, tokens), 0).astype(f32)
    spread = [
        jnp.where(slot == keys[e : e + 1, :], share[e : e + 1, :], 0.0)
        for e in range(experts)
    ]
    same = ones_where(iota((tokens, tokens), 0) == iota((tokens, tokens), 1))
    for n, term in enumerate(split3(jnp.concatenate(spread, axis=0))):
        out_ref[n] = mm(same, term, NT).astype(bf16)


def fetch_kernel(*refs):
    count = (len(refs) - 1) // 2
    sems = refs[-1]
    copies = [
        pltpu.make_async_copy(refs[n], refs[count + n], sems.at[n]) for n in range(count)
    ]
    for copy in copies:
        copy.start()
    for copy in copies:
        copy.wait()


def combine_kernel(share_ref, back_ref, out_ref):
    back = back_ref[...]
    out = mm(share_ref[0], back) + (mm(share_ref[1], back) + mm(share_ref[2], back))
    out_ref[...] = out.astype(bf16)


def columns(source, which, feats):
    return source.at[0, :, pl.ds(pl.multiple_of(which * feats, feats), feats)]


def hidden_kernel(parts, senders, start, load, me_ref, *refs):
    packs = refs[:parts]
    blocks = refs[parts : 2 * parts]
    refs = refs[2 * parts :]
    if load:
        sources = refs[:3]
        hidden_ref, odd_ref, gate_ref, up_ref, down_ref, normed_ref, sems = refs[3:]
    else:
        gate_ref, up_ref, down_ref, hidden_ref, odd_ref, normed_ref = refs
    rows, units = hidden_ref.shape
    full, feats = blocks[0].shape
    width = parts * feats
    chunk = rows // senders
    me = me_ref[0]
    lead = packs[0].shape[1] - feats
    size = min(units, 256)
    unit_loads, down_loads = [], []
    if load:
        for n in range(units // size):
            cols = pl.ds(n * size, size)
            unit_loads.append([
                pltpu.make_async_copy(
                    source.at[0, :, cols], ref.at[0, :, cols], sems.at[m, n]
                )
                for m, (source, ref) in enumerate(zip(sources, (gate_ref, up_ref)))
            ])
        for n in range(odd_ref.shape[0]):
            down_loads.append(
                pltpu.make_async_copy(
                    columns(sources[2], me ^ (2 * n + 3), feats), down_ref.at[n], sems.at[2, n]
                )
            )
        for copy in sum(unit_loads, down_loads[:0]) + down_loads:
            copy.start()

    def body(sender, unused):
        here = pl.ds(pl.multiple_of(sender * chunk, chunk), chunk)
        there = pl.ds(pl.multiple_of(sender * (full // senders) + start, chunk), chunk)
        at = [there if k < 2 else here for k in range(parts)]
        total = jnp.zeros((chunk, 1), f32)
        square = jnp.zeros((chunk, 1), f32)
        for k, block in enumerate(blocks):
            wide = block[at[k], :].astype(f32)
            total = total + jnp.sum(wide, axis=1, keepdims=True)
            square = square + jnp.sum(wide * wide, axis=1, keepdims=True)
        mean = total / width
        scale = lax.rsqrt(square / width - mean * mean + norm_eps)
        for k, block in enumerate(blocks):
            gain = packs[k][:, lead:]
            value = (block[at[k], :].astype(f32) - mean) * scale * gain
            cols = pl.ds(pl.multiple_of((me ^ k) * feats, feats), feats)
            normed_ref[here, cols] = value.astype(bf16)
        return unused

    lax.fori_loop(0, senders, body, 0, unroll=4)
    for at in range(0, units, size):
        cols = pl.ds(at, size)
        for copy in unit_loads[at // size] if load else ():
            copy.wait()
        normed = normed_ref[...]
        gate = mm(normed, gate_ref[0, :, cols])
        up = mm(normed, up_ref[0, :, cols])
        hidden_ref[:, cols] = (gate * jax.nn.sigmoid(gate) * up).astype(bf16)
    for copy in down_loads:
        copy.wait()
    for n in range(odd_ref.shape[0]):
        odd_ref[n] = mm(hidden_ref[...], down_ref[n]).astype(bf16)


def rest_kernel(load, me_ref, hidden_ref, *refs):
    if load:
        source, even_ref, near_ref, own_ref, down_ref, sems = refs
    else:
        down_ref, even_ref, near_ref, own_ref = refs
    feats = near_ref.shape[1]
    outs = [even_ref.at[n] for n in range(even_ref.shape[0])] + [near_ref, own_ref]
    offsets = [2 * n + 2 for n in range(even_ref.shape[0])] + [1, 0]
    loads = []
    if load:
        for n, offset in enumerate(offsets):
            loads.append(
                pltpu.make_async_copy(
                    columns(source, me_ref[0] ^ offset, feats), down_ref.at[n], sems.at[n]
                )
            )
        for copy in loads:
            copy.start()
    for n, out in enumerate(outs):
        if load:
            loads[n].wait()
        out[...] = mm(hidden_ref[...], down_ref[n]).astype(bf16)


def join_kernel(count, senders, *refs):
    out_ref = refs[-1]
    terms = (len(refs) - 1) // count
    chunk = refs[0].shape[0] // senders
    for c in range(count):
        for e in range(senders):
            total = None
            for ref in refs[c * terms : (c + 1) * terms]:
                term = ref[pl.ds(e * chunk, chunk), :].astype(f32)
                total = term if total is None else total + term
            out_ref[pl.ds((e * count + c) * chunk, chunk), :] = total.astype(bf16)


def reorder(rows, back):
    steps = rows // LANES
    row, col = iota((rows, rows), 1 if back else 0), iota((rows, rows), 0 if back else 1)
    return ones_where(col == (row % LANES) * steps + row // LANES)


def in_line(table, width):
    states = table.shape[1]
    wide = spread_table(table, states, 1, states, width)
    return jnp.sum(wide, axis=0, keepdims=True)


def sin_cos(angle):
    turns = jnp.floor(angle * 0.6366197723675814 + 0.5)
    rest = angle - turns * 1.5703125
    rest = rest - turns * 4.83751296997070312e-4
    rest = rest - turns * 7.54978995489188e-8
    z = rest * rest
    sine = rest + rest * z * (
        -1.6666654611e-1 + z * (8.3321608736e-3 + z * -1.9515295891e-4)
    )
    cosine = 1.0 - 0.5 * z + z * z * (
        4.166664568298827e-2 + z * (-1.388731625493765e-3 + z * 2.443315711809948e-5)
    )
    quarter = turns.astype(jnp.int32)
    odd = (quarter & 1) != 0
    first = jnp.where(odd, cosine, sine)
    second = jnp.where(odd, sine, cosine)
    first = jnp.where((quarter & 2) != 0, -first, first)
    second = jnp.where(((quarter + 1) & 2) != 0, -second, second)
    return first, second


def spread_table(table, inner, outer_rows, outer_cols, width):
    rows = table.shape[0]
    pick = ones_where(iota((inner, width), 1) % inner == iota((inner, width), 0))
    high, mid, low = split3(table)
    wide = mm(high, pick) + (mm(mid, pick) + mm(low, pick))
    same = iota((rows, width), 0) // outer_rows == iota((rows, width), 1) // outer_cols
    return jnp.where(same, wide, 0.0)


def poles_kernel(step_ref, pr_ref, pi_ref, ar_ref, ai_ref, over_ref):
    groups, states = pr_ref.shape
    rows, flat = ar_ref.shape
    order = reorder(rows, False)
    poles_re = in_line(pr_ref[...], flat)
    poles_im = in_line(pi_ref[...], flat)
    size = poles_re * poles_re + poles_im * poles_im
    over_ref[0:1, :] = poles_re / size
    over_ref[1:2, :] = -poles_im / size
    d_high, d_mid, d_low = (
        mm(part, order, NT).astype(bf16) for part in split3(step_ref[...])
    )
    piece = min(flat, 256)
    for at in range(0, flat, piece):
        cols = pl.ds(at, piece)
        expand = ones_where(
            iota((groups, piece), 0) == (iota((groups, piece), 1) + at) // states
        )
        delta = mm(d_high, expand, TN) + (mm(d_mid, expand, TN) + mm(d_low, expand, TN))
        size = jnp.exp(poles_re[:, at : at + piece] * delta)
        sine, cosine = sin_cos(poles_im[:, at : at + piece] * delta)
        ar_ref[:, cols] = size * cosine
        ai_ref[:, cols] = size * sine


def scan_kernel(
    total, parts, x_ref, gain_ref, ar_ref, ai_ref, over_ref, ir_ref, ii_ref, *refs,
):
    packs = refs[:parts]
    h_re_out, h_im_out, c_re_out, c_im_out, end_ref = refs[parts : parts + 5]
    hr_ref, hi_ref, cr_ref, ci_ref, sems = refs[parts + 5 :]
    rows, feats = x_ref.shape
    flat = ar_ref.shape[1]
    states = ir_ref.shape[1]
    inner = feats // (flat // states)
    steps = rows // LANES
    order = reorder(rows, False)
    packed = packs[0][:, : 2 * rows]
    for other in packs[1:]:
        packed = packed + other[:, : 2 * rows]
    mean = packed[:, :rows] / total
    scale = lax.rsqrt(packed[:, rows:] / total - mean * mean + norm_eps)
    match = iota((rows, rows), 1) == (iota((rows, rows), 0) % LANES) * steps + iota(
        (rows, rows), 0
    ) // LANES
    mean_col = jnp.sum(jnp.where(match, mean, 0.0), axis=1, keepdims=True)
    scale_col = jnp.sum(jnp.where(match, scale, 0.0), axis=1, keepdims=True)
    cw = min(feats, 256)
    sw = cw // inner * states
    copies = []
    for b in range(feats // cw):
        chans = pl.ds(b * cw, cw)
        cols = pl.ds(b * sw, sw)
        rows_in = mm(order, x_ref[:, chans])
        normed = split2((rows_in - mean_col) * scale_col * gain_ref[:, chans])
        real = split2(spread_table(ir_ref[chans, :], states, inner, states, sw))
        imag = split2(spread_table(ii_ref[chans, :], states, inner, states, sw))
        hr_ref[:, cols], hi_ref[:, cols] = mul(
            mm3(normed, real, NN), mm3(normed, imag, NN), over_ref[0:1, cols], over_ref[1:2, cols]
        )

        def body(j, carry):
            h_re, h_im, c_re, c_im = carry
            here = pl.ds(pl.multiple_of(j * LANES, LANES), LANES)
            a_re, a_im = ar_ref[here, cols], ai_ref[here, cols]
            d_re, d_im = hr_ref[here, cols], hi_ref[here, cols]
            h_re, h_im = mul(a_re, a_im, h_re + d_re, h_im + d_im)
            h_re, h_im = h_re - d_re, h_im - d_im
            c_re, c_im = mul(a_re, a_im, c_re, c_im)
            hr_ref[here, cols], hi_ref[here, cols] = h_re, h_im
            cr_ref[here, cols], ci_ref[here, cols] = c_re, c_im
            return h_re, h_im, c_re, c_im

        zero = jnp.zeros((LANES, sw), f32)
        lax.fori_loop(0, steps, body, (zero, zero, zero + 1.0, zero), unroll=2)
        for n, (ref, out) in enumerate((
            (hr_ref, h_re_out), (hi_ref, h_im_out), (cr_ref, c_re_out), (ci_ref, c_im_out),
        )):
            copies.append(
                pltpu.make_async_copy(ref.at[:, cols], out.at[:, cols], sems.at[b, n])
            )
            copies[-1].start()
    last = pl.ds(rows - LANES, LANES)
    h_re, h_im, c_re, c_im = hr_ref[last, :], hi_ref[last, :], cr_ref[last, :], ci_ref[last, :]
    p_re, p_im = c_re[0:1], c_im[0:1]
    s_re, s_im = h_re[0:1], h_im[0:1]
    for c in range(1, LANES):
        k_re, k_im = c_re[c : c + 1], c_im[c : c + 1]
        p_re, p_im = mul(k_re, k_im, p_re, p_im)
        s_re, s_im = mul(k_re, k_im, s_re, s_im)
        s_re, s_im = s_re + h_re[c : c + 1], s_im + h_im[c : c + 1]
    ends = jnp.concatenate([p_re, p_im, s_re, s_im], axis=0)
    for i in range(end_ref.shape[0]):
        end_ref[i] = ends
    for copy in copies:
        copy.wait()


def read_kernel(
    me_ref, got_ref, h_re_in, h_im_in, c_re_in, c_im_in, rr_ref, ri_ref, out_ref,
    hr_ref, hi_ref, cr_ref, ci_ref, sems,
):
    rows, flat = hr_ref.shape
    feats = out_ref.shape[1]
    states = rr_ref.shape[1]
    inner = feats // (flat // states)
    steps = rows // LANES
    me = me_ref[0]
    cw = min(feats, 256)
    sw = cw // inner * states
    last = pl.ds(rows - LANES, LANES)
    pairs = ((h_re_in, hr_ref), (h_im_in, hi_ref), (c_re_in, cr_ref), (c_im_in, ci_ref))
    loads = []
    for b in range(feats // cw):
        cols = pl.ds(b * sw, sw)
        loads.append([
            pltpu.make_async_copy(src.at[:, cols], ref.at[:, cols], sems.at[b, n])
            for n, (src, ref) in enumerate(pairs)
        ])
        for copy in loads[-1]:
            copy.start()
    s_re = jnp.zeros((1, flat), f32)
    s_im = jnp.zeros((1, flat), f32)
    for i in range(got_ref.shape[0] - 1):
        ends = got_ref[i]
        n_re, n_im = mul(ends[0:1], ends[1:2], s_re, s_im)
        s_re = jnp.where(i < me, n_re + ends[2:3], s_re)
        s_im = jnp.where(i < me, n_im + ends[3:4], s_im)
    back = reorder(rows, True)
    for b in range(feats // cw):
        chans = pl.ds(b * cw, cw)
        lo = b * sw
        cols = pl.ds(lo, sw)
        real = split2(spread_table(rr_ref[chans, :], states, inner, states, sw))
        imag = split2(spread_table(ri_ref[chans, :], states, inner, states, sw))
        for copy in loads[b]:
            copy.wait()
        h_re, h_im, c_re, c_im = (
            ref[last, cols] for ref in (hr_ref, hi_ref, cr_ref, ci_ref)
        )
        in_re, in_im = [s_re[:, lo : lo + sw]], [s_im[:, lo : lo + sw]]
        for c in range(LANES - 1):
            n_re, n_im = mul(c_re[c : c + 1], c_im[c : c + 1], in_re[-1], in_im[-1])
            in_re.append(n_re + h_re[c : c + 1])
            in_im.append(n_im + h_im[c : c + 1])
        g_re = jnp.concatenate(in_re, axis=0)[None]
        g_im = jnp.concatenate(in_im, axis=0)[None]
        shape = (steps, LANES, sw)
        c_re, c_im = cr_ref[:, cols].reshape(shape), ci_ref[:, cols].reshape(shape)
        f_re = hr_ref[:, cols].reshape(shape) + (c_re * g_re - c_im * g_im)
        f_im = hi_ref[:, cols].reshape(shape) + (c_re * g_im + c_im * g_re)
        response = mm3(split2(f_re.reshape(rows, sw)), real, NT) - mm3(
            split2(f_im.reshape(rows, sw)), imag, NT
        )
        cube = response + 0.044715 * (response * response * response)
        mixed = 0.5 * response * (1.0 + jnp.tanh(0.7978845608028654 * cube))
        out_ref[:, chans] = mm(back, mixed.astype(bf16)).astype(bf16)


def output_kernel(parts, me_ref, *refs):
    pieces = refs[:parts]
    value_ref, gate_ref, out_ref = refs[parts:]
    feats = pieces[0].shape[1]
    value = gate = None
    for k, piece in enumerate(pieces):
        at = pl.ds(pl.multiple_of((me_ref[0] ^ k) * feats, feats), feats)
        rows = piece[...]
        v, g = mm(rows, value_ref[at, :]), mm(rows, gate_ref[at, :])
        value, gate = (v, g) if value is None else (value + v, gate + g)
    out_ref[...] = (value * jax.nn.sigmoid(gate)).astype(bf16)


vmem = pl.BlockSpec(memory_space=pltpu.VMEM)
hbm = pl.BlockSpec(memory_space=pltpu.HBM)
smem = pl.BlockSpec(memory_space=pltpu.SMEM)


def stay(value):
    return pltpu.with_memory_space_constraint(value, pltpu.HBM)


def params(mib):
    return pltpu.CompilerParams(vmem_limit_bytes=mib << 20)


def swap(value, bit):
    count = lax.axis_size("tp")
    return lax.ppermute(value, "tp", [(i, i ^ bit) for i in range(count)])


def gather_tp(value):
    count = lax.axis_size("tp")
    blocks = {0: value}
    bit = count // 2
    while bit >= 1:
        blocks.update({k ^ bit: swap(block, bit) for k, block in list(blocks.items())})
        bit //= 2
    return [blocks[k] for k in range(count)]


def shards(
    mixer_input, mixer_gain, time_step, pole_real, pole_imag, input_real, input_imag,
    read_real, read_imag, out_value, out_gate, expert_input, expert_gain, routes,
    route_weight, expert_gate, expert_up, expert_down,
):
    n_tp, n_ep = lax.axis_size("tp"), lax.axis_size("ep")
    tp_at = lax.axis_index("tp").astype(jnp.int32).reshape(1)
    ep_at = lax.axis_index("ep").astype(jnp.int32).reshape(1)
    tokens, feats = expert_input.shape
    top = routes.shape[1]
    capacity = 2 * top * tokens // n_ep
    slots = n_ep * capacity
    routes_t = routes.T
    weight_t = route_weight.T

    rows, chans = mixer_input.shape
    send, packed = pl.pallas_call(
        functools.partial(send_kernel, n_ep, capacity),
        out_shape=(
            jax.ShapeDtypeStruct((slots, feats), bf16),
            jax.ShapeDtypeStruct((1, 2 * rows + feats), f32),
        ),
        in_specs=[vmem] * 4, out_specs=(vmem, vmem), compiler_params=params(8),
        name="send_rows",
    )(
        stay(routes_t), stay(expert_input), stay(mixer_input),
        stay(expert_gain.reshape(1, feats)),
    )
    arrived = lax.all_to_all(send, "ep", split_axis=0, concat_axis=0, tiled=True)
    packed, tp_at, ep_at = lax.optimization_barrier((packed, tp_at, ep_at))
    packs = gather_tp(packed)

    groups, states = pole_real.shape
    flat = groups * states
    big = jax.ShapeDtypeStruct((rows, flat), f32)
    a_re, a_im, over = pl.pallas_call(
        poles_kernel,
        out_shape=(big, big, jax.ShapeDtypeStruct((2, flat), f32)),
        in_specs=[vmem] * 3, out_specs=(vmem,) * 3, compiler_params=params(20),
        name="mixer_poles",
    )(stay(time_step.T), stay(pole_real), stay(pole_imag))
    n_block = max(1, chans // 256)
    far_big = pltpu.HBM((rows, flat), f32)
    *carried, ends = pl.pallas_call(
        functools.partial(scan_kernel, float(chans * n_tp), n_tp),
        out_shape=(far_big,) * 4 + (jax.ShapeDtypeStruct((n_ep, 4, flat), f32),),
        in_specs=[vmem] * (7 + n_tp), out_specs=(hbm,) * 4 + (vmem,),
        scratch_shapes=[pltpu.VMEM((rows, flat), f32)] * 4
        + [pltpu.SemaphoreType.DMA((n_block, 4))],
        compiler_params=params(24), name="mixer_scan",
    )(
        stay(mixer_input), stay(mixer_gain.reshape(1, chans)), a_re, a_im, over,
        stay(jnp.swapaxes(input_real, 1, 2).reshape(chans, states)),
        stay(jnp.swapaxes(input_imag, 1, 2).reshape(chans, states)),
        *packs,
    )
    n_half = 2 if capacity % 32 == 0 else 1
    half = capacity // n_half
    share = pl.pallas_call(
        functools.partial(share_kernel, n_ep, capacity),
        out_shape=jax.ShapeDtypeStruct((3, tokens, slots), bf16),
        in_specs=[vmem, vmem], out_specs=vmem, compiler_params=params(8), name="route_share",
    )(stay(routes_t), stay(weight_t))
    got = lax.all_to_all(ends, "ep", split_axis=0, concat_axis=0)

    units = expert_gate.shape[2]
    n_far = n_tp // 2 - 1
    part = n_ep * half
    by_sender = arrived.reshape(n_ep, capacity, feats)
    halves = [by_sender[:, c * half : (c + 1) * half].reshape(part, feats) for c in range(n_half)]
    far_blocks = []
    for c in range(n_half):
        evens = {0: halves[c]}
        bit = n_tp // 2
        while bit > 1:
            evens.update({k ^ bit: swap(b, bit) for k, b in list(evens.items())})
            bit //= 2
        far_blocks.append(evens)
    partner = swap(arrived, 1)

    def fetch(*weights):
        return pl.pallas_call(
            fetch_kernel,
            out_shape=tuple(jax.ShapeDtypeStruct(w.shape, w.dtype) for w in weights),
            in_specs=[hbm] * len(weights), out_specs=(vmem,) * len(weights),
            scratch_shapes=[pltpu.SemaphoreType.DMA((len(weights),))],
            compiler_params=params(10),
        )(*(stay(w) for w in weights))

    weights = (stay(expert_gate), stay(expert_up), stay(expert_down))
    down_rest = weights[2]
    n_unit = max(1, units // 256)
    n_rest = n_far + 2
    terms = []
    for c in range(n_half):
        blocks = [arrived, partner]
        for k in range(2, n_tp, 2):
            blocks += [far_blocks[c][k], swap(far_blocks[c][k], 1)]
        far_shape = jax.ShapeDtypeStruct((n_far, part, feats), bf16)
        part_shape = jax.ShapeDtypeStruct((part, feats), bf16)
        load = c == 0
        kept = [jax.ShapeDtypeStruct(w.shape, bf16) for w in (expert_gate, expert_up)]
        kept = kept + [jax.ShapeDtypeStruct((n_far, units, feats), bf16)] if load else []
        hidden, odd_far, *held = pl.pallas_call(
            functools.partial(hidden_kernel, n_tp, n_ep, c * half, load),
            in_specs=[smem] + [vmem] * (2 * n_tp) + [hbm if load else vmem] * 3,
            out_specs=(vmem,) * (2 + len(kept)),
            scratch_shapes=[pltpu.VMEM((part, n_tp * feats), bf16)]
            + ([pltpu.SemaphoreType.DMA((3, max(n_unit, n_far)))] if load else []),
            out_shape=(jax.ShapeDtypeStruct((part, units), bf16), far_shape, *kept),
            compiler_params=params(12),
        )(tp_at, *packs, *blocks, *weights)
        weights = held or weights
        theirs = swap(odd_far, 1)
        kept = [jax.ShapeDtypeStruct((n_rest, units, feats), bf16)] if load else []
        even_far, near, own, *held = pl.pallas_call(
            functools.partial(rest_kernel, load),
            in_specs=[smem, vmem, hbm if load else vmem],
            out_specs=(vmem,) * (3 + len(kept)),
            scratch_shapes=[pltpu.SemaphoreType.DMA((n_rest,))] if load else [],
            out_shape=(far_shape, part_shape, part_shape, *kept),
            compiler_params=params(8),
        )(tp_at, hidden, down_rest)
        down_rest = held[0] if held else down_rest
        far = even_far.astype(f32) + theirs.astype(f32)
        terms += [own, swap(near, 1)]
        bit = n_tp // 4
        while bit >= 1:
            come = swap(far[bit - 1 :].astype(bf16), 2 * bit)
            terms.append(come[0])
            far = far[: bit - 1] + come[1:].astype(f32)
            bit //= 2
    result = pl.pallas_call(
        functools.partial(join_kernel, n_half, n_ep),
        out_shape=jax.ShapeDtypeStruct((slots, feats), bf16),
        in_specs=[vmem] * len(terms), out_specs=vmem, compiler_params=params(8),
        name="expert_join",
    )(*terms)
    back = lax.all_to_all(result, "ep", split_axis=0, concat_axis=0, tiled=True)

    mixed = pl.pallas_call(
        read_kernel,
        out_shape=jax.ShapeDtypeStruct((rows, chans), bf16),
        in_specs=[smem, vmem] + [hbm] * 4 + [vmem] * 2, out_specs=vmem,
        scratch_shapes=[pltpu.VMEM((rows, flat), f32)] * 4
        + [pltpu.SemaphoreType.DMA((n_block, 4))],
        compiler_params=params(20), name="mixer_read",
    )(
        ep_at, got, *(stay(x) for x in carried),
        stay(read_real.reshape(chans, states)), stay(read_imag.reshape(chans, states)),
    )
    pieces = gather_tp(mixed)
    value_w, gate_w = fetch(out_value, out_gate)
    mixer_output = pl.pallas_call(
        functools.partial(output_kernel, n_tp),
        out_shape=jax.ShapeDtypeStruct((rows, out_value.shape[1]), bf16),
        in_specs=[smem] + [vmem] * (n_tp + 2), out_specs=vmem, compiler_params=params(10),
        name="mixer_out",
    )(tp_at, *pieces, value_w, gate_w)
    expert_output = pl.pallas_call(
        combine_kernel,
        out_shape=jax.ShapeDtypeStruct((tokens, feats), bf16),
        in_specs=[vmem] * 2, out_specs=vmem, compiler_params=params(8), name="combine",
    )(share, back)
    return mixer_output, expert_output


def solution(mesh):
    return jax.shard_map(
        shards,
        mesh=mesh,
        in_specs=(
            P("ep", "tp"), P("tp"), P("ep", "tp"), P("tp", None), P("tp", None),
            P("tp", None, None), P("tp", None, None), P("tp", None, None), P("tp", None, None),
            P(None, "tp"), P(None, "tp"), P("ep", "tp"), P("tp"), P("ep", None), P("ep", None),
            P("ep", None, "tp"), P("ep", None, "tp"), P("ep", "tp", None),
        ),
        out_specs=(P("ep", "tp"), P("ep", "tp")),
        check_vma=False,
    )
```

```python
import functools

import jax
import jax.numpy as jnp
from jax import lax
from jax.experimental import pallas as pl
from jax.experimental.pallas import tpu as pltpu
from jax.sharding import PartitionSpec as P


f32 = jnp.float32
bf16 = jnp.bfloat16
norm_eps = 1e-05
LANES = 8
NN = (((1,), (0,)), ((), ()))
NT = (((1,), (1,)), ((), ()))
TN = (((0,), (0,)), ((), ()))


def iota(shape, dim):
    return lax.broadcasted_iota(jnp.int32, shape, dim)


def ones_where(mask):
    return jnp.where(mask, 1.0, 0.0).astype(bf16)


def split2(value):
    high = value.astype(bf16)
    return high, (value - high.astype(f32)).astype(bf16)


def split3(value):
    high = value.astype(bf16)
    rest = value - high.astype(f32)
    mid = rest.astype(bf16)
    return high, mid, (rest - mid.astype(f32)).astype(bf16)


def mm(left, right, dims=NN):
    return lax.dot_general(left, right, dims, preferred_element_type=f32)


def mm3(left, right, dims):
    lh, ll = left
    rh, rl = right
    return mm(lh, rh, dims) + (mm(ll, rh, dims) + mm(lh, rl, dims))


def mul(ar, ai, br, bi):
    return ar * br - ai * bi, ar * bi + ai * br


def slot_keys(routes_t, experts):
    top, tokens = routes_t.shape
    number = iota((experts, tokens), 0)
    hit = routes_t[0:1, :] == number
    for k in range(1, top):
        hit = hit | (routes_t[k : k + 1, :] == number)
    before = ones_where(iota((tokens, tokens), 0) < iota((tokens, tokens), 1))
    place = mm(ones_where(hit), before)
    return jnp.where(hit, place, -1.0)


def send_kernel(
    experts, capacity, routes_ref, rows_ref, x_hbm, gain_ref, out_hbm, sums_ref,
    x_ref, out_ref, sems,
):
    come = pltpu.make_async_copy(x_hbm, x_ref, sems.at[0])
    leave = pltpu.make_async_copy(out_ref, out_hbm, sems.at[1])
    come.start()
    keys = slot_keys(routes_ref[...], experts)
    tokens = keys.shape[1]
    slot = iota((capacity, tokens), 0).astype(f32)
    chosen = [ones_where(slot == keys[e : e + 1, :]) for e in range(experts)]
    out_ref[...] = mm(jnp.concatenate(chosen, axis=0), rows_ref[...]).astype(bf16)
    leave.start()
    come.wait()
    rows = x_ref[...]
    count = rows.shape[0]
    ones = jnp.ones((8, rows.shape[1]), bf16)
    wide = rows.astype(f32)
    high, low = split2(wide * wide)
    sums_ref[:, :count] = mm(ones, rows, NT)[0:1]
    sums_ref[:, count : 2 * count] = (mm(ones, high, NT) + mm(ones, low, NT))[0:1]
    sums_ref[:, 2 * count :] = gain_ref[...]
    leave.wait()


def share_kernel(experts, capacity, routes_ref, weight_ref, out_ref):
    routes_t = routes_ref[...]
    weight_t = weight_ref[...]
    keys = slot_keys(routes_t, experts)
    tokens = keys.shape[1]
    number = iota((experts, tokens), 0)
    share = jnp.zeros((experts, tokens), f32)
    for k in range(routes_t.shape[0]):
        share = share + jnp.where(routes_t[k : k + 1, :] == number, weight_t[k : k + 1, :], 0.0)
    slot = iota((capacity, tokens), 0).astype(f32)
    spread = [
        jnp.where(slot == keys[e : e + 1, :], share[e : e + 1, :], 0.0)
        for e in range(experts)
    ]
    same = ones_where(iota((tokens, tokens), 0) == iota((tokens, tokens), 1))
    for n, term in enumerate(split3(jnp.concatenate(spread, axis=0))):
        out_ref[n] = mm(same, term, NT).astype(bf16)


def fetch_kernel(*refs):
    count = (len(refs) - 1) // 2
    sems = refs[-1]
    copies = [
        pltpu.make_async_copy(refs[n], refs[count + n], sems.at[n]) for n in range(count)
    ]
    for copy in copies:
        copy.start()
    for copy in copies:
        copy.wait()


def combine_kernel(share_ref, back_ref, out_ref):
    back = back_ref[...]
    out = mm(share_ref[0], back) + (mm(share_ref[1], back) + mm(share_ref[2], back))
    out_ref[...] = out.astype(bf16)


def first_kernel(*refs):
    count = (len(refs) - 1) // 2
    sems = refs[-1]
    copies = []
    for n in range(count):
        out = refs[count + n]
        copies.append(
            pltpu.make_async_copy(
                refs[n].at[0, :, pl.ds(0, out.shape[1])], out, sems.at[n]
            )
        )
        copies[-1].start()
    for copy in copies:
        copy.wait()


def hidden_kernel(parts, senders, start, load, me_ref, *refs):
    packs = refs[:parts]
    blocks = refs[parts : 2 * parts]
    firsts = refs[2 * parts : 2 * parts + 2]
    refs = refs[2 * parts + 2 :]
    if load:
        sources = refs[:3]
        hidden_ref, odd_ref, gate_ref, up_ref, down_ref, normed_ref, sems = refs[3:]
    else:
        gate_ref, up_ref, down_ref, hidden_ref, odd_ref, normed_ref = refs
    rows, units = hidden_ref.shape
    full, feats = blocks[0].shape
    width = parts * feats
    chunk = rows // senders
    me = me_ref[0]
    lead = packs[0].shape[1] - feats
    middle = firsts[0].shape[1]
    size = min(middle, 256)
    loads = []
    if load:
        for n in range((units - middle) // size):
            cols = pl.ds(n * size, size)
            loads.append([
                pltpu.make_async_copy(
                    source.at[0, :, pl.ds(middle + n * size, size)], ref.at[:, cols],
                    sems.at[m, n],
                )
                for m, (source, ref) in enumerate(zip(sources, (gate_ref, up_ref)))
            ])
        loads.append([pltpu.make_async_copy(sources[2], down_ref, sems.at[2, 0])])
        for group in loads:
            for copy in group:
                copy.start()

    def body(sender, unused):
        here = pl.ds(pl.multiple_of(sender * chunk, chunk), chunk)
        there = pl.ds(pl.multiple_of(sender * (full // senders) + start, chunk), chunk)
        at = [there if k < 2 else here for k in range(parts)]
        total = jnp.zeros((chunk, 1), f32)
        square = jnp.zeros((chunk, 1), f32)
        for k, block in enumerate(blocks):
            wide = block[at[k], :].astype(f32)
            total = total + jnp.sum(wide, axis=1, keepdims=True)
            square = square + jnp.sum(wide * wide, axis=1, keepdims=True)
        mean = total / width
        scale = lax.rsqrt(square / width - mean * mean + norm_eps)
        for k, block in enumerate(blocks):
            gain = packs[k][:, lead:]
            value = (block[at[k], :].astype(f32) - mean) * scale * gain
            cols = pl.ds(pl.multiple_of((me ^ k) * feats, feats), feats)
            normed_ref[here, cols] = value.astype(bf16)
        return unused

    lax.fori_loop(0, senders, body, 0, unroll=4)
    for at in range(0, units, size):
        tables, where = (firsts, at) if at < middle else ((gate_ref, up_ref), at - middle)
        if load and at >= middle:
            for copy in loads[where // size]:
                copy.wait()
        normed = normed_ref[...]
        gate = mm(normed, tables[0][:, pl.ds(where, size)])
        up = mm(normed, tables[1][:, pl.ds(where, size)])
        hidden_ref[:, pl.ds(at, size)] = (gate * jax.nn.sigmoid(gate) * up).astype(bf16)
    if load:
        loads[-1][0].wait()
    for n in range(odd_ref.shape[0]):
        odd_ref[n] = down_part(me ^ (2 * n + 3), hidden_ref, down_ref, feats)


def down_part(which, hidden_ref, weight_ref, feats):
    cols = pl.ds(pl.multiple_of(which * feats, feats), feats)
    return mm(hidden_ref[...], weight_ref[0, :, cols]).astype(bf16)


def rest_kernel(me_ref, hidden_ref, down_ref, even_ref, near_ref, own_ref):
    me = me_ref[0]
    feats = near_ref.shape[1]
    for n in range(even_ref.shape[0]):
        even_ref[n] = down_part(me ^ (2 * n + 2), hidden_ref, down_ref, feats)
    near_ref[...] = down_part(me ^ 1, hidden_ref, down_ref, feats)
    own_ref[...] = down_part(me, hidden_ref, down_ref, feats)


def join_kernel(count, senders, *refs):
    out_ref = refs[-1]
    terms = (len(refs) - 1) // count
    chunk = refs[0].shape[0] // senders
    for c in range(count):
        for e in range(senders):
            total = None
            for ref in refs[c * terms : (c + 1) * terms]:
                term = ref[pl.ds(e * chunk, chunk), :].astype(f32)
                total = term if total is None else total + term
            out_ref[pl.ds((e * count + c) * chunk, chunk), :] = total.astype(bf16)


def reorder(rows, back):
    steps = rows // LANES
    row, col = iota((rows, rows), 1 if back else 0), iota((rows, rows), 0 if back else 1)
    return ones_where(col == (row % LANES) * steps + row // LANES)


def in_line(table, width):
    states = table.shape[1]
    wide = spread_table(table, states, 1, states, width)
    return jnp.sum(wide, axis=0, keepdims=True)


def sin_cos(angle):
    turns = jnp.floor(angle * 0.6366197723675814 + 0.5)
    rest = angle - turns * 1.5703125
    rest = rest - turns * 4.83751296997070312e-4
    rest = rest - turns * 7.54978995489188e-8
    z = rest * rest
    sine = rest + rest * z * (
        -1.6666654611e-1 + z * (8.3321608736e-3 + z * -1.9515295891e-4)
    )
    cosine = 1.0 - 0.5 * z + z * z * (
        4.166664568298827e-2 + z * (-1.388731625493765e-3 + z * 2.443315711809948e-5)
    )
    quarter = turns.astype(jnp.int32)
    odd = (quarter & 1) != 0
    first = jnp.where(odd, cosine, sine)
    second = jnp.where(odd, sine, cosine)
    first = jnp.where((quarter & 2) != 0, -first, first)
    second = jnp.where(((quarter + 1) & 2) != 0, -second, second)
    return first, second


def spread_table(table, inner, outer_rows, outer_cols, width):
    rows = table.shape[0]
    pick = ones_where(iota((inner, width), 1) % inner == iota((inner, width), 0))
    high, mid, low = split3(table)
    wide = mm(high, pick) + (mm(mid, pick) + mm(low, pick))
    same = iota((rows, width), 0) // outer_rows == iota((rows, width), 1) // outer_cols
    return jnp.where(same, wide, 0.0)


def poles_kernel(step_ref, pr_ref, pi_ref, ar_ref, ai_ref, over_ref):
    groups, states = pr_ref.shape
    rows, flat = ar_ref.shape
    order = reorder(rows, False)
    poles_re = in_line(pr_ref[...], flat)
    poles_im = in_line(pi_ref[...], flat)
    size = poles_re * poles_re + poles_im * poles_im
    over_ref[0:1, :] = poles_re / size
    over_ref[1:2, :] = -poles_im / size
    d_high, d_mid, d_low = (
        mm(part, order, NT).astype(bf16) for part in split3(step_ref[...])
    )
    piece = min(flat, 256)
    for at in range(0, flat, piece):
        cols = pl.ds(at, piece)
        expand = ones_where(
            iota((groups, piece), 0) == (iota((groups, piece), 1) + at) // states
        )
        delta = mm(d_high, expand, TN) + (mm(d_mid, expand, TN) + mm(d_low, expand, TN))
        size = jnp.exp(poles_re[:, at : at + piece] * delta)
        sine, cosine = sin_cos(poles_im[:, at : at + piece] * delta)
        ar_ref[:, cols] = size * cosine
        ai_ref[:, cols] = size * sine


def scan_kernel(
    total, parts, x_ref, gain_ref, ar_ref, ai_ref, over_ref, ir_ref, ii_ref, *refs,
):
    packs = refs[:parts]
    h_re_out, h_im_out, c_re_out, c_im_out, end_ref = refs[parts : parts + 5]
    hr_ref, hi_ref, cr_ref, ci_ref, sems = refs[parts + 5 :]
    rows, feats = x_ref.shape
    flat = ar_ref.shape[1]
    states = ir_ref.shape[1]
    inner = feats // (flat // states)
    steps = rows // LANES
    order = reorder(rows, False)
    packed = packs[0][:, : 2 * rows]
    for other in packs[1:]:
        packed = packed + other[:, : 2 * rows]
    mean = packed[:, :rows] / total
    scale = lax.rsqrt(packed[:, rows:] / total - mean * mean + norm_eps)
    match = iota((rows, rows), 1) == (iota((rows, rows), 0) % LANES) * steps + iota(
        (rows, rows), 0
    ) // LANES
    mean_col = jnp.sum(jnp.where(match, mean, 0.0), axis=1, keepdims=True)
    scale_col = jnp.sum(jnp.where(match, scale, 0.0), axis=1, keepdims=True)
    cw = min(feats, 256)
    sw = cw // inner * states
    copies = []
    for b in range(feats // cw):
        chans = pl.ds(b * cw, cw)
        cols = pl.ds(b * sw, sw)
        rows_in = mm(order, x_ref[:, chans])
        normed = split2((rows_in - mean_col) * scale_col * gain_ref[:, chans])
        real = split2(spread_table(ir_ref[chans, :], states, inner, states, sw))
        imag = split2(spread_table(ii_ref[chans, :], states, inner, states, sw))
        hr_ref[:, cols], hi_ref[:, cols] = mul(
            mm3(normed, real, NN), mm3(normed, imag, NN), over_ref[0:1, cols], over_ref[1:2, cols]
        )

        def body(j, carry):
            h_re, h_im, c_re, c_im = carry
            here = pl.ds(pl.multiple_of(j * LANES, LANES), LANES)
            a_re, a_im = ar_ref[here, cols], ai_ref[here, cols]
            d_re, d_im = hr_ref[here, cols], hi_ref[here, cols]
            h_re, h_im = mul(a_re, a_im, h_re + d_re, h_im + d_im)
            h_re, h_im = h_re - d_re, h_im - d_im
            c_re, c_im = mul(a_re, a_im, c_re, c_im)
            hr_ref[here, cols], hi_ref[here, cols] = h_re, h_im
            cr_ref[here, cols], ci_ref[here, cols] = c_re, c_im
            return h_re, h_im, c_re, c_im

        zero = jnp.zeros((LANES, sw), f32)
        lax.fori_loop(0, steps, body, (zero, zero, zero + 1.0, zero), unroll=2)
        for n, (ref, out) in enumerate((
            (hr_ref, h_re_out), (hi_ref, h_im_out), (cr_ref, c_re_out), (ci_ref, c_im_out),
        )):
            copies.append(
                pltpu.make_async_copy(ref.at[:, cols], out.at[:, cols], sems.at[b, n])
            )
            copies[-1].start()
    last = pl.ds(rows - LANES, LANES)
    h_re, h_im, c_re, c_im = hr_ref[last, :], hi_ref[last, :], cr_ref[last, :], ci_ref[last, :]
    p_re, p_im = c_re[0:1], c_im[0:1]
    s_re, s_im = h_re[0:1], h_im[0:1]
    for c in range(1, LANES):
        k_re, k_im = c_re[c : c + 1], c_im[c : c + 1]
        p_re, p_im = mul(k_re, k_im, p_re, p_im)
        s_re, s_im = mul(k_re, k_im, s_re, s_im)
        s_re, s_im = s_re + h_re[c : c + 1], s_im + h_im[c : c + 1]
    ends = jnp.concatenate([p_re, p_im, s_re, s_im], axis=0)
    for i in range(end_ref.shape[0]):
        end_ref[i] = ends
    for copy in copies:
        copy.wait()


def read_kernel(
    me_ref, got_ref, h_re_in, h_im_in, c_re_in, c_im_in, rr_ref, ri_ref, out_ref,
    hr_ref, hi_ref, cr_ref, ci_ref, sems,
):
    rows, flat = hr_ref.shape
    feats = out_ref.shape[1]
    states = rr_ref.shape[1]
    inner = feats // (flat // states)
    steps = rows // LANES
    me = me_ref[0]
    cw = min(feats, 256)
    sw = cw // inner * states
    last = pl.ds(rows - LANES, LANES)
    pairs = ((h_re_in, hr_ref), (h_im_in, hi_ref), (c_re_in, cr_ref), (c_im_in, ci_ref))
    loads = []
    for b in range(feats // cw):
        cols = pl.ds(b * sw, sw)
        loads.append([
            pltpu.make_async_copy(src.at[:, cols], ref.at[:, cols], sems.at[b, n])
            for n, (src, ref) in enumerate(pairs)
        ])
        for copy in loads[-1]:
            copy.start()
    s_re = jnp.zeros((1, flat), f32)
    s_im = jnp.zeros((1, flat), f32)
    for i in range(got_ref.shape[0] - 1):
        ends = got_ref[i]
        n_re, n_im = mul(ends[0:1], ends[1:2], s_re, s_im)
        s_re = jnp.where(i < me, n_re + ends[2:3], s_re)
        s_im = jnp.where(i < me, n_im + ends[3:4], s_im)
    back = reorder(rows, True)
    for b in range(feats // cw):
        chans = pl.ds(b * cw, cw)
        lo = b * sw
        cols = pl.ds(lo, sw)
        real = split2(spread_table(rr_ref[chans, :], states, inner, states, sw))
        imag = split2(spread_table(ri_ref[chans, :], states, inner, states, sw))
        for copy in loads[b]:
            copy.wait()
        h_re, h_im, c_re, c_im = (
            ref[last, cols] for ref in (hr_ref, hi_ref, cr_ref, ci_ref)
        )
        in_re, in_im = [s_re[:, lo : lo + sw]], [s_im[:, lo : lo + sw]]
        for c in range(LANES - 1):
            n_re, n_im = mul(c_re[c : c + 1], c_im[c : c + 1], in_re[-1], in_im[-1])
            in_re.append(n_re + h_re[c : c + 1])
            in_im.append(n_im + h_im[c : c + 1])
        g_re = jnp.concatenate(in_re, axis=0)[None]
        g_im = jnp.concatenate(in_im, axis=0)[None]
        shape = (steps, LANES, sw)
        c_re, c_im = cr_ref[:, cols].reshape(shape), ci_ref[:, cols].reshape(shape)
        f_re = hr_ref[:, cols].reshape(shape) + (c_re * g_re - c_im * g_im)
        f_im = hi_ref[:, cols].reshape(shape) + (c_re * g_im + c_im * g_re)
        response = mm3(split2(f_re.reshape(rows, sw)), real, NT) - mm3(
            split2(f_im.reshape(rows, sw)), imag, NT
        )
        cube = response + 0.044715 * (response * response * response)
        mixed = 0.5 * response * (1.0 + jnp.tanh(0.7978845608028654 * cube))
        out_ref[:, chans] = mm(back, mixed.astype(bf16)).astype(bf16)


def output_kernel(parts, me_ref, *refs):
    pieces = refs[:parts]
    value_ref, gate_ref, out_ref = refs[parts:]
    feats = pieces[0].shape[1]
    value = gate = None
    for k, piece in enumerate(pieces):
        at = pl.ds(pl.multiple_of((me_ref[0] ^ k) * feats, feats), feats)
        rows = piece[...]
        v, g = mm(rows, value_ref[at, :]), mm(rows, gate_ref[at, :])
        value, gate = (v, g) if value is None else (value + v, gate + g)
    out_ref[...] = (value * jax.nn.sigmoid(gate)).astype(bf16)


vmem = pl.BlockSpec(memory_space=pltpu.VMEM)
hbm = pl.BlockSpec(memory_space=pltpu.HBM)
smem = pl.BlockSpec(memory_space=pltpu.SMEM)


def stay(value):
    return pltpu.with_memory_space_constraint(value, pltpu.HBM)


def params(mib):
    return pltpu.CompilerParams(vmem_limit_bytes=mib << 20)


def swap(value, bit):
    count = lax.axis_size("tp")
    return lax.ppermute(value, "tp", [(i, i ^ bit) for i in range(count)])


def gather_tp(value):
    count = lax.axis_size("tp")
    blocks = {0: value}
    bit = count // 2
    while bit >= 1:
        blocks.update({k ^ bit: swap(block, bit) for k, block in list(blocks.items())})
        bit //= 2
    return [blocks[k] for k in range(count)]


def shards(
    mixer_input, mixer_gain, time_step, pole_real, pole_imag, input_real, input_imag,
    read_real, read_imag, out_value, out_gate, expert_input, expert_gain, routes,
    route_weight, expert_gate, expert_up, expert_down,
):
    n_tp, n_ep = lax.axis_size("tp"), lax.axis_size("ep")
    tp_at = lax.axis_index("tp").astype(jnp.int32).reshape(1)
    ep_at = lax.axis_index("ep").astype(jnp.int32).reshape(1)
    tokens, feats = expert_input.shape
    top = routes.shape[1]
    capacity = 2 * top * tokens // n_ep
    slots = n_ep * capacity
    routes_t = routes.T
    weight_t = route_weight.T

    rows, chans = mixer_input.shape
    send, packed = pl.pallas_call(
        functools.partial(send_kernel, n_ep, capacity),
        out_shape=(
            pltpu.HBM((slots, feats), bf16),
            jax.ShapeDtypeStruct((1, 2 * rows + feats), f32),
        ),
        in_specs=[vmem, vmem, hbm, vmem], out_specs=(hbm, vmem),
        scratch_shapes=[
            pltpu.VMEM((rows, chans), bf16), pltpu.VMEM((slots, feats), bf16),
            pltpu.SemaphoreType.DMA((2,)),
        ],
        compiler_params=params(8), name="send_rows",
    )(
        stay(routes_t), stay(expert_input), stay(mixer_input),
        stay(expert_gain.reshape(1, feats)),
    )
    arrived = lax.all_to_all(send, "ep", split_axis=0, concat_axis=0, tiled=True)
    packed, tp_at, ep_at = lax.optimization_barrier((packed, tp_at, ep_at))
    packs = gather_tp(packed)

    groups, states = pole_real.shape
    flat = groups * states
    big = jax.ShapeDtypeStruct((rows, flat), f32)
    a_re, a_im, over = pl.pallas_call(
        poles_kernel,
        out_shape=(big, big, jax.ShapeDtypeStruct((2, flat), f32)),
        in_specs=[vmem] * 3, out_specs=(vmem,) * 3, compiler_params=params(20),
        name="mixer_poles",
    )(stay(time_step.T), stay(pole_real), stay(pole_imag))
    n_block = max(1, chans // 256)
    far_big = pltpu.HBM((rows, flat), f32)
    *carried, ends = pl.pallas_call(
        functools.partial(scan_kernel, float(chans * n_tp), n_tp),
        out_shape=(far_big,) * 4 + (jax.ShapeDtypeStruct((n_ep, 4, flat), f32),),
        in_specs=[vmem] * (7 + n_tp), out_specs=(hbm,) * 4 + (vmem,),
        scratch_shapes=[pltpu.VMEM((rows, flat), f32)] * 4
        + [pltpu.SemaphoreType.DMA((n_block, 4))],
        compiler_params=params(24), name="mixer_scan",
    )(
        stay(mixer_input), stay(mixer_gain.reshape(1, chans)), a_re, a_im, over,
        stay(jnp.swapaxes(input_real, 1, 2).reshape(chans, states)),
        stay(jnp.swapaxes(input_imag, 1, 2).reshape(chans, states)),
        *packs,
    )
    n_half = 2 if capacity % 32 == 0 else 1
    half = capacity // n_half
    share = pl.pallas_call(
        functools.partial(share_kernel, n_ep, capacity),
        out_shape=jax.ShapeDtypeStruct((3, tokens, slots), bf16),
        in_specs=[vmem, vmem], out_specs=vmem, compiler_params=params(8), name="route_share",
    )(stay(routes_t), stay(weight_t))
    got = lax.all_to_all(ends, "ep", split_axis=0, concat_axis=0)

    units = expert_gate.shape[2]
    n_far = n_tp // 2 - 1
    part = n_ep * half
    by_sender = arrived.reshape(n_ep, capacity, feats)
    halves = [by_sender[:, c * half : (c + 1) * half].reshape(part, feats) for c in range(n_half)]
    far_blocks = []
    for c in range(n_half):
        evens = {0: halves[c]}
        bit = n_tp // 2
        while bit > 1:
            evens.update({k ^ bit: swap(b, bit) for k, b in list(evens.items())})
            bit //= 2
        far_blocks.append(evens)
    partner = swap(arrived, 1)

    def fetch(*weights):
        return pl.pallas_call(
            fetch_kernel,
            out_shape=tuple(jax.ShapeDtypeStruct(w.shape, w.dtype) for w in weights),
            in_specs=[hbm] * len(weights), out_specs=(vmem,) * len(weights),
            scratch_shapes=[pltpu.SemaphoreType.DMA((len(weights),))],
            compiler_params=params(10),
        )(*(stay(w) for w in weights))

    weights = (stay(expert_gate), stay(expert_up), stay(expert_down))
    middle = units // 2
    half_shape = jax.ShapeDtypeStruct((n_tp * feats, middle), bf16)
    rest_shape = jax.ShapeDtypeStruct((n_tp * feats, units - middle), bf16)
    firsts = pl.pallas_call(
        first_kernel,
        out_shape=(half_shape, half_shape), in_specs=[hbm] * 2, out_specs=(vmem,) * 2,
        scratch_shapes=[pltpu.SemaphoreType.DMA((2,))],
        compiler_params=params(10), name="fetch_first",
    )(*weights[:2])
    n_unit = max(1, (units - middle) // 256)
    terms = []
    for c in range(n_half):
        blocks = [arrived, partner]
        for k in range(2, n_tp, 2):
            blocks += [far_blocks[c][k], swap(far_blocks[c][k], 1)]
        far_shape = jax.ShapeDtypeStruct((n_far, part, feats), bf16)
        part_shape = jax.ShapeDtypeStruct((part, feats), bf16)
        load = c == 0
        kept = [rest_shape, rest_shape, jax.ShapeDtypeStruct(expert_down.shape, bf16)]
        kept = kept if load else []
        hidden, odd_far, *held = pl.pallas_call(
            functools.partial(hidden_kernel, n_tp, n_ep, c * half, load),
            in_specs=[smem] + [vmem] * (2 * n_tp + 2) + [hbm if load else vmem] * 3,
            out_specs=(vmem,) * (2 + len(kept)),
            scratch_shapes=[pltpu.VMEM((part, n_tp * feats), bf16)]
            + ([pltpu.SemaphoreType.DMA((3, n_unit))] if load else []),
            out_shape=(jax.ShapeDtypeStruct((part, units), bf16), far_shape, *kept),
            compiler_params=params(12),
        )(tp_at, *packs, *blocks, *firsts, *weights)
        weights = held or weights
        theirs = swap(odd_far, 1)
        even_far, near, own = pl.pallas_call(
            rest_kernel,
            in_specs=[smem] + [vmem] * 2, out_specs=(vmem,) * 3,
            out_shape=(far_shape, part_shape, part_shape),
            compiler_params=params(8),
        )(tp_at, hidden, weights[2])
        far = even_far.astype(f32) + theirs.astype(f32)
        terms += [own, swap(near, 1)]
        bit = n_tp // 4
        while bit >= 1:
            come = swap(far[bit - 1 :].astype(bf16), 2 * bit)
            terms.append(come[0])
            far = far[: bit - 1] + come[1:].astype(f32)
            bit //= 2
    result = pl.pallas_call(
        functools.partial(join_kernel, n_half, n_ep),
        out_shape=jax.ShapeDtypeStruct((slots, feats), bf16),
        in_specs=[vmem] * len(terms), out_specs=vmem, compiler_params=params(8),
        name="expert_join",
    )(*terms)
    back = lax.all_to_all(result, "ep", split_axis=0, concat_axis=0, tiled=True)

    mixed = pl.pallas_call(
        read_kernel,
        out_shape=jax.ShapeDtypeStruct((rows, chans), bf16),
        in_specs=[smem, vmem] + [hbm] * 4 + [vmem] * 2, out_specs=vmem,
        scratch_shapes=[pltpu.VMEM((rows, flat), f32)] * 4
        + [pltpu.SemaphoreType.DMA((n_block, 4))],
        compiler_params=params(20), name="mixer_read",
    )(
        ep_at, got, *(stay(x) for x in carried),
        stay(read_real.reshape(chans, states)), stay(read_imag.reshape(chans, states)),
    )
    pieces = gather_tp(mixed)
    value_w, gate_w = fetch(out_value, out_gate)
    mixer_output = pl.pallas_call(
        functools.partial(output_kernel, n_tp),
        out_shape=jax.ShapeDtypeStruct((rows, out_value.shape[1]), bf16),
        in_specs=[smem] + [vmem] * (n_tp + 2), out_specs=vmem, compiler_params=params(10),
        name="mixer_out",
    )(tp_at, *pieces, value_w, gate_w)
    expert_output = pl.pallas_call(
        combine_kernel,
        out_shape=jax.ShapeDtypeStruct((tokens, feats), bf16),
        in_specs=[vmem] * 2, out_specs=vmem, compiler_params=params(8), name="combine",
    )(share, back)
    return mixer_output, expert_output


def solution(mesh):
    return jax.shard_map(
        shards,
        mesh=mesh,
        in_specs=(
            P("ep", "tp"), P("tp"), P("ep", "tp"), P("tp", None), P("tp", None),
            P("tp", None, None), P("tp", None, None), P("tp", None, None), P("tp", None, None),
            P(None, "tp"), P(None, "tp"), P("ep", "tp"), P("tp"), P("ep", None), P("ep", None),
            P("ep", None, "tp"), P("ep", None, "tp"), P("ep", "tp", None),
        ),
        out_specs=(P("ep", "tp"), P("ep", "tp")),
        check_vma=False,
    )
```

```python
import functools

import jax
import jax.numpy as jnp
from jax import lax
from jax.experimental import pallas as pl
from jax.experimental.pallas import tpu as pltpu
from jax.sharding import PartitionSpec as P


f32 = jnp.float32
bf16 = jnp.bfloat16
norm_eps = 1e-05
LANES = 8
NN = (((1,), (0,)), ((), ()))
NT = (((1,), (1,)), ((), ()))
TN = (((0,), (0,)), ((), ()))


def iota(shape, dim):
    return lax.broadcasted_iota(jnp.int32, shape, dim)


def ones_where(mask):
    return jnp.where(mask, 1.0, 0.0).astype(bf16)


def split2(value):
    high = value.astype(bf16)
    return high, (value - high.astype(f32)).astype(bf16)


def split3(value):
    high = value.astype(bf16)
    rest = value - high.astype(f32)
    mid = rest.astype(bf16)
    return high, mid, (rest - mid.astype(f32)).astype(bf16)


def mm(left, right, dims=NN):
    return lax.dot_general(left, right, dims, preferred_element_type=f32)


def mm3(left, right, dims):
    lh, ll = left
    rh, rl = right
    return mm(lh, rh, dims) + (mm(ll, rh, dims) + mm(lh, rl, dims))


def mul(ar, ai, br, bi):
    return ar * br - ai * bi, ar * bi + ai * br


def slot_keys(routes_t, experts):
    top, tokens = routes_t.shape
    number = iota((experts, tokens), 0)
    hit = routes_t[0:1, :] == number
    for k in range(1, top):
        hit = hit | (routes_t[k : k + 1, :] == number)
    before = ones_where(iota((tokens, tokens), 0) < iota((tokens, tokens), 1))
    place = mm(ones_where(hit), before)
    return jnp.where(hit, place, -1.0)


def send_kernel(
    experts, capacity, routes_ref, rows_ref, x_hbm, gain_ref, out_hbm, sums_ref,
    x_ref, out_ref, sems,
):
    come = pltpu.make_async_copy(x_hbm, x_ref, sems.at[0])
    leave = pltpu.make_async_copy(out_ref, out_hbm, sems.at[1])
    come.start()
    keys = slot_keys(routes_ref[...], experts)
    tokens = keys.shape[1]
    slot = iota((capacity, tokens), 0).astype(f32)
    chosen = [ones_where(slot == keys[e : e + 1, :]) for e in range(experts)]
    out_ref[...] = mm(jnp.concatenate(chosen, axis=0), rows_ref[...]).astype(bf16)
    leave.start()
    come.wait()
    rows = x_ref[...]
    count = rows.shape[0]
    ones = jnp.ones((8, rows.shape[1]), bf16)
    wide = rows.astype(f32)
    high, low = split2(wide * wide)
    sums_ref[:, :count] = mm(ones, rows, NT)[0:1]
    sums_ref[:, count : 2 * count] = (mm(ones, high, NT) + mm(ones, low, NT))[0:1]
    sums_ref[:, 2 * count :] = gain_ref[...]
    leave.wait()


def share_kernel(experts, capacity, routes_ref, weight_ref, out_ref):
    routes_t = routes_ref[...]
    weight_t = weight_ref[...]
    keys = slot_keys(routes_t, experts)
    tokens = keys.shape[1]
    number = iota((experts, tokens), 0)
    share = jnp.zeros((experts, tokens), f32)
    for k in range(routes_t.shape[0]):
        share = share + jnp.where(routes_t[k : k + 1, :] == number, weight_t[k : k + 1, :], 0.0)
    slot = iota((capacity, tokens), 0).astype(f32)
    spread = [
        jnp.where(slot == keys[e : e + 1, :], share[e : e + 1, :], 0.0)
        for e in range(experts)
    ]
    same = ones_where(iota((tokens, tokens), 0) == iota((tokens, tokens), 1))
    for n, term in enumerate(split3(jnp.concatenate(spread, axis=0))):
        out_ref[n] = mm(same, term, NT).astype(bf16)


def fetch_kernel(*refs):
    count = (len(refs) - 1) // 2
    sems = refs[-1]
    copies = [
        pltpu.make_async_copy(refs[n], refs[count + n], sems.at[n]) for n in range(count)
    ]
    for copy in copies:
        copy.start()
    for copy in copies:
        copy.wait()


def combine_kernel(share_ref, back_ref, out_ref):
    back = back_ref[...]
    out = mm(share_ref[0], back) + (mm(share_ref[1], back) + mm(share_ref[2], back))
    out_ref[...] = out.astype(bf16)


def first_kernel(*refs):
    count = (len(refs) - 1) // 2
    sems = refs[-1]
    copies = []
    for n in range(count):
        out = refs[count + n]
        copies.append(
            pltpu.make_async_copy(
                refs[n].at[0, :, pl.ds(0, out.shape[1])], out, sems.at[n]
            )
        )
        copies[-1].start()
    for copy in copies:
        copy.wait()


def hidden_kernel(parts, senders, start, load, me_ref, *refs):
    packs = refs[:parts]
    blocks = refs[parts : 2 * parts]
    firsts = refs[2 * parts : 2 * parts + 2]
    refs = refs[2 * parts + 2 :]
    if load:
        sources = refs[:3]
        hidden_ref, odd_ref, gate_ref, up_ref, down_ref, normed_ref, sems = refs[3:]
    else:
        gate_ref, up_ref, down_ref, hidden_ref, odd_ref, normed_ref = refs
    rows, units = hidden_ref.shape
    full, feats = blocks[0].shape
    width = parts * feats
    chunk = rows // senders
    me = me_ref[0]
    lead = packs[0].shape[1] - feats
    middle = firsts[0].shape[1]
    size = min(middle, 256)
    loads = []
    if load:
        for n in range((units - middle) // size):
            cols = pl.ds(n * size, size)
            loads.append([
                pltpu.make_async_copy(
                    source.at[0, :, pl.ds(middle + n * size, size)], ref.at[:, cols],
                    sems.at[m, n],
                )
                for m, (source, ref) in enumerate(zip(sources, (gate_ref, up_ref)))
            ])
        loads.append([pltpu.make_async_copy(sources[2], down_ref, sems.at[2, 0])])
        for group in loads:
            for copy in group:
                copy.start()

    def body(sender, unused):
        here = pl.ds(pl.multiple_of(sender * chunk, chunk), chunk)
        there = pl.ds(pl.multiple_of(sender * (full // senders) + start, chunk), chunk)
        at = [there if k < 2 else here for k in range(parts)]
        total = jnp.zeros((chunk, 1), f32)
        square = jnp.zeros((chunk, 1), f32)
        for k, block in enumerate(blocks):
            wide = block[at[k], :].astype(f32)
            total = total + jnp.sum(wide, axis=1, keepdims=True)
            square = square + jnp.sum(wide * wide, axis=1, keepdims=True)
        mean = total / width
        scale = lax.rsqrt(square / width - mean * mean + norm_eps)
        for k, block in enumerate(blocks):
            gain = packs[k][:, lead:]
            value = (block[at[k], :].astype(f32) - mean) * scale * gain
            cols = pl.ds(pl.multiple_of((me ^ k) * feats, feats), feats)
            normed_ref[here, cols] = value.astype(bf16)
        return unused

    lax.fori_loop(0, senders, body, 0, unroll=4)
    for at in range(0, units, size):
        tables, where = (firsts, at) if at < middle else ((gate_ref, up_ref), at - middle)
        if load and at >= middle:
            for copy in loads[where // size]:
                copy.wait()
        normed = normed_ref[...]
        gate = mm(normed, tables[0][:, pl.ds(where, size)])
        up = mm(normed, tables[1][:, pl.ds(where, size)])
        hidden_ref[:, pl.ds(at, size)] = (gate * jax.nn.sigmoid(gate) * up).astype(bf16)
    if load:
        loads[-1][0].wait()
    for n in range(odd_ref.shape[0]):
        odd_ref[n] = down_part(me ^ (2 * n + 3), hidden_ref, down_ref, feats)


def down_part(which, hidden_ref, weight_ref, feats):
    cols = pl.ds(pl.multiple_of(which * feats, feats), feats)
    return mm(hidden_ref[...], weight_ref[0, :, cols]).astype(bf16)


def rest_kernel(me_ref, hidden_ref, down_ref, even_ref, near_ref, own_ref):
    me = me_ref[0]
    feats = near_ref.shape[1]
    for n in range(even_ref.shape[0]):
        even_ref[n] = down_part(me ^ (2 * n + 2), hidden_ref, down_ref, feats)
    near_ref[...] = down_part(me ^ 1, hidden_ref, down_ref, feats)
    own_ref[...] = down_part(me, hidden_ref, down_ref, feats)


def join_kernel(count, senders, *refs):
    out_hbm, sum_ref, sems = refs[-3:]
    terms = (len(refs) - 3) // count
    chunk = refs[0].shape[0] // senders
    copies = []
    for c in range(count):
        for e in range(senders):
            total = None
            for ref in refs[c * terms : (c + 1) * terms]:
                term = ref[pl.ds(e * chunk, chunk), :].astype(f32)
                total = term if total is None else total + term
            sum_ref[c, e] = total.astype(bf16)
        copies.append(
            pltpu.make_async_copy(
                sum_ref.at[c], out_hbm.at[:, pl.ds(c * chunk, chunk), :], sems.at[c]
            )
        )
        copies[-1].start()
    for copy in copies:
        copy.wait()


def reorder(rows, back):
    steps = rows // LANES
    row, col = iota((rows, rows), 1 if back else 0), iota((rows, rows), 0 if back else 1)
    return ones_where(col == (row % LANES) * steps + row // LANES)


def in_line(table, width):
    states = table.shape[1]
    wide = spread_table(table, states, 1, states, width)
    return jnp.sum(wide, axis=0, keepdims=True)


def sin_cos(angle):
    turns = jnp.floor(angle * 0.6366197723675814 + 0.5)
    rest = angle - turns * 1.5703125
    rest = rest - turns * 4.83751296997070312e-4
    rest = rest - turns * 7.54978995489188e-8
    z = rest * rest
    sine = rest + rest * z * (
        -1.6666654611e-1 + z * (8.3321608736e-3 + z * -1.9515295891e-4)
    )
    cosine = 1.0 - 0.5 * z + z * z * (
        4.166664568298827e-2 + z * (-1.388731625493765e-3 + z * 2.443315711809948e-5)
    )
    quarter = turns.astype(jnp.int32)
    odd = (quarter & 1) != 0
    first = jnp.where(odd, cosine, sine)
    second = jnp.where(odd, sine, cosine)
    first = jnp.where((quarter & 2) != 0, -first, first)
    second = jnp.where(((quarter + 1) & 2) != 0, -second, second)
    return first, second


def spread_table(table, inner, outer_rows, outer_cols, width):
    rows = table.shape[0]
    pick = ones_where(iota((inner, width), 1) % inner == iota((inner, width), 0))
    high, mid, low = split3(table)
    wide = mm(high, pick) + (mm(mid, pick) + mm(low, pick))
    same = iota((rows, width), 0) // outer_rows == iota((rows, width), 1) // outer_cols
    return jnp.where(same, wide, 0.0)


def poles_kernel(count, step_ref, pr_ref, pi_ref, *refs):
    ar_ref, ai_ref, over_ref = refs[count : count + 3]
    copies = [
        pltpu.make_async_copy(refs[n], refs[count + 3 + n], refs[-1].at[n])
        for n in range(count)
    ]
    for copy in copies:
        copy.start()
    groups, states = pr_ref.shape
    rows, flat = ar_ref.shape
    order = reorder(rows, False)
    poles_re = in_line(pr_ref[...], flat)
    poles_im = in_line(pi_ref[...], flat)
    size = poles_re * poles_re + poles_im * poles_im
    over_ref[0:1, :] = poles_re / size
    over_ref[1:2, :] = -poles_im / size
    d_high, d_mid, d_low = (
        mm(part, order, NT).astype(bf16) for part in split3(step_ref[...])
    )
    piece = min(flat, 256)
    for at in range(0, flat, piece):
        cols = pl.ds(at, piece)
        expand = ones_where(
            iota((groups, piece), 0) == (iota((groups, piece), 1) + at) // states
        )
        delta = mm(d_high, expand, TN) + (mm(d_mid, expand, TN) + mm(d_low, expand, TN))
        size = jnp.exp(poles_re[:, at : at + piece] * delta)
        sine, cosine = sin_cos(poles_im[:, at : at + piece] * delta)
        ar_ref[:, cols] = size * cosine
        ai_ref[:, cols] = size * sine
    for copy in copies:
        copy.wait()


def scan_kernel(
    total, parts, x_ref, gain_ref, ar_ref, ai_ref, over_ref, ir_ref, ii_ref, *refs,
):
    packs = refs[:parts]
    h_re_out, h_im_out, c_re_out, c_im_out, end_ref = refs[parts : parts + 5]
    hr_ref, hi_ref, cr_ref, ci_ref, sems = refs[parts + 5 :]
    rows, feats = x_ref.shape
    flat = ar_ref.shape[1]
    states = ir_ref.shape[1]
    inner = feats // (flat // states)
    steps = rows // LANES
    order = reorder(rows, False)
    packed = packs[0][:, : 2 * rows]
    for other in packs[1:]:
        packed = packed + other[:, : 2 * rows]
    mean = packed[:, :rows] / total
    scale = lax.rsqrt(packed[:, rows:] / total - mean * mean + norm_eps)
    match = iota((rows, rows), 1) == (iota((rows, rows), 0) % LANES) * steps + iota(
        (rows, rows), 0
    ) // LANES
    mean_col = jnp.sum(jnp.where(match, mean, 0.0), axis=1, keepdims=True)
    scale_col = jnp.sum(jnp.where(match, scale, 0.0), axis=1, keepdims=True)
    cw = min(feats, 256)
    sw = cw // inner * states
    copies = []
    for b in range(feats // cw):
        chans = pl.ds(b * cw, cw)
        cols = pl.ds(b * sw, sw)
        rows_in = mm(order, x_ref[:, chans])
        normed = split2((rows_in - mean_col) * scale_col * gain_ref[:, chans])
        real = split2(spread_table(ir_ref[chans, :], states, inner, states, sw))
        imag = split2(spread_table(ii_ref[chans, :], states, inner, states, sw))
        hr_ref[:, cols], hi_ref[:, cols] = mul(
            mm3(normed, real, NN), mm3(normed, imag, NN), over_ref[0:1, cols], over_ref[1:2, cols]
        )

        def body(j, carry):
            h_re, h_im, c_re, c_im = carry
            here = pl.ds(pl.multiple_of(j * LANES, LANES), LANES)
            a_re, a_im = ar_ref[here, cols], ai_ref[here, cols]
            d_re, d_im = hr_ref[here, cols], hi_ref[here, cols]
            h_re, h_im = mul(a_re, a_im, h_re + d_re, h_im + d_im)
            h_re, h_im = h_re - d_re, h_im - d_im
            c_re, c_im = mul(a_re, a_im, c_re, c_im)
            hr_ref[here, cols], hi_ref[here, cols] = h_re, h_im
            cr_ref[here, cols], ci_ref[here, cols] = c_re, c_im
            return h_re, h_im, c_re, c_im

        zero = jnp.zeros((LANES, sw), f32)
        lax.fori_loop(0, steps, body, (zero, zero, zero + 1.0, zero), unroll=2)
        for n, (ref, out) in enumerate((
            (hr_ref, h_re_out), (hi_ref, h_im_out), (cr_ref, c_re_out), (ci_ref, c_im_out),
        )):
            copies.append(
                pltpu.make_async_copy(ref.at[:, cols], out.at[:, cols], sems.at[b, n])
            )
            copies[-1].start()
    last = pl.ds(rows - LANES, LANES)
    h_re, h_im, c_re, c_im = hr_ref[last, :], hi_ref[last, :], cr_ref[last, :], ci_ref[last, :]
    p_re, p_im = c_re[0:1], c_im[0:1]
    s_re, s_im = h_re[0:1], h_im[0:1]
    for c in range(1, LANES):
        k_re, k_im = c_re[c : c + 1], c_im[c : c + 1]
        p_re, p_im = mul(k_re, k_im, p_re, p_im)
        s_re, s_im = mul(k_re, k_im, s_re, s_im)
        s_re, s_im = s_re + h_re[c : c + 1], s_im + h_im[c : c + 1]
    ends = jnp.concatenate([p_re, p_im, s_re, s_im], axis=0)
    for i in range(end_ref.shape[0]):
        end_ref[i] = ends
    for copy in copies:
        copy.wait()


def read_kernel(
    me_ref, got_ref, h_re_in, h_im_in, c_re_in, c_im_in, rr_ref, ri_ref, out_ref,
    hr_ref, hi_ref, cr_ref, ci_ref, sems,
):
    rows, flat = hr_ref.shape
    feats = out_ref.shape[1]
    states = rr_ref.shape[1]
    inner = feats // (flat // states)
    steps = rows // LANES
    me = me_ref[0]
    cw = min(feats, 256)
    sw = cw // inner * states
    last = pl.ds(rows - LANES, LANES)
    pairs = ((h_re_in, hr_ref), (h_im_in, hi_ref), (c_re_in, cr_ref), (c_im_in, ci_ref))
    loads = []
    for b in range(feats // cw):
        cols = pl.ds(b * sw, sw)
        loads.append([
            pltpu.make_async_copy(src.at[:, cols], ref.at[:, cols], sems.at[b, n])
            for n, (src, ref) in enumerate(pairs)
        ])
        for copy in loads[-1]:
            copy.start()
    s_re = jnp.zeros((1, flat), f32)
    s_im = jnp.zeros((1, flat), f32)
    for i in range(got_ref.shape[0] - 1):
        ends = got_ref[i]
        n_re, n_im = mul(ends[0:1], ends[1:2], s_re, s_im)
        s_re = jnp.where(i < me, n_re + ends[2:3], s_re)
        s_im = jnp.where(i < me, n_im + ends[3:4], s_im)
    back = reorder(rows, True)
    for b in range(feats // cw):
        chans = pl.ds(b * cw, cw)
        lo = b * sw
        cols = pl.ds(lo, sw)
        real = split2(spread_table(rr_ref[chans, :], states, inner, states, sw))
        imag = split2(spread_table(ri_ref[chans, :], states, inner, states, sw))
        for copy in loads[b]:
            copy.wait()
        h_re, h_im, c_re, c_im = (
            ref[last, cols] for ref in (hr_ref, hi_ref, cr_ref, ci_ref)
        )
        in_re, in_im = [s_re[:, lo : lo + sw]], [s_im[:, lo : lo + sw]]
        for c in range(LANES - 1):
            n_re, n_im = mul(c_re[c : c + 1], c_im[c : c + 1], in_re[-1], in_im[-1])
            in_re.append(n_re + h_re[c : c + 1])
            in_im.append(n_im + h_im[c : c + 1])
        g_re = jnp.concatenate(in_re, axis=0)[None]
        g_im = jnp.concatenate(in_im, axis=0)[None]
        shape = (steps, LANES, sw)
        c_re, c_im = cr_ref[:, cols].reshape(shape), ci_ref[:, cols].reshape(shape)
        f_re = hr_ref[:, cols].reshape(shape) + (c_re * g_re - c_im * g_im)
        f_im = hi_ref[:, cols].reshape(shape) + (c_re * g_im + c_im * g_re)
        response = mm3(split2(f_re.reshape(rows, sw)), real, NT) - mm3(
            split2(f_im.reshape(rows, sw)), imag, NT
        )
        cube = response + 0.044715 * (response * response * response)
        mixed = 0.5 * response * (1.0 + jnp.tanh(0.7978845608028654 * cube))
        out_ref[:, chans] = mm(back, mixed.astype(bf16)).astype(bf16)


def output_kernel(parts, me_ref, *refs):
    pieces = refs[:parts]
    value_ref, gate_ref, out_ref = refs[parts:]
    feats = pieces[0].shape[1]
    value = gate = None
    for k, piece in enumerate(pieces):
        at = pl.ds(pl.multiple_of((me_ref[0] ^ k) * feats, feats), feats)
        rows = piece[...]
        v, g = mm(rows, value_ref[at, :]), mm(rows, gate_ref[at, :])
        value, gate = (v, g) if value is None else (value + v, gate + g)
    out_ref[...] = (value * jax.nn.sigmoid(gate)).astype(bf16)


vmem = pl.BlockSpec(memory_space=pltpu.VMEM)
hbm = pl.BlockSpec(memory_space=pltpu.HBM)
smem = pl.BlockSpec(memory_space=pltpu.SMEM)


def stay(value):
    return pltpu.with_memory_space_constraint(value, pltpu.HBM)


def params(mib):
    return pltpu.CompilerParams(vmem_limit_bytes=mib << 20)


def swap(value, bit):
    count = lax.axis_size("tp")
    return lax.ppermute(value, "tp", [(i, i ^ bit) for i in range(count)])


def gather_tp(value):
    count = lax.axis_size("tp")
    blocks = {0: value}
    bit = count // 2
    while bit >= 1:
        blocks.update({k ^ bit: swap(block, bit) for k, block in list(blocks.items())})
        bit //= 2
    return [blocks[k] for k in range(count)]


def shards(
    mixer_input, mixer_gain, time_step, pole_real, pole_imag, input_real, input_imag,
    read_real, read_imag, out_value, out_gate, expert_input, expert_gain, routes,
    route_weight, expert_gate, expert_up, expert_down,
):
    n_tp, n_ep = lax.axis_size("tp"), lax.axis_size("ep")
    tp_at = lax.axis_index("tp").astype(jnp.int32).reshape(1)
    ep_at = lax.axis_index("ep").astype(jnp.int32).reshape(1)
    tokens, feats = expert_input.shape
    top = routes.shape[1]
    capacity = 2 * top * tokens // n_ep
    slots = n_ep * capacity
    routes_t = routes.T
    weight_t = route_weight.T

    rows, chans = mixer_input.shape
    send, packed = pl.pallas_call(
        functools.partial(send_kernel, n_ep, capacity),
        out_shape=(
            pltpu.HBM((slots, feats), bf16),
            jax.ShapeDtypeStruct((1, 2 * rows + feats), f32),
        ),
        in_specs=[vmem, vmem, hbm, vmem], out_specs=(hbm, vmem),
        scratch_shapes=[
            pltpu.VMEM((rows, chans), bf16), pltpu.VMEM((slots, feats), bf16),
            pltpu.SemaphoreType.DMA((2,)),
        ],
        compiler_params=params(8), name="send_rows",
    )(
        stay(routes_t), stay(expert_input), stay(mixer_input),
        stay(expert_gain.reshape(1, feats)),
    )
    arrived = lax.all_to_all(send, "ep", split_axis=0, concat_axis=0, tiled=True)
    packed, tp_at, ep_at = lax.optimization_barrier((packed, tp_at, ep_at))
    packs = [packed] + [swap(packed, k) for k in range(1, n_tp)]

    groups, states = pole_real.shape
    flat = groups * states
    big = jax.ShapeDtypeStruct((rows, flat), f32)
    inputs = (
        mixer_input,
        jnp.swapaxes(input_real, 1, 2).reshape(chans, states),
        jnp.swapaxes(input_imag, 1, 2).reshape(chans, states),
    )
    a_re, a_im, over, x_here, real_here, imag_here = pl.pallas_call(
        functools.partial(poles_kernel, len(inputs)),
        out_shape=(big, big, jax.ShapeDtypeStruct((2, flat), f32))
        + tuple(jax.ShapeDtypeStruct(x.shape, x.dtype) for x in inputs),
        in_specs=[vmem] * 3 + [hbm] * len(inputs), out_specs=(vmem,) * (3 + len(inputs)),
        scratch_shapes=[pltpu.SemaphoreType.DMA((len(inputs),))],
        compiler_params=params(20), name="mixer_poles",
    )(stay(time_step.T), stay(pole_real), stay(pole_imag), *(stay(x) for x in inputs))
    n_block = max(1, chans // 256)
    far_big = pltpu.HBM((rows, flat), f32)
    *carried, ends = pl.pallas_call(
        functools.partial(scan_kernel, float(chans * n_tp), n_tp),
        out_shape=(far_big,) * 4 + (jax.ShapeDtypeStruct((n_ep, 4, flat), f32),),
        in_specs=[vmem] * (7 + n_tp), out_specs=(hbm,) * 4 + (vmem,),
        scratch_shapes=[pltpu.VMEM((rows, flat), f32)] * 4
        + [pltpu.SemaphoreType.DMA((n_block, 4))],
        compiler_params=params(24), name="mixer_scan",
    )(
        x_here, stay(mixer_gain.reshape(1, chans)), a_re, a_im, over, real_here, imag_here,
        *packs,
    )
    n_half = 2 if capacity % 32 == 0 else 1
    half = capacity // n_half
    share = pl.pallas_call(
        functools.partial(share_kernel, n_ep, capacity),
        out_shape=jax.ShapeDtypeStruct((3, tokens, slots), bf16),
        in_specs=[vmem, vmem], out_specs=vmem, compiler_params=params(8), name="route_share",
    )(stay(routes_t), stay(weight_t))
    got = lax.all_to_all(ends, "ep", split_axis=0, concat_axis=0)

    units = expert_gate.shape[2]
    n_far = n_tp // 2 - 1
    part = n_ep * half
    by_sender = arrived.reshape(n_ep, capacity, feats)
    halves = [by_sender[:, c * half : (c + 1) * half].reshape(part, feats) for c in range(n_half)]
    far_blocks = []
    for c in range(n_half):
        evens = {0: halves[c]}
        bit = n_tp // 2
        while bit > 1:
            evens.update({k ^ bit: swap(b, bit) for k, b in list(evens.items())})
            bit //= 2
        far_blocks.append(evens)
    partner = swap(arrived, 1)

    def fetch(*weights):
        return pl.pallas_call(
            fetch_kernel,
            out_shape=tuple(jax.ShapeDtypeStruct(w.shape, w.dtype) for w in weights),
            in_specs=[hbm] * len(weights), out_specs=(vmem,) * len(weights),
            scratch_shapes=[pltpu.SemaphoreType.DMA((len(weights),))],
            compiler_params=params(10),
        )(*(stay(w) for w in weights))

    weights = (stay(expert_gate), stay(expert_up), stay(expert_down))
    middle = units // 2
    half_shape = jax.ShapeDtypeStruct((n_tp * feats, middle), bf16)
    rest_shape = jax.ShapeDtypeStruct((n_tp * feats, units - middle), bf16)
    firsts = pl.pallas_call(
        first_kernel,
        out_shape=(half_shape, half_shape), in_specs=[hbm] * 2, out_specs=(vmem,) * 2,
        scratch_shapes=[pltpu.SemaphoreType.DMA((2,))],
        compiler_params=params(10), name="fetch_first",
    )(*weights[:2])
    n_unit = max(1, (units - middle) // 256)
    terms = []
    for c in range(n_half):
        blocks = [arrived, partner]
        for k in range(2, n_tp, 2):
            blocks += [far_blocks[c][k], swap(far_blocks[c][k], 1)]
        far_shape = jax.ShapeDtypeStruct((n_far, part, feats), bf16)
        part_shape = jax.ShapeDtypeStruct((part, feats), bf16)
        load = c == 0
        kept = [rest_shape, rest_shape, jax.ShapeDtypeStruct(expert_down.shape, bf16)]
        kept = kept if load else []
        hidden, odd_far, *held = pl.pallas_call(
            functools.partial(hidden_kernel, n_tp, n_ep, c * half, load),
            in_specs=[smem] + [vmem] * (2 * n_tp + 2) + [hbm if load else vmem] * 3,
            out_specs=(vmem,) * (2 + len(kept)),
            scratch_shapes=[pltpu.VMEM((part, n_tp * feats), bf16)]
            + ([pltpu.SemaphoreType.DMA((3, n_unit))] if load else []),
            out_shape=(jax.ShapeDtypeStruct((part, units), bf16), far_shape, *kept),
            compiler_params=params(12),
        )(tp_at, *packs, *blocks, *firsts, *weights)
        weights = held or weights
        theirs = swap(odd_far, 1)
        even_far, near, own = pl.pallas_call(
            rest_kernel,
            in_specs=[smem] + [vmem] * 2, out_specs=(vmem,) * 3,
            out_shape=(far_shape, part_shape, part_shape),
            compiler_params=params(8),
        )(tp_at, hidden, weights[2])
        far = even_far.astype(f32) + theirs.astype(f32)
        terms += [own, swap(near, 1)]
        bit = n_tp // 4
        while bit >= 1:
            come = swap(far[bit - 1 :].astype(bf16), 2 * bit)
            terms.append(come[0])
            far = far[: bit - 1] + come[1:].astype(f32)
            bit //= 2
    result = pl.pallas_call(
        functools.partial(join_kernel, n_half, n_ep),
        out_shape=pltpu.HBM((n_ep, capacity, feats), bf16),
        in_specs=[vmem] * len(terms), out_specs=hbm,
        scratch_shapes=[
            pltpu.VMEM((n_half, n_ep, half, feats), bf16),
            pltpu.SemaphoreType.DMA((n_half,)),
        ],
        compiler_params=params(8), name="expert_join",
    )(*terms).reshape(slots, feats)
    back = lax.all_to_all(result, "ep", split_axis=0, concat_axis=0, tiled=True)

    mixed = pl.pallas_call(
        read_kernel,
        out_shape=jax.ShapeDtypeStruct((rows, chans), bf16),
        in_specs=[smem, vmem] + [hbm] * 4 + [vmem] * 2, out_specs=vmem,
        scratch_shapes=[pltpu.VMEM((rows, flat), f32)] * 4
        + [pltpu.SemaphoreType.DMA((n_block, 4))],
        compiler_params=params(20), name="mixer_read",
    )(
        ep_at, got, *(stay(x) for x in carried),
        stay(read_real.reshape(chans, states)), stay(read_imag.reshape(chans, states)),
    )
    pieces = gather_tp(mixed)
    value_w, gate_w = fetch(out_value, out_gate)
    mixer_output = pl.pallas_call(
        functools.partial(output_kernel, n_tp),
        out_shape=jax.ShapeDtypeStruct((rows, out_value.shape[1]), bf16),
        in_specs=[smem] + [vmem] * (n_tp + 2), out_specs=vmem, compiler_params=params(10),
        name="mixer_out",
    )(tp_at, *pieces, value_w, gate_w)
    expert_output = pl.pallas_call(
        combine_kernel,
        out_shape=jax.ShapeDtypeStruct((tokens, feats), bf16),
        in_specs=[vmem] * 2, out_specs=vmem, compiler_params=params(8), name="combine",
    )(share, back)
    return mixer_output, expert_output


def solution(mesh):
    return jax.shard_map(
        shards,
        mesh=mesh,
        in_specs=(
            P("ep", "tp"), P("tp"), P("ep", "tp"), P("tp", None), P("tp", None),
            P("tp", None, None), P("tp", None, None), P("tp", None, None), P("tp", None, None),
            P(None, "tp"), P(None, "tp"), P("ep", "tp"), P("tp"), P("ep", None), P("ep", None),
            P("ep", None, "tp"), P("ep", None, "tp"), P("ep", "tp", None),
        ),
        out_specs=(P("ep", "tp"), P("ep", "tp")),
        check_vma=False,
    )
```

```python
import functools

import jax
import jax.numpy as jnp
from jax import lax
from jax.experimental import pallas as pl
from jax.experimental.pallas import tpu as pltpu
from jax.sharding import PartitionSpec as P


f32 = jnp.float32
bf16 = jnp.bfloat16
norm_eps = 1e-05
LANES = 8
NN = (((1,), (0,)), ((), ()))
NT = (((1,), (1,)), ((), ()))
TN = (((0,), (0,)), ((), ()))


def iota(shape, dim):
    return lax.broadcasted_iota(jnp.int32, shape, dim)


def ones_where(mask):
    return jnp.where(mask, 1.0, 0.0).astype(bf16)


def split2(value):
    high = value.astype(bf16)
    return high, (value - high.astype(f32)).astype(bf16)


def split3(value):
    high = value.astype(bf16)
    rest = value - high.astype(f32)
    mid = rest.astype(bf16)
    return high, mid, (rest - mid.astype(f32)).astype(bf16)


def mm(left, right, dims=NN):
    return lax.dot_general(left, right, dims, preferred_element_type=f32)


def mm3(left, right, dims):
    lh, ll = left
    rh, rl = right
    return mm(lh, rh, dims) + (mm(ll, rh, dims) + mm(lh, rl, dims))


def mul(ar, ai, br, bi):
    return ar * br - ai * bi, ar * bi + ai * br


def slot_keys(routes_t, experts):
    top, tokens = routes_t.shape
    number = iota((experts, tokens), 0)
    hit = routes_t[0:1, :] == number
    for k in range(1, top):
        hit = hit | (routes_t[k : k + 1, :] == number)
    before = ones_where(iota((tokens, tokens), 0) < iota((tokens, tokens), 1))
    place = mm(ones_where(hit), before)
    return jnp.where(hit, place, -1.0)


def send_kernel(
    experts, capacity, routes_ref, rows_ref, x_hbm, gain_ref, out_hbm, sums_ref,
    x_ref, out_ref, sems,
):
    come = pltpu.make_async_copy(x_hbm, x_ref, sems.at[0])
    leave = pltpu.make_async_copy(out_ref, out_hbm, sems.at[1])
    come.start()
    keys = slot_keys(routes_ref[...], experts)
    tokens = keys.shape[1]
    slot = iota((capacity, tokens), 0).astype(f32)
    chosen = [ones_where(slot == keys[e : e + 1, :]) for e in range(experts)]
    out_ref[...] = mm(jnp.concatenate(chosen, axis=0), rows_ref[...]).astype(bf16)
    leave.start()
    come.wait()
    rows = x_ref[...]
    count = rows.shape[0]
    ones = jnp.ones((8, rows.shape[1]), bf16)
    wide = rows.astype(f32)
    high, low = split2(wide * wide)
    sums_ref[:, :count] = mm(ones, rows, NT)[0:1]
    sums_ref[:, count : 2 * count] = (mm(ones, high, NT) + mm(ones, low, NT))[0:1]
    sums_ref[:, 2 * count :] = gain_ref[...]
    leave.wait()


def share_kernel(experts, capacity, routes_ref, weight_ref, out_ref):
    routes_t = routes_ref[...]
    weight_t = weight_ref[...]
    keys = slot_keys(routes_t, experts)
    tokens = keys.shape[1]
    number = iota((experts, tokens), 0)
    share = jnp.zeros((experts, tokens), f32)
    for k in range(routes_t.shape[0]):
        share = share + jnp.where(routes_t[k : k + 1, :] == number, weight_t[k : k + 1, :], 0.0)
    slot = iota((capacity, tokens), 0).astype(f32)
    spread = [
        jnp.where(slot == keys[e : e + 1, :], share[e : e + 1, :], 0.0)
        for e in range(experts)
    ]
    same = ones_where(iota((tokens, tokens), 0) == iota((tokens, tokens), 1))
    for n, term in enumerate(split3(jnp.concatenate(spread, axis=0))):
        out_ref[n] = mm(same, term, NT).astype(bf16)


def fetch_kernel(*refs):
    count = (len(refs) - 1) // 2
    sems = refs[-1]
    copies = [
        pltpu.make_async_copy(refs[n], refs[count + n], sems.at[n]) for n in range(count)
    ]
    for copy in copies:
        copy.start()
    for copy in copies:
        copy.wait()


def combine_kernel(share_ref, back_ref, out_ref):
    back = back_ref[...]
    out = mm(share_ref[0], back) + (mm(share_ref[1], back) + mm(share_ref[2], back))
    out_ref[...] = out.astype(bf16)


CUTS = 4


def in_pieces(source, target, sems):
    rows = target.shape[0] // CUTS
    return [
        pltpu.make_async_copy(
            source.at[pl.ds(n * rows, rows), :], target.at[pl.ds(n * rows, rows), :], sems.at[n]
        )
        for n in range(CUTS)
    ]


def first_kernel(*refs):
    count = (len(refs) - 1) // 2
    sems = refs[-1]
    copies = []
    for n in range(count):
        out = refs[count + n]
        copies += in_pieces(refs[n].at[0, :, pl.ds(0, out.shape[1])], out, sems.at[n])
    for copy in copies:
        copy.start()
    for copy in copies:
        copy.wait()


def hidden_kernel(parts, senders, start, load, me_ref, *refs):
    packs = refs[:parts]
    blocks = refs[parts : 2 * parts]
    firsts = refs[2 * parts : 2 * parts + 2]
    refs = refs[2 * parts + 2 :]
    if load:
        sources = refs[:3]
        hidden_ref, odd_ref, gate_ref, up_ref, down_ref, normed_ref, sems = refs[3:]
    else:
        gate_ref, up_ref, down_ref, hidden_ref, odd_ref, normed_ref = refs
    rows, units = hidden_ref.shape
    full, feats = blocks[0].shape
    width = parts * feats
    chunk = rows // senders
    me = me_ref[0]
    lead = packs[0].shape[1] - feats
    middle = firsts[0].shape[1]
    size = min(middle, 256)
    loads = []
    if load:
        for n in range((units - middle) // size):
            cols = pl.ds(n * size, size)
            loads.append([
                copy
                for m, (source, ref) in enumerate(zip(sources, (gate_ref, up_ref)))
                for copy in in_pieces(
                    source.at[0, :, pl.ds(middle + n * size, size)], ref.at[:, cols],
                    sems.at[m, n],
                )
            ])
        loads.append(in_pieces(sources[2].at[0], down_ref.at[0], sems.at[2, 0]))
        for group in loads:
            for copy in group:
                copy.start()

    def body(sender, unused):
        here = pl.ds(pl.multiple_of(sender * chunk, chunk), chunk)
        there = pl.ds(pl.multiple_of(sender * (full // senders) + start, chunk), chunk)
        at = [there if k < 2 else here for k in range(parts)]
        total = jnp.zeros((chunk, 1), f32)
        square = jnp.zeros((chunk, 1), f32)
        for k, block in enumerate(blocks):
            wide = block[at[k], :].astype(f32)
            total = total + jnp.sum(wide, axis=1, keepdims=True)
            square = square + jnp.sum(wide * wide, axis=1, keepdims=True)
        mean = total / width
        scale = lax.rsqrt(square / width - mean * mean + norm_eps)
        for k, block in enumerate(blocks):
            gain = packs[k][:, lead:]
            value = (block[at[k], :].astype(f32) - mean) * scale * gain
            cols = pl.ds(pl.multiple_of((me ^ k) * feats, feats), feats)
            normed_ref[here, cols] = value.astype(bf16)
        return unused

    lax.fori_loop(0, senders, body, 0, unroll=4)
    for at in range(0, units, size):
        tables, where = (firsts, at) if at < middle else ((gate_ref, up_ref), at - middle)
        if load and at >= middle:
            for copy in loads[where // size]:
                copy.wait()
        normed = normed_ref[...]
        gate = mm(normed, tables[0][:, pl.ds(where, size)])
        up = mm(normed, tables[1][:, pl.ds(where, size)])
        hidden_ref[:, pl.ds(at, size)] = (gate * jax.nn.sigmoid(gate) * up).astype(bf16)
    if load:
        for copy in loads[-1]:
            copy.wait()
    for n in range(odd_ref.shape[0]):
        odd_ref[n] = down_part(me ^ (2 * n + 3), hidden_ref, down_ref, feats)


def down_part(which, hidden_ref, weight_ref, feats):
    cols = pl.ds(pl.multiple_of(which * feats, feats), feats)
    return mm(hidden_ref[...], weight_ref[0, :, cols]).astype(bf16)


def rest_kernel(me_ref, hidden_ref, down_ref, even_ref, near_ref, own_ref):
    me = me_ref[0]
    feats = near_ref.shape[1]
    for n in range(even_ref.shape[0]):
        even_ref[n] = down_part(me ^ (2 * n + 2), hidden_ref, down_ref, feats)
    near_ref[...] = down_part(me ^ 1, hidden_ref, down_ref, feats)
    own_ref[...] = down_part(me, hidden_ref, down_ref, feats)


def join_kernel(count, senders, *refs):
    out_hbm, sum_ref, sems = refs[-3:]
    terms = (len(refs) - 3) // count
    chunk = refs[0].shape[0] // senders
    copies = []
    for c in range(count):
        for e in range(senders):
            total = None
            for ref in refs[c * terms : (c + 1) * terms]:
                term = ref[pl.ds(e * chunk, chunk), :].astype(f32)
                total = term if total is None else total + term
            sum_ref[c, e] = total.astype(bf16)
        copies.append(
            pltpu.make_async_copy(
                sum_ref.at[c], out_hbm.at[:, pl.ds(c * chunk, chunk), :], sems.at[c]
            )
        )
        copies[-1].start()
    for copy in copies:
        copy.wait()


def reorder(rows, back):
    steps = rows // LANES
    row, col = iota((rows, rows), 1 if back else 0), iota((rows, rows), 0 if back else 1)
    return ones_where(col == (row % LANES) * steps + row // LANES)


def in_line(table, width):
    states = table.shape[1]
    wide = spread_table(table, states, 1, states, width)
    return jnp.sum(wide, axis=0, keepdims=True)


def sin_cos(angle):
    turns = jnp.floor(angle * 0.6366197723675814 + 0.5)
    rest = angle - turns * 1.5703125
    rest = rest - turns * 4.83751296997070312e-4
    rest = rest - turns * 7.54978995489188e-8
    z = rest * rest
    sine = rest + rest * z * (
        -1.6666654611e-1 + z * (8.3321608736e-3 + z * -1.9515295891e-4)
    )
    cosine = 1.0 - 0.5 * z + z * z * (
        4.166664568298827e-2 + z * (-1.388731625493765e-3 + z * 2.443315711809948e-5)
    )
    quarter = turns.astype(jnp.int32)
    odd = (quarter & 1) != 0
    first = jnp.where(odd, cosine, sine)
    second = jnp.where(odd, sine, cosine)
    first = jnp.where((quarter & 2) != 0, -first, first)
    second = jnp.where(((quarter + 1) & 2) != 0, -second, second)
    return first, second


def spread_table(table, inner, outer_rows, outer_cols, width):
    rows = table.shape[0]
    pick = ones_where(iota((inner, width), 1) % inner == iota((inner, width), 0))
    high, mid, low = split3(table)
    wide = mm(high, pick) + (mm(mid, pick) + mm(low, pick))
    same = iota((rows, width), 0) // outer_rows == iota((rows, width), 1) // outer_cols
    return jnp.where(same, wide, 0.0)


def poles_kernel(count, step_ref, pr_ref, pi_ref, *refs):
    ar_ref, ai_ref, over_ref = refs[count : count + 3]
    copies = [
        pltpu.make_async_copy(refs[n], refs[count + 3 + n], refs[-1].at[n])
        for n in range(count)
    ]
    for copy in copies:
        copy.start()
    groups, states = pr_ref.shape
    rows, flat = ar_ref.shape
    order = reorder(rows, False)
    poles_re = in_line(pr_ref[...], flat)
    poles_im = in_line(pi_ref[...], flat)
    size = poles_re * poles_re + poles_im * poles_im
    over_ref[0:1, :] = poles_re / size
    over_ref[1:2, :] = -poles_im / size
    d_high, d_mid, d_low = (
        mm(part, order, NT).astype(bf16) for part in split3(step_ref[...])
    )
    piece = min(flat, 256)
    for at in range(0, flat, piece):
        cols = pl.ds(at, piece)
        expand = ones_where(
            iota((groups, piece), 0) == (iota((groups, piece), 1) + at) // states
        )
        delta = mm(d_high, expand, TN) + (mm(d_mid, expand, TN) + mm(d_low, expand, TN))
        size = jnp.exp(poles_re[:, at : at + piece] * delta)
        sine, cosine = sin_cos(poles_im[:, at : at + piece] * delta)
        ar_ref[:, cols] = size * cosine
        ai_ref[:, cols] = size * sine
    for copy in copies:
        copy.wait()


def scan_kernel(
    total, parts, x_ref, gain_ref, ar_ref, ai_ref, over_ref, ir_ref, ii_ref, *refs,
):
    packs = refs[:parts]
    h_re_out, h_im_out, c_re_out, c_im_out, end_ref = refs[parts : parts + 5]
    hr_ref, hi_ref, cr_ref, ci_ref, sems = refs[parts + 5 :]
    rows, feats = x_ref.shape
    flat = ar_ref.shape[1]
    states = ir_ref.shape[1]
    inner = feats // (flat // states)
    steps = rows // LANES
    order = reorder(rows, False)
    packed = packs[0][:, : 2 * rows]
    for other in packs[1:]:
        packed = packed + other[:, : 2 * rows]
    mean = packed[:, :rows] / total
    scale = lax.rsqrt(packed[:, rows:] / total - mean * mean + norm_eps)
    match = iota((rows, rows), 1) == (iota((rows, rows), 0) % LANES) * steps + iota(
        (rows, rows), 0
    ) // LANES
    mean_col = jnp.sum(jnp.where(match, mean, 0.0), axis=1, keepdims=True)
    scale_col = jnp.sum(jnp.where(match, scale, 0.0), axis=1, keepdims=True)
    cw = min(feats, 256)
    sw = cw // inner * states
    copies = []
    for b in range(feats // cw):
        chans = pl.ds(b * cw, cw)
        cols = pl.ds(b * sw, sw)
        rows_in = mm(order, x_ref[:, chans])
        normed = split2((rows_in - mean_col) * scale_col * gain_ref[:, chans])
        real = split2(spread_table(ir_ref[chans, :], states, inner, states, sw))
        imag = split2(spread_table(ii_ref[chans, :], states, inner, states, sw))
        hr_ref[:, cols], hi_ref[:, cols] = mul(
            mm3(normed, real, NN), mm3(normed, imag, NN), over_ref[0:1, cols], over_ref[1:2, cols]
        )

        def body(j, carry):
            h_re, h_im, c_re, c_im = carry
            here = pl.ds(pl.multiple_of(j * LANES, LANES), LANES)
            a_re, a_im = ar_ref[here, cols], ai_ref[here, cols]
            d_re, d_im = hr_ref[here, cols], hi_ref[here, cols]
            h_re, h_im = mul(a_re, a_im, h_re + d_re, h_im + d_im)
            h_re, h_im = h_re - d_re, h_im - d_im
            c_re, c_im = mul(a_re, a_im, c_re, c_im)
            hr_ref[here, cols], hi_ref[here, cols] = h_re, h_im
            cr_ref[here, cols], ci_ref[here, cols] = c_re, c_im
            return h_re, h_im, c_re, c_im

        zero = jnp.zeros((LANES, sw), f32)
        lax.fori_loop(0, steps, body, (zero, zero, zero + 1.0, zero), unroll=2)
        for n, (ref, out) in enumerate((
            (hr_ref, h_re_out), (hi_ref, h_im_out), (cr_ref, c_re_out), (ci_ref, c_im_out),
        )):
            copies.append(
                pltpu.make_async_copy(ref.at[:, cols], out.at[:, cols], sems.at[b, n])
            )
            copies[-1].start()
    last = pl.ds(rows - LANES, LANES)
    h_re, h_im, c_re, c_im = hr_ref[last, :], hi_ref[last, :], cr_ref[last, :], ci_ref[last, :]
    p_re, p_im = c_re[0:1], c_im[0:1]
    s_re, s_im = h_re[0:1], h_im[0:1]
    for c in range(1, LANES):
        k_re, k_im = c_re[c : c + 1], c_im[c : c + 1]
        p_re, p_im = mul(k_re, k_im, p_re, p_im)
        s_re, s_im = mul(k_re, k_im, s_re, s_im)
        s_re, s_im = s_re + h_re[c : c + 1], s_im + h_im[c : c + 1]
    ends = jnp.concatenate([p_re, p_im, s_re, s_im], axis=0)
    for i in range(end_ref.shape[0]):
        end_ref[i] = ends
    for copy in copies:
        copy.wait()


def read_kernel(
    me_ref, got_ref, h_re_in, h_im_in, c_re_in, c_im_in, rr_ref, ri_ref, out_ref,
    hr_ref, hi_ref, cr_ref, ci_ref, sems,
):
    rows, flat = hr_ref.shape
    feats = out_ref.shape[1]
    states = rr_ref.shape[1]
    inner = feats // (flat // states)
    steps = rows // LANES
    me = me_ref[0]
    cw = min(feats, 256)
    sw = cw // inner * states
    last = pl.ds(rows - LANES, LANES)
    pairs = ((h_re_in, hr_ref), (h_im_in, hi_ref), (c_re_in, cr_ref), (c_im_in, ci_ref))
    loads = []
    for b in range(feats // cw):
        cols = pl.ds(b * sw, sw)
        loads.append([
            pltpu.make_async_copy(src.at[:, cols], ref.at[:, cols], sems.at[b, n])
            for n, (src, ref) in enumerate(pairs)
        ])
        for copy in loads[-1]:
            copy.start()
    s_re = jnp.zeros((1, flat), f32)
    s_im = jnp.zeros((1, flat), f32)
    for i in range(got_ref.shape[0] - 1):
        ends = got_ref[i]
        n_re, n_im = mul(ends[0:1], ends[1:2], s_re, s_im)
        s_re = jnp.where(i < me, n_re + ends[2:3], s_re)
        s_im = jnp.where(i < me, n_im + ends[3:4], s_im)
    back = reorder(rows, True)
    for b in range(feats // cw):
        chans = pl.ds(b * cw, cw)
        lo = b * sw
        cols = pl.ds(lo, sw)
        real = split2(spread_table(rr_ref[chans, :], states, inner, states, sw))
        imag = split2(spread_table(ri_ref[chans, :], states, inner, states, sw))
        for copy in loads[b]:
            copy.wait()
        h_re, h_im, c_re, c_im = (
            ref[last, cols] for ref in (hr_ref, hi_ref, cr_ref, ci_ref)
        )
        in_re, in_im = [s_re[:, lo : lo + sw]], [s_im[:, lo : lo + sw]]
        for c in range(LANES - 1):
            n_re, n_im = mul(c_re[c : c + 1], c_im[c : c + 1], in_re[-1], in_im[-1])
            in_re.append(n_re + h_re[c : c + 1])
            in_im.append(n_im + h_im[c : c + 1])
        g_re = jnp.concatenate(in_re, axis=0)[None]
        g_im = jnp.concatenate(in_im, axis=0)[None]
        shape = (steps, LANES, sw)
        c_re, c_im = cr_ref[:, cols].reshape(shape), ci_ref[:, cols].reshape(shape)
        f_re = hr_ref[:, cols].reshape(shape) + (c_re * g_re - c_im * g_im)
        f_im = hi_ref[:, cols].reshape(shape) + (c_re * g_im + c_im * g_re)
        response = mm3(split2(f_re.reshape(rows, sw)), real, NT) - mm3(
            split2(f_im.reshape(rows, sw)), imag, NT
        )
        cube = response + 0.044715 * (response * response * response)
        mixed = 0.5 * response * (1.0 + jnp.tanh(0.7978845608028654 * cube))
        out_ref[:, chans] = mm(back, mixed.astype(bf16)).astype(bf16)


def output_kernel(parts, me_ref, *refs):
    pieces = refs[:parts]
    value_ref, gate_ref, out_ref = refs[parts:]
    feats = pieces[0].shape[1]
    value = gate = None
    for k, piece in enumerate(pieces):
        at = pl.ds(pl.multiple_of((me_ref[0] ^ k) * feats, feats), feats)
        rows = piece[...]
        v, g = mm(rows, value_ref[at, :]), mm(rows, gate_ref[at, :])
        value, gate = (v, g) if value is None else (value + v, gate + g)
    out_ref[...] = (value * jax.nn.sigmoid(gate)).astype(bf16)


vmem = pl.BlockSpec(memory_space=pltpu.VMEM)
hbm = pl.BlockSpec(memory_space=pltpu.HBM)
smem = pl.BlockSpec(memory_space=pltpu.SMEM)


def stay(value):
    return pltpu.with_memory_space_constraint(value, pltpu.HBM)


def params(mib):
    return pltpu.CompilerParams(vmem_limit_bytes=mib << 20)


def swap(value, bit):
    count = lax.axis_size("tp")
    return lax.ppermute(value, "tp", [(i, i ^ bit) for i in range(count)])


def gather_tp(value):
    count = lax.axis_size("tp")
    blocks = {0: value}
    bit = count // 2
    while bit >= 1:
        blocks.update({k ^ bit: swap(block, bit) for k, block in list(blocks.items())})
        bit //= 2
    return [blocks[k] for k in range(count)]


def shards(
    mixer_input, mixer_gain, time_step, pole_real, pole_imag, input_real, input_imag,
    read_real, read_imag, out_value, out_gate, expert_input, expert_gain, routes,
    route_weight, expert_gate, expert_up, expert_down,
):
    n_tp, n_ep = lax.axis_size("tp"), lax.axis_size("ep")
    tp_at = lax.axis_index("tp").astype(jnp.int32).reshape(1)
    ep_at = lax.axis_index("ep").astype(jnp.int32).reshape(1)
    tokens, feats = expert_input.shape
    top = routes.shape[1]
    capacity = 2 * top * tokens // n_ep
    slots = n_ep * capacity
    routes_t = routes.T
    weight_t = route_weight.T

    rows, chans = mixer_input.shape
    send, packed = pl.pallas_call(
        functools.partial(send_kernel, n_ep, capacity),
        out_shape=(
            pltpu.HBM((slots, feats), bf16),
            jax.ShapeDtypeStruct((1, 2 * rows + feats), f32),
        ),
        in_specs=[vmem, vmem, hbm, vmem], out_specs=(hbm, vmem),
        scratch_shapes=[
            pltpu.VMEM((rows, chans), bf16), pltpu.VMEM((slots, feats), bf16),
            pltpu.SemaphoreType.DMA((2,)),
        ],
        compiler_params=params(8), name="send_rows",
    )(
        stay(routes_t), stay(expert_input), stay(mixer_input),
        stay(expert_gain.reshape(1, feats)),
    )
    arrived = lax.all_to_all(send, "ep", split_axis=0, concat_axis=0, tiled=True)
    packed, tp_at, ep_at = lax.optimization_barrier((packed, tp_at, ep_at))
    packs = [packed] + [swap(packed, k) for k in range(1, n_tp)]

    groups, states = pole_real.shape
    flat = groups * states
    big = jax.ShapeDtypeStruct((rows, flat), f32)
    inputs = (
        mixer_input,
        jnp.swapaxes(input_real, 1, 2).reshape(chans, states),
        jnp.swapaxes(input_imag, 1, 2).reshape(chans, states),
    )
    a_re, a_im, over, x_here, real_here, imag_here = pl.pallas_call(
        functools.partial(poles_kernel, len(inputs)),
        out_shape=(big, big, jax.ShapeDtypeStruct((2, flat), f32))
        + tuple(jax.ShapeDtypeStruct(x.shape, x.dtype) for x in inputs),
        in_specs=[vmem] * 3 + [hbm] * len(inputs), out_specs=(vmem,) * (3 + len(inputs)),
        scratch_shapes=[pltpu.SemaphoreType.DMA((len(inputs),))],
        compiler_params=params(20), name="mixer_poles",
    )(stay(time_step.T), stay(pole_real), stay(pole_imag), *(stay(x) for x in inputs))
    n_block = max(1, chans // 256)
    far_big = pltpu.HBM((rows, flat), f32)
    *carried, ends = pl.pallas_call(
        functools.partial(scan_kernel, float(chans * n_tp), n_tp),
        out_shape=(far_big,) * 4 + (jax.ShapeDtypeStruct((n_ep, 4, flat), f32),),
        in_specs=[vmem] * (7 + n_tp), out_specs=(hbm,) * 4 + (vmem,),
        scratch_shapes=[pltpu.VMEM((rows, flat), f32)] * 4
        + [pltpu.SemaphoreType.DMA((n_block, 4))],
        compiler_params=params(24), name="mixer_scan",
    )(
        x_here, stay(mixer_gain.reshape(1, chans)), a_re, a_im, over, real_here, imag_here,
        *packs,
    )
    n_half = 2 if capacity % 32 == 0 else 1
    half = capacity // n_half
    share = pl.pallas_call(
        functools.partial(share_kernel, n_ep, capacity),
        out_shape=jax.ShapeDtypeStruct((3, tokens, slots), bf16),
        in_specs=[vmem, vmem], out_specs=vmem, compiler_params=params(8), name="route_share",
    )(stay(routes_t), stay(weight_t))
    got = lax.all_to_all(ends, "ep", split_axis=0, concat_axis=0)

    units = expert_gate.shape[2]
    n_far = n_tp // 2 - 1
    part = n_ep * half
    by_sender = arrived.reshape(n_ep, capacity, feats)
    halves = [by_sender[:, c * half : (c + 1) * half].reshape(part, feats) for c in range(n_half)]
    far_blocks = []
    for c in range(n_half):
        evens = {0: halves[c]}
        bit = n_tp // 2
        while bit > 1:
            evens.update({k ^ bit: swap(b, bit) for k, b in list(evens.items())})
            bit //= 2
        far_blocks.append(evens)
    partner = swap(arrived, 1)

    def fetch(*weights):
        return pl.pallas_call(
            fetch_kernel,
            out_shape=tuple(jax.ShapeDtypeStruct(w.shape, w.dtype) for w in weights),
            in_specs=[hbm] * len(weights), out_specs=(vmem,) * len(weights),
            scratch_shapes=[pltpu.SemaphoreType.DMA((len(weights),))],
            compiler_params=params(10),
        )(*(stay(w) for w in weights))

    weights = (stay(expert_gate), stay(expert_up), stay(expert_down))
    middle = units // 2
    half_shape = jax.ShapeDtypeStruct((n_tp * feats, middle), bf16)
    rest_shape = jax.ShapeDtypeStruct((n_tp * feats, units - middle), bf16)
    firsts = pl.pallas_call(
        first_kernel,
        out_shape=(half_shape, half_shape), in_specs=[hbm] * 2, out_specs=(vmem,) * 2,
        scratch_shapes=[pltpu.SemaphoreType.DMA((2, CUTS))],
        compiler_params=params(10), name="fetch_first",
    )(*weights[:2])
    n_unit = max(1, (units - middle) // 256)
    terms = []
    for c in range(n_half):
        blocks = [arrived, partner]
        for k in range(2, n_tp, 2):
            blocks += [far_blocks[c][k], swap(far_blocks[c][k], 1)]
        far_shape = jax.ShapeDtypeStruct((n_far, part, feats), bf16)
        part_shape = jax.ShapeDtypeStruct((part, feats), bf16)
        load = c == 0
        kept = [rest_shape, rest_shape, jax.ShapeDtypeStruct(expert_down.shape, bf16)]
        kept = kept if load else []
        hidden, odd_far, *held = pl.pallas_call(
            functools.partial(hidden_kernel, n_tp, n_ep, c * half, load),
            in_specs=[smem] + [vmem] * (2 * n_tp + 2) + [hbm if load else vmem] * 3,
            out_specs=(vmem,) * (2 + len(kept)),
            scratch_shapes=[pltpu.VMEM((part, n_tp * feats), bf16)]
            + ([pltpu.SemaphoreType.DMA((3, n_unit, CUTS))] if load else []),
            out_shape=(jax.ShapeDtypeStruct((part, units), bf16), far_shape, *kept),
            compiler_params=params(12),
        )(tp_at, *packs, *blocks, *firsts, *weights)
        weights = held or weights
        theirs = swap(odd_far, 1)
        even_far, near, own = pl.pallas_call(
            rest_kernel,
            in_specs=[smem] + [vmem] * 2, out_specs=(vmem,) * 3,
            out_shape=(far_shape, part_shape, part_shape),
            compiler_params=params(8),
        )(tp_at, hidden, weights[2])
        far = even_far.astype(f32) + theirs.astype(f32)
        terms += [own, swap(near, 1)]
        bit = n_tp // 4
        while bit >= 1:
            come = swap(far[bit - 1 :].astype(bf16), 2 * bit)
            terms.append(come[0])
            far = far[: bit - 1] + come[1:].astype(f32)
            bit //= 2
    result = pl.pallas_call(
        functools.partial(join_kernel, n_half, n_ep),
        out_shape=pltpu.HBM((n_ep, capacity, feats), bf16),
        in_specs=[vmem] * len(terms), out_specs=hbm,
        scratch_shapes=[
            pltpu.VMEM((n_half, n_ep, half, feats), bf16),
            pltpu.SemaphoreType.DMA((n_half,)),
        ],
        compiler_params=params(8), name="expert_join",
    )(*terms).reshape(slots, feats)
    back = lax.all_to_all(result, "ep", split_axis=0, concat_axis=0, tiled=True)

    mixed = pl.pallas_call(
        read_kernel,
        out_shape=jax.ShapeDtypeStruct((rows, chans), bf16),
        in_specs=[smem, vmem] + [hbm] * 4 + [vmem] * 2, out_specs=vmem,
        scratch_shapes=[pltpu.VMEM((rows, flat), f32)] * 4
        + [pltpu.SemaphoreType.DMA((n_block, 4))],
        compiler_params=params(20), name="mixer_read",
    )(
        ep_at, got, *(stay(x) for x in carried),
        stay(read_real.reshape(chans, states)), stay(read_imag.reshape(chans, states)),
    )
    pieces = gather_tp(mixed)
    value_w, gate_w = fetch(out_value, out_gate)
    mixer_output = pl.pallas_call(
        functools.partial(output_kernel, n_tp),
        out_shape=jax.ShapeDtypeStruct((rows, out_value.shape[1]), bf16),
        in_specs=[smem] + [vmem] * (n_tp + 2), out_specs=vmem, compiler_params=params(10),
        name="mixer_out",
    )(tp_at, *pieces, value_w, gate_w)
    expert_output = pl.pallas_call(
        combine_kernel,
        out_shape=jax.ShapeDtypeStruct((tokens, feats), bf16),
        in_specs=[vmem] * 2, out_specs=vmem, compiler_params=params(8), name="combine",
    )(share, back)
    return mixer_output, expert_output


def solution(mesh):
    return jax.shard_map(
        shards,
        mesh=mesh,
        in_specs=(
            P("ep", "tp"), P("tp"), P("ep", "tp"), P("tp", None), P("tp", None),
            P("tp", None, None), P("tp", None, None), P("tp", None, None), P("tp", None, None),
            P(None, "tp"), P(None, "tp"), P("ep", "tp"), P("tp"), P("ep", None), P("ep", None),
            P("ep", None, "tp"), P("ep", None, "tp"), P("ep", "tp", None),
        ),
        out_specs=(P("ep", "tp"), P("ep", "tp")),
        check_vma=False,
    )
```

```python
import functools

import jax
import jax.numpy as jnp
from jax import lax
from jax.experimental import pallas as pl
from jax.experimental.pallas import tpu as pltpu
from jax.sharding import PartitionSpec as P


f32 = jnp.float32
bf16 = jnp.bfloat16
norm_eps = 1e-05
LANES = 8
NN = (((1,), (0,)), ((), ()))
NT = (((1,), (1,)), ((), ()))
TN = (((0,), (0,)), ((), ()))


def iota(shape, dim):
    return lax.broadcasted_iota(jnp.int32, shape, dim)


def ones_where(mask):
    return jnp.where(mask, 1.0, 0.0).astype(bf16)


def split2(value):
    high = value.astype(bf16)
    return high, (value - high.astype(f32)).astype(bf16)


def split3(value):
    high = value.astype(bf16)
    rest = value - high.astype(f32)
    mid = rest.astype(bf16)
    return high, mid, (rest - mid.astype(f32)).astype(bf16)


def mm(left, right, dims=NN):
    return lax.dot_general(left, right, dims, preferred_element_type=f32)


def mm3(left, right, dims):
    lh, ll = left
    rh, rl = right
    return mm(lh, rh, dims) + (mm(ll, rh, dims) + mm(lh, rl, dims))


def mul(ar, ai, br, bi):
    return ar * br - ai * bi, ar * bi + ai * br


def slot_keys(routes_t, experts):
    top, tokens = routes_t.shape
    number = iota((experts, tokens), 0)
    hit = routes_t[0:1, :] == number
    for k in range(1, top):
        hit = hit | (routes_t[k : k + 1, :] == number)
    before = ones_where(iota((tokens, tokens), 0) < iota((tokens, tokens), 1))
    place = mm(ones_where(hit), before)
    return jnp.where(hit, place, -1.0)


def send_kernel(
    experts, capacity, routes_ref, rows_ref, x_hbm, gain_ref, out_hbm, sums_ref,
    x_ref, out_ref, sems,
):
    come = pltpu.make_async_copy(x_hbm, x_ref, sems.at[0])
    leave = pltpu.make_async_copy(out_ref, out_hbm, sems.at[1])
    come.start()
    keys = slot_keys(routes_ref[...], experts)
    tokens = keys.shape[1]
    slot = iota((capacity, tokens), 0).astype(f32)
    chosen = [ones_where(slot == keys[e : e + 1, :]) for e in range(experts)]
    out_ref[...] = mm(jnp.concatenate(chosen, axis=0), rows_ref[...]).astype(bf16)
    leave.start()
    come.wait()
    rows = x_ref[...]
    count = rows.shape[0]
    ones = jnp.ones((8, rows.shape[1]), bf16)
    wide = rows.astype(f32)
    high, low = split2(wide * wide)
    sums_ref[:, :count] = mm(ones, rows, NT)[0:1]
    sums_ref[:, count : 2 * count] = (mm(ones, high, NT) + mm(ones, low, NT))[0:1]
    sums_ref[:, 2 * count :] = gain_ref[...]
    leave.wait()


def share_kernel(experts, capacity, routes_ref, weight_ref, out_ref):
    routes_t = routes_ref[...]
    weight_t = weight_ref[...]
    keys = slot_keys(routes_t, experts)
    tokens = keys.shape[1]
    number = iota((experts, tokens), 0)
    share = jnp.zeros((experts, tokens), f32)
    for k in range(routes_t.shape[0]):
        share = share + jnp.where(routes_t[k : k + 1, :] == number, weight_t[k : k + 1, :], 0.0)
    slot = iota((capacity, tokens), 0).astype(f32)
    spread = [
        jnp.where(slot == keys[e : e + 1, :], share[e : e + 1, :], 0.0)
        for e in range(experts)
    ]
    same = ones_where(iota((tokens, tokens), 0) == iota((tokens, tokens), 1))
    for n, term in enumerate(split3(jnp.concatenate(spread, axis=0))):
        out_ref[n] = mm(same, term, NT).astype(bf16)


def fetch_kernel(*refs):
    count = (len(refs) - 1) // 2
    sems = refs[-1]
    copies = [
        pltpu.make_async_copy(refs[n], refs[count + n], sems.at[n]) for n in range(count)
    ]
    for copy in copies:
        copy.start()
    for copy in copies:
        copy.wait()


def combine_kernel(share_ref, back_ref, out_ref):
    back = back_ref[...]
    out = mm(share_ref[0], back) + (mm(share_ref[1], back) + mm(share_ref[2], back))
    out_ref[...] = out.astype(bf16)


def first_kernel(skip, *refs):
    count = (len(refs) - 1) // 2
    sems = refs[-1]
    copies = []
    for n in range(count):
        out = refs[count + n]
        copies.append(
            pltpu.make_async_copy(
                refs[n].at[0, :, pl.ds(skip, out.shape[1])], out, sems.at[n]
            )
        )
        copies[-1].start()
    for copy in copies:
        copy.wait()


def hidden_kernel(parts, senders, start, load, early, me_ref, *refs):
    packs = refs[:parts]
    blocks = refs[parts : 2 * parts]
    heads, firsts, refs = refs[2 * parts :][:early], refs[2 * parts + early :], None
    firsts, refs = firsts[:2], firsts[2:]
    if load:
        sources = refs[:3]
        hidden_ref, odd_ref, gate_ref, up_ref, down_ref, normed_ref, sems = refs[3:]
    else:
        gate_ref, up_ref, down_ref, hidden_ref, odd_ref, normed_ref = refs
    rows, units = hidden_ref.shape
    full, feats = blocks[0].shape
    width = parts * feats
    chunk = rows // senders
    me = me_ref[0]
    lead = packs[0].shape[1] - feats
    skip = heads[0].shape[1] if heads else 0
    middle = skip + firsts[0].shape[1]
    size = min(middle, 256)
    loads = []
    if load:
        for n in range((units - middle) // size):
            cols = pl.ds(n * size, size)
            loads.append([
                pltpu.make_async_copy(
                    source.at[0, :, pl.ds(middle + n * size, size)], ref.at[:, cols],
                    sems.at[m, n],
                )
                for m, (source, ref) in enumerate(zip(sources, (gate_ref, up_ref)))
            ])
        loads.append([pltpu.make_async_copy(sources[2], down_ref, sems.at[2, 0])])
        for group in loads:
            for copy in group:
                copy.start()

    def body(sender, unused):
        here = pl.ds(pl.multiple_of(sender * chunk, chunk), chunk)
        there = pl.ds(pl.multiple_of(sender * (full // senders) + start, chunk), chunk)
        at = [there if k < 2 else here for k in range(parts)]
        total = jnp.zeros((chunk, 1), f32)
        square = jnp.zeros((chunk, 1), f32)
        for k, block in enumerate(blocks):
            wide = block[at[k], :].astype(f32)
            total = total + jnp.sum(wide, axis=1, keepdims=True)
            square = square + jnp.sum(wide * wide, axis=1, keepdims=True)
        mean = total / width
        scale = lax.rsqrt(square / width - mean * mean + norm_eps)
        for k, block in enumerate(blocks):
            gain = packs[k][:, lead:]
            value = (block[at[k], :].astype(f32) - mean) * scale * gain
            cols = pl.ds(pl.multiple_of((me ^ k) * feats, feats), feats)
            normed_ref[here, cols] = value.astype(bf16)
        return unused

    lax.fori_loop(0, senders, body, 0, unroll=4)
    for at in range(0, units, size):
        if at < skip:
            tables, where = heads, at
        elif at < middle:
            tables, where = firsts, at - skip
        else:
            tables, where = (gate_ref, up_ref), at - middle
        if load and at >= middle:
            for copy in loads[where // size]:
                copy.wait()
        normed = normed_ref[...]
        gate = mm(normed, tables[0][:, pl.ds(where, size)])
        up = mm(normed, tables[1][:, pl.ds(where, size)])
        hidden_ref[:, pl.ds(at, size)] = (gate * jax.nn.sigmoid(gate) * up).astype(bf16)
    if load:
        loads[-1][0].wait()
    for n in range(odd_ref.shape[0]):
        odd_ref[n] = down_part(me ^ (2 * n + 3), hidden_ref, down_ref, feats)


def down_part(which, hidden_ref, weight_ref, feats):
    cols = pl.ds(pl.multiple_of(which * feats, feats), feats)
    return mm(hidden_ref[...], weight_ref[0, :, cols]).astype(bf16)


def rest_kernel(me_ref, hidden_ref, down_ref, even_ref, near_ref, own_ref):
    me = me_ref[0]
    feats = near_ref.shape[1]
    for n in range(even_ref.shape[0]):
        even_ref[n] = down_part(me ^ (2 * n + 2), hidden_ref, down_ref, feats)
    near_ref[...] = down_part(me ^ 1, hidden_ref, down_ref, feats)
    own_ref[...] = down_part(me, hidden_ref, down_ref, feats)


def join_kernel(count, senders, *refs):
    out_ref = refs[-1]
    terms = (len(refs) - 1) // count
    chunk = refs[0].shape[0] // senders
    for c in range(count):
        for e in range(senders):
            total = None
            for ref in refs[c * terms : (c + 1) * terms]:
                term = ref[pl.ds(e * chunk, chunk), :].astype(f32)
                total = term if total is None else total + term
            out_ref[pl.ds((e * count + c) * chunk, chunk), :] = total.astype(bf16)


def reorder(rows, back):
    steps = rows // LANES
    row, col = iota((rows, rows), 1 if back else 0), iota((rows, rows), 0 if back else 1)
    return ones_where(col == (row % LANES) * steps + row // LANES)


def in_line(table, width):
    states = table.shape[1]
    wide = spread_table(table, states, 1, states, width)
    return jnp.sum(wide, axis=0, keepdims=True)


def sin_cos(angle):
    turns = jnp.floor(angle * 0.6366197723675814 + 0.5)
    rest = angle - turns * 1.5703125
    rest = rest - turns * 4.83751296997070312e-4
    rest = rest - turns * 7.54978995489188e-8
    z = rest * rest
    sine = rest + rest * z * (
        -1.6666654611e-1 + z * (8.3321608736e-3 + z * -1.9515295891e-4)
    )
    cosine = 1.0 - 0.5 * z + z * z * (
        4.166664568298827e-2 + z * (-1.388731625493765e-3 + z * 2.443315711809948e-5)
    )
    quarter = turns.astype(jnp.int32)
    odd = (quarter & 1) != 0
    first = jnp.where(odd, cosine, sine)
    second = jnp.where(odd, sine, cosine)
    first = jnp.where((quarter & 2) != 0, -first, first)
    second = jnp.where(((quarter + 1) & 2) != 0, -second, second)
    return first, second


def spread_table(table, inner, outer_rows, outer_cols, width):
    rows = table.shape[0]
    pick = ones_where(iota((inner, width), 1) % inner == iota((inner, width), 0))
    high, mid, low = split3(table)
    wide = mm(high, pick) + (mm(mid, pick) + mm(low, pick))
    same = iota((rows, width), 0) // outer_rows == iota((rows, width), 1) // outer_cols
    return jnp.where(same, wide, 0.0)


def poles_kernel(step_ref, pr_ref, pi_ref, ar_ref, ai_ref, over_ref):
    groups, states = pr_ref.shape
    rows, flat = ar_ref.shape
    order = reorder(rows, False)
    poles_re = in_line(pr_ref[...], flat)
    poles_im = in_line(pi_ref[...], flat)
    size = poles_re * poles_re + poles_im * poles_im
    over_ref[0:1, :] = poles_re / size
    over_ref[1:2, :] = -poles_im / size
    d_high, d_mid, d_low = (
        mm(part, order, NT).astype(bf16) for part in split3(step_ref[...])
    )
    piece = min(flat, 256)
    for at in range(0, flat, piece):
        cols = pl.ds(at, piece)
        expand = ones_where(
            iota((groups, piece), 0) == (iota((groups, piece), 1) + at) // states
        )
        delta = mm(d_high, expand, TN) + (mm(d_mid, expand, TN) + mm(d_low, expand, TN))
        size = jnp.exp(poles_re[:, at : at + piece] * delta)
        sine, cosine = sin_cos(poles_im[:, at : at + piece] * delta)
        ar_ref[:, cols] = size * cosine
        ai_ref[:, cols] = size * sine


def scan_kernel(
    total, parts, early, x_ref, gain_ref, ar_ref, ai_ref, over_ref, ir_ref, ii_ref, *refs,
):
    packs = refs[:parts]
    refs = refs[parts:]
    sources, refs = refs[:early], refs[early:]
    h_re_out, h_im_out, c_re_out, c_im_out, end_ref = refs[:5]
    heads, refs = refs[5 : 5 + early], refs[5 + early :]
    hr_ref, hi_ref, cr_ref, ci_ref, sems, head_sems = refs
    head_copies = [
        pltpu.make_async_copy(
            source.at[0, :, pl.ds(0, head.shape[1])], head, head_sems.at[n]
        )
        for n, (source, head) in enumerate(zip(sources, heads))
    ]
    for copy in head_copies:
        copy.start()
    rows, feats = x_ref.shape
    flat = ar_ref.shape[1]
    states = ir_ref.shape[1]
    inner = feats // (flat // states)
    steps = rows // LANES
    order = reorder(rows, False)
    packed = packs[0][:, : 2 * rows]
    for other in packs[1:]:
        packed = packed + other[:, : 2 * rows]
    mean = packed[:, :rows] / total
    scale = lax.rsqrt(packed[:, rows:] / total - mean * mean + norm_eps)
    match = iota((rows, rows), 1) == (iota((rows, rows), 0) % LANES) * steps + iota(
        (rows, rows), 0
    ) // LANES
    mean_col = jnp.sum(jnp.where(match, mean, 0.0), axis=1, keepdims=True)
    scale_col = jnp.sum(jnp.where(match, scale, 0.0), axis=1, keepdims=True)
    cw = min(feats, 256)
    sw = cw // inner * states
    copies = []
    for b in range(feats // cw):
        chans = pl.ds(b * cw, cw)
        cols = pl.ds(b * sw, sw)
        rows_in = mm(order, x_ref[:, chans])
        normed = split2((rows_in - mean_col) * scale_col * gain_ref[:, chans])
        real = split2(spread_table(ir_ref[chans, :], states, inner, states, sw))
        imag = split2(spread_table(ii_ref[chans, :], states, inner, states, sw))
        hr_ref[:, cols], hi_ref[:, cols] = mul(
            mm3(normed, real, NN), mm3(normed, imag, NN), over_ref[0:1, cols], over_ref[1:2, cols]
        )

        def body(j, carry):
            h_re, h_im, c_re, c_im = carry
            here = pl.ds(pl.multiple_of(j * LANES, LANES), LANES)
            a_re, a_im = ar_ref[here, cols], ai_ref[here, cols]
            d_re, d_im = hr_ref[here, cols], hi_ref[here, cols]
            h_re, h_im = mul(a_re, a_im, h_re + d_re, h_im + d_im)
            h_re, h_im = h_re - d_re, h_im - d_im
            c_re, c_im = mul(a_re, a_im, c_re, c_im)
            hr_ref[here, cols], hi_ref[here, cols] = h_re, h_im
            cr_ref[here, cols], ci_ref[here, cols] = c_re, c_im
            return h_re, h_im, c_re, c_im

        zero = jnp.zeros((LANES, sw), f32)
        lax.fori_loop(0, steps, body, (zero, zero, zero + 1.0, zero), unroll=2)
        for n, (ref, out) in enumerate((
            (hr_ref, h_re_out), (hi_ref, h_im_out), (cr_ref, c_re_out), (ci_ref, c_im_out),
        )):
            copies.append(
                pltpu.make_async_copy(ref.at[:, cols], out.at[:, cols], sems.at[b, n])
            )
            copies[-1].start()
    last = pl.ds(rows - LANES, LANES)
    h_re, h_im, c_re, c_im = hr_ref[last, :], hi_ref[last, :], cr_ref[last, :], ci_ref[last, :]
    p_re, p_im = c_re[0:1], c_im[0:1]
    s_re, s_im = h_re[0:1], h_im[0:1]
    for c in range(1, LANES):
        k_re, k_im = c_re[c : c + 1], c_im[c : c + 1]
        p_re, p_im = mul(k_re, k_im, p_re, p_im)
        s_re, s_im = mul(k_re, k_im, s_re, s_im)
        s_re, s_im = s_re + h_re[c : c + 1], s_im + h_im[c : c + 1]
    ends = jnp.concatenate([p_re, p_im, s_re, s_im], axis=0)
    for i in range(end_ref.shape[0]):
        end_ref[i] = ends
    for copy in copies + head_copies:
        copy.wait()


def read_kernel(
    me_ref, got_ref, h_re_in, h_im_in, c_re_in, c_im_in, rr_ref, ri_ref, out_ref,
    hr_ref, hi_ref, cr_ref, ci_ref, sems,
):
    rows, flat = hr_ref.shape
    feats = out_ref.shape[1]
    states = rr_ref.shape[1]
    inner = feats // (flat // states)
    steps = rows // LANES
    me = me_ref[0]
    cw = min(feats, 256)
    sw = cw // inner * states
    last = pl.ds(rows - LANES, LANES)
    pairs = ((h_re_in, hr_ref), (h_im_in, hi_ref), (c_re_in, cr_ref), (c_im_in, ci_ref))
    loads = []
    for b in range(feats // cw):
        cols = pl.ds(b * sw, sw)
        loads.append([
            pltpu.make_async_copy(src.at[:, cols], ref.at[:, cols], sems.at[b, n])
            for n, (src, ref) in enumerate(pairs)
        ])
        for copy in loads[-1]:
            copy.start()
    s_re = jnp.zeros((1, flat), f32)
    s_im = jnp.zeros((1, flat), f32)
    for i in range(got_ref.shape[0] - 1):
        ends = got_ref[i]
        n_re, n_im = mul(ends[0:1], ends[1:2], s_re, s_im)
        s_re = jnp.where(i < me, n_re + ends[2:3], s_re)
        s_im = jnp.where(i < me, n_im + ends[3:4], s_im)
    back = reorder(rows, True)
    for b in range(feats // cw):
        chans = pl.ds(b * cw, cw)
        lo = b * sw
        cols = pl.ds(lo, sw)
        real = split2(spread_table(rr_ref[chans, :], states, inner, states, sw))
        imag = split2(spread_table(ri_ref[chans, :], states, inner, states, sw))
        for copy in loads[b]:
            copy.wait()
        h_re, h_im, c_re, c_im = (
            ref[last, cols] for ref in (hr_ref, hi_ref, cr_ref, ci_ref)
        )
        in_re, in_im = [s_re[:, lo : lo + sw]], [s_im[:, lo : lo + sw]]
        for c in range(LANES - 1):
            n_re, n_im = mul(c_re[c : c + 1], c_im[c : c + 1], in_re[-1], in_im[-1])
            in_re.append(n_re + h_re[c : c + 1])
            in_im.append(n_im + h_im[c : c + 1])
        g_re = jnp.concatenate(in_re, axis=0)[None]
        g_im = jnp.concatenate(in_im, axis=0)[None]
        shape = (steps, LANES, sw)
        c_re, c_im = cr_ref[:, cols].reshape(shape), ci_ref[:, cols].reshape(shape)
        f_re = hr_ref[:, cols].reshape(shape) + (c_re * g_re - c_im * g_im)
        f_im = hi_ref[:, cols].reshape(shape) + (c_re * g_im + c_im * g_re)
        response = mm3(split2(f_re.reshape(rows, sw)), real, NT) - mm3(
            split2(f_im.reshape(rows, sw)), imag, NT
        )
        cube = response + 0.044715 * (response * response * response)
        mixed = 0.5 * response * (1.0 + jnp.tanh(0.7978845608028654 * cube))
        out_ref[:, chans] = mm(back, mixed.astype(bf16)).astype(bf16)


def output_kernel(parts, me_ref, *refs):
    pieces = refs[:parts]
    value_ref, gate_ref, out_ref = refs[parts:]
    feats = pieces[0].shape[1]
    value = gate = None
    for k, piece in enumerate(pieces):
        at = pl.ds(pl.multiple_of((me_ref[0] ^ k) * feats, feats), feats)
        rows = piece[...]
        v, g = mm(rows, value_ref[at, :]), mm(rows, gate_ref[at, :])
        value, gate = (v, g) if value is None else (value + v, gate + g)
    out_ref[...] = (value * jax.nn.sigmoid(gate)).astype(bf16)


vmem = pl.BlockSpec(memory_space=pltpu.VMEM)
hbm = pl.BlockSpec(memory_space=pltpu.HBM)
smem = pl.BlockSpec(memory_space=pltpu.SMEM)


def stay(value):
    return pltpu.with_memory_space_constraint(value, pltpu.HBM)


def params(mib):
    return pltpu.CompilerParams(vmem_limit_bytes=mib << 20)


def swap(value, bit):
    count = lax.axis_size("tp")
    return lax.ppermute(value, "tp", [(i, i ^ bit) for i in range(count)])


def gather_tp(value):
    count = lax.axis_size("tp")
    blocks = {0: value}
    bit = count // 2
    while bit >= 1:
        blocks.update({k ^ bit: swap(block, bit) for k, block in list(blocks.items())})
        bit //= 2
    return [blocks[k] for k in range(count)]


def shards(
    mixer_input, mixer_gain, time_step, pole_real, pole_imag, input_real, input_imag,
    read_real, read_imag, out_value, out_gate, expert_input, expert_gain, routes,
    route_weight, expert_gate, expert_up, expert_down,
):
    n_tp, n_ep = lax.axis_size("tp"), lax.axis_size("ep")
    tp_at = lax.axis_index("tp").astype(jnp.int32).reshape(1)
    ep_at = lax.axis_index("ep").astype(jnp.int32).reshape(1)
    tokens, feats = expert_input.shape
    top = routes.shape[1]
    capacity = 2 * top * tokens // n_ep
    slots = n_ep * capacity
    routes_t = routes.T
    weight_t = route_weight.T

    rows, chans = mixer_input.shape
    send, packed = pl.pallas_call(
        functools.partial(send_kernel, n_ep, capacity),
        out_shape=(
            pltpu.HBM((slots, feats), bf16),
            jax.ShapeDtypeStruct((1, 2 * rows + feats), f32),
        ),
        in_specs=[vmem, vmem, hbm, vmem], out_specs=(hbm, vmem),
        scratch_shapes=[
            pltpu.VMEM((rows, chans), bf16), pltpu.VMEM((slots, feats), bf16),
            pltpu.SemaphoreType.DMA((2,)),
        ],
        compiler_params=params(8), name="send_rows",
    )(
        stay(routes_t), stay(expert_input), stay(mixer_input),
        stay(expert_gain.reshape(1, feats)),
    )
    arrived = lax.all_to_all(send, "ep", split_axis=0, concat_axis=0, tiled=True)
    packed, tp_at, ep_at = lax.optimization_barrier((packed, tp_at, ep_at))
    packs = gather_tp(packed)

    groups, states = pole_real.shape
    flat = groups * states
    big = jax.ShapeDtypeStruct((rows, flat), f32)
    a_re, a_im, over = pl.pallas_call(
        poles_kernel,
        out_shape=(big, big, jax.ShapeDtypeStruct((2, flat), f32)),
        in_specs=[vmem] * 3, out_specs=(vmem,) * 3, compiler_params=params(20),
        name="mixer_poles",
    )(stay(time_step.T), stay(pole_real), stay(pole_imag))
    n_block = max(1, chans // 256)
    far_big = pltpu.HBM((rows, flat), f32)
    middle = expert_gate.shape[2] // 2
    head = 256 if middle > 256 else 0
    early = [stay(expert_gate), stay(expert_up)] if head else []
    head_shape = jax.ShapeDtypeStruct((n_tp * feats, head), bf16)
    *carried, ends = pl.pallas_call(
        functools.partial(scan_kernel, float(chans * n_tp), n_tp, len(early)),
        out_shape=(far_big,) * 4
        + (jax.ShapeDtypeStruct((n_ep, 4, flat), f32),)
        + (head_shape,) * len(early),
        in_specs=[vmem] * (7 + n_tp) + [hbm] * len(early),
        out_specs=(hbm,) * 4 + (vmem,) * (1 + len(early)),
        scratch_shapes=[pltpu.VMEM((rows, flat), f32)] * 4
        + [pltpu.SemaphoreType.DMA((n_block, 4)), pltpu.SemaphoreType.DMA((2,))],
        compiler_params=params(24), name="mixer_scan",
    )(
        stay(mixer_input), stay(mixer_gain.reshape(1, chans)), a_re, a_im, over,
        stay(jnp.swapaxes(input_real, 1, 2).reshape(chans, states)),
        stay(jnp.swapaxes(input_imag, 1, 2).reshape(chans, states)),
        *packs, *early,
    )
    carried, ends, heads = carried[:4], (carried + [ends])[4], (carried + [ends])[5:]
    n_half = 2 if capacity % 32 == 0 else 1
    half = capacity // n_half
    share = pl.pallas_call(
        functools.partial(share_kernel, n_ep, capacity),
        out_shape=jax.ShapeDtypeStruct((3, tokens, slots), bf16),
        in_specs=[vmem, vmem], out_specs=vmem, compiler_params=params(8), name="route_share",
    )(stay(routes_t), stay(weight_t))
    got = lax.all_to_all(ends, "ep", split_axis=0, concat_axis=0)

    units = expert_gate.shape[2]
    n_far = n_tp // 2 - 1
    part = n_ep * half
    by_sender = arrived.reshape(n_ep, capacity, feats)
    halves = [by_sender[:, c * half : (c + 1) * half].reshape(part, feats) for c in range(n_half)]
    far_blocks = []
    for c in range(n_half):
        evens = {0: halves[c]}
        bit = n_tp // 2
        while bit > 1:
            evens.update({k ^ bit: swap(b, bit) for k, b in list(evens.items())})
            bit //= 2
        far_blocks.append(evens)
    partner = swap(arrived, 1)

    def fetch(*weights):
        return pl.pallas_call(
            fetch_kernel,
            out_shape=tuple(jax.ShapeDtypeStruct(w.shape, w.dtype) for w in weights),
            in_specs=[hbm] * len(weights), out_specs=(vmem,) * len(weights),
            scratch_shapes=[pltpu.SemaphoreType.DMA((len(weights),))],
            compiler_params=params(10),
        )(*(stay(w) for w in weights))

    weights = (stay(expert_gate), stay(expert_up), stay(expert_down))
    half_shape = jax.ShapeDtypeStruct((n_tp * feats, middle - head), bf16)
    rest_shape = jax.ShapeDtypeStruct((n_tp * feats, units - middle), bf16)
    firsts = pl.pallas_call(
        functools.partial(first_kernel, head),
        out_shape=(half_shape, half_shape), in_specs=[hbm] * 2, out_specs=(vmem,) * 2,
        scratch_shapes=[pltpu.SemaphoreType.DMA((2,))],
        compiler_params=params(10), name="fetch_first",
    )(*weights[:2])
    n_unit = max(1, (units - middle) // 256)
    terms = []
    for c in range(n_half):
        blocks = [arrived, partner]
        for k in range(2, n_tp, 2):
            blocks += [far_blocks[c][k], swap(far_blocks[c][k], 1)]
        far_shape = jax.ShapeDtypeStruct((n_far, part, feats), bf16)
        part_shape = jax.ShapeDtypeStruct((part, feats), bf16)
        load = c == 0
        kept = [rest_shape, rest_shape, jax.ShapeDtypeStruct(expert_down.shape, bf16)]
        kept = kept if load else []
        hidden, odd_far, *held = pl.pallas_call(
            functools.partial(hidden_kernel, n_tp, n_ep, c * half, load, len(early)),
            in_specs=[smem]
            + [vmem] * (2 * n_tp + 2 + len(early))
            + [hbm if load else vmem] * 3,
            out_specs=(vmem,) * (2 + len(kept)),
            scratch_shapes=[pltpu.VMEM((part, n_tp * feats), bf16)]
            + ([pltpu.SemaphoreType.DMA((3, n_unit))] if load else []),
            out_shape=(jax.ShapeDtypeStruct((part, units), bf16), far_shape, *kept),
            compiler_params=params(12),
        )(tp_at, *packs, *blocks, *heads, *firsts, *weights)
        weights = held or weights
        theirs = swap(odd_far, 1)
        even_far, near, own = pl.pallas_call(
            rest_kernel,
            in_specs=[smem] + [vmem] * 2, out_specs=(vmem,) * 3,
            out_shape=(far_shape, part_shape, part_shape),
            compiler_params=params(8),
        )(tp_at, hidden, weights[2])
        far = even_far.astype(f32) + theirs.astype(f32)
        terms += [own, swap(near, 1)]
        bit = n_tp // 4
        while bit >= 1:
            come = swap(far[bit - 1 :].astype(bf16), 2 * bit)
            terms.append(come[0])
            far = far[: bit - 1] + come[1:].astype(f32)
            bit //= 2
    result = pl.pallas_call(
        functools.partial(join_kernel, n_half, n_ep),
        out_shape=jax.ShapeDtypeStruct((slots, feats), bf16),
        in_specs=[vmem] * len(terms), out_specs=vmem, compiler_params=params(8),
        name="expert_join",
    )(*terms)
    back = lax.all_to_all(result, "ep", split_axis=0, concat_axis=0, tiled=True)

    mixed = pl.pallas_call(
        read_kernel,
        out_shape=jax.ShapeDtypeStruct((rows, chans), bf16),
        in_specs=[smem, vmem] + [hbm] * 4 + [vmem] * 2, out_specs=vmem,
        scratch_shapes=[pltpu.VMEM((rows, flat), f32)] * 4
        + [pltpu.SemaphoreType.DMA((n_block, 4))],
        compiler_params=params(20), name="mixer_read",
    )(
        ep_at, got, *(stay(x) for x in carried),
        stay(read_real.reshape(chans, states)), stay(read_imag.reshape(chans, states)),
    )
    pieces = gather_tp(mixed)
    value_w, gate_w = fetch(out_value, out_gate)
    mixer_output = pl.pallas_call(
        functools.partial(output_kernel, n_tp),
        out_shape=jax.ShapeDtypeStruct((rows, out_value.shape[1]), bf16),
        in_specs=[smem] + [vmem] * (n_tp + 2), out_specs=vmem, compiler_params=params(10),
        name="mixer_out",
    )(tp_at, *pieces, value_w, gate_w)
    expert_output = pl.pallas_call(
        combine_kernel,
        out_shape=jax.ShapeDtypeStruct((tokens, feats), bf16),
        in_specs=[vmem] * 2, out_specs=vmem, compiler_params=params(8), name="combine",
    )(share, back)
    return mixer_output, expert_output


def solution(mesh):
    return jax.shard_map(
        shards,
        mesh=mesh,
        in_specs=(
            P("ep", "tp"), P("tp"), P("ep", "tp"), P("tp", None), P("tp", None),
            P("tp", None, None), P("tp", None, None), P("tp", None, None), P("tp", None, None),
            P(None, "tp"), P(None, "tp"), P("ep", "tp"), P("tp"), P("ep", None), P("ep", None),
            P("ep", None, "tp"), P("ep", None, "tp"), P("ep", "tp", None),
        ),
        out_specs=(P("ep", "tp"), P("ep", "tp")),
        check_vma=False,
    )
```
